32 devices in a mesh: sp: 16 (over z, y, x), tp: 2 (over core).
Axes of the slice: x: 2, y: 2, z: 4, core: 2. Of those that a mesh axis runs over, the one named last changes fastest.
Arguments:
- hidden_in: bfloat16 [4096, 2048], P('sp', 'tp'), may hold values from -6 to 6
- w_query_rec: bfloat16 [2048, 2048], P('sp', 'tp'), may hold values from -0.125 to 0.125
- w_forget: bfloat16 [2048, 2048], P('sp', 'tp'), may hold values from -0.125 to 0.125
- w_input: bfloat16 [2048, 2048], P('sp', 'tp'), may hold values from -0.125 to 0.125
- forget_gap: float32 [2048], P('tp'), may hold values from 1e-05 to 0.08
- decay_extra: float32 [4096, 16], P('sp', 'tp'), may hold values from -0.75 to 0
- rec_gain: float32 [128], replicated, may hold values from 0.1 to 1.9
- w_q_down: bfloat16 [2048, 512], P(None, 'tp'), may hold values from -0.125 to 0.125
- w_kv_down: bfloat16 [2048, 256], P(None, 'tp'), may hold values from -0.125 to 0.125
- w_key_rope: bfloat16 [2048, 32], replicated, may hold values from -0.125 to 0.125
- q_gain: float32 [512], replicated, may hold values from 1.4 to 7
- kv_gain: float32 [256], replicated, may hold values from 1.4 to 7
- w_q_nope: bfloat16 [512, 1024], P(None, 'tp'), may hold values from -0.25 to 0.25
- w_q_rope: bfloat16 [512, 512], P(None, 'tp'), may hold values from -0.25 to 0.25
- w_k_up: bfloat16 [256, 1024], P(None, 'tp'), may hold values from -0.375 to 0.375
- w_v_up: bfloat16 [256, 1024], P(None, 'tp'), may hold values from -0.375 to 0.375
- w_out_rec: bfloat16 [2048, 2048], P('tp'), may hold values from -0.109375 to 0.109375
- w_out_att: bfloat16 [1024, 2048], P('tp'), may hold values from -0.109375 to 0.109375
Outputs:
- mixed_out: bfloat16 [4096, 2048], P(('sp', 'tp'))
The draws below stay inside these ranges and needn't reach their ends.
All inputs are finite; a program needn't handle non-finite values.
Results may differ from the reference program's by a relative error of at most 0.02.
The reference program's roundings to bfloat16 on the way count: a program that leaves them out, or rounds other values in their place, can miss the bound.
Values may be sent and summed in bfloat16 or wider, within the bound.
A program may use at most 128 MiB of HBM per device.

```python
import math
import jax
import jax.numpy as jnp
from jax import lax

D = 2048
RECURRENT_HEADS = 16
HG_KDIM = 128
HG_VDIM = 128
HG_BLOCK = 64
MLA_HEADS = 16
NOPE = 64
ROPE = 32
MLA_V = 64
Q_RANK = 512
KV_RANK = 256
TOK_DEV = 256
SEQUENCE_TOKENS = 4096


def draw_forget_gap(key, part):
    first_key, key_second_draw, key_third_draw = jax.random.split(jax.random.fold_in(key, 11), 3)
    fast_share = 0.5
    fast_heads = jax.random.uniform(first_key, (RECURRENT_HEADS, 1)) < fast_share
    slow_gap = jnp.exp(jax.random.uniform(key_second_draw, (RECURRENT_HEADS, HG_KDIM), jnp.float32, jnp.log(1e-05), jnp.log(0.0001)))
    fast_gap = jnp.exp(jax.random.uniform(key_third_draw, (RECURRENT_HEADS, HG_KDIM), jnp.float32, jnp.log(0.03), jnp.log(0.08)))
    return jnp.where(fast_heads, fast_gap, slow_gap).reshape(RECURRENT_HEADS * HG_KDIM).astype(jnp.float32)


def draw_decay_extra(key, part):
    first_key, key_second_draw, key_third_draw = jax.random.split(jax.random.fold_in(key, 23), 3)
    block_count = SEQUENCE_TOKENS // TOK_DEV
    forget_base_rate = jnp.exp(jax.random.uniform(first_key, (block_count, 1, RECURRENT_HEADS), jnp.float32, jnp.log(0.2), 0.0)) / SEQUENCE_TOKENS
    forget_base_rate = jnp.broadcast_to(forget_base_rate, (block_count, TOK_DEV, RECURRENT_HEADS)).reshape(SEQUENCE_TOKENS, RECURRENT_HEADS)
    spike_events = jax.random.uniform(key_second_draw, (SEQUENCE_TOKENS, RECURRENT_HEADS)) < 3.0 / SEQUENCE_TOKENS
    spike_depth = jax.random.uniform(key_third_draw, (SEQUENCE_TOKENS, RECURRENT_HEADS), jnp.float32, jnp.log(0.5), jnp.log(0.8))
    return (jnp.where(spike_events, spike_depth, 0.0) - forget_base_rate).astype(jnp.float32)


def draw_q_gain(key, part):
    values = jax.random.uniform(jax.random.fold_in(key, 31), (Q_RANK,), jnp.float32, 1.4, 2.6)
    return values.astype(jnp.float32)


def draw_kv_gain(key, part):
    values = jax.random.uniform(jax.random.fold_in(key, 37), (KV_RANK,), jnp.float32, 1.4, 2.6)
    return values.astype(jnp.float32)


def level_of(key, dims, shards, low, high):
    def one(dim, parts):
        heights = jax.random.uniform(jax.random.fold_in(jax.random.fold_in(key, 6), dim), (parts,), jnp.float32, low / len(shards), high / len(shards))
        return jnp.repeat(jnp.exp(heights), dims[dim] // parts).reshape((-1,) + (1,) * (len(dims) - dim - 1))

    loudness = one(*shards[0])
    for cut in shards[1:]:
        loudness = loudness * one(*cut)
    return loudness


def scatter_about(key, dims, deviation, bound, cuts=(), kind=jnp.bfloat16):
    drawn = deviation * jax.random.normal(key, dims, jnp.float32)
    if cuts:
        drawn = drawn * level_of(key, dims, cuts, -0.22, 0.18)
    return jnp.clip(drawn, -bound, bound).astype(kind)


def setup_inputs(seed: int = 0) -> dict:
    arg_keys = jax.random.split(jax.random.key(seed), 19)
    return {
        "hidden_in": scatter_about(arg_keys[0], (SEQUENCE_TOKENS, D), 1.0, 6.0, ((0, 16), (1, 2))),
        "w_query_rec": scatter_about(arg_keys[1], (D, RECURRENT_HEADS * HG_KDIM), D ** -0.5, 0.125, ((0, 16), (1, 2))),
        "w_forget": scatter_about(arg_keys[2], (D, RECURRENT_HEADS * HG_KDIM), D ** -0.5, 0.125, ((0, 16), (1, 2))),
        "w_input": scatter_about(arg_keys[3], (D, RECURRENT_HEADS * HG_VDIM), D ** -0.5, 0.125, ((0, 16), (1, 2))),
        "forget_gap": draw_forget_gap(jax.random.fold_in(arg_keys[18], 71), 0),
        "decay_extra": draw_decay_extra(jax.random.fold_in(arg_keys[18], 71), 0),
        "rec_gain": jnp.clip(1.0 + 0.18 * jax.random.normal(arg_keys[6], (HG_VDIM,), jnp.float32), 0.1, 1.9),
        "w_q_down": scatter_about(arg_keys[7], (D, Q_RANK), D ** -0.5, 0.125, ((1, 2),)),
        "w_kv_down": scatter_about(arg_keys[8], (D, KV_RANK), D ** -0.5, 0.125, ((1, 2),)),
        "w_key_rope": scatter_about(arg_keys[9], (D, ROPE), D ** -0.5, 0.125),
        "q_gain": draw_q_gain(jax.random.fold_in(arg_keys[18], 71), 0),
        "kv_gain": draw_kv_gain(jax.random.fold_in(arg_keys[18], 71), 0),
        "w_q_nope": scatter_about(arg_keys[12], (Q_RANK, MLA_HEADS * NOPE), Q_RANK ** -0.5, 0.25, ((1, 2),)),
        "w_q_rope": scatter_about(arg_keys[13], (Q_RANK, MLA_HEADS * ROPE), Q_RANK ** -0.5, 0.25, ((1, 2),)),
        "w_k_up": scatter_about(arg_keys[14], (KV_RANK, MLA_HEADS * NOPE), KV_RANK ** -0.5, 0.375, ((1, 2),)),
        "w_v_up": scatter_about(arg_keys[15], (KV_RANK, MLA_HEADS * MLA_V), KV_RANK ** -0.5, 0.375, ((1, 2),)),
        "w_out_rec": scatter_about(arg_keys[16], (RECURRENT_HEADS * HG_VDIM, D), (RECURRENT_HEADS * HG_VDIM + MLA_HEADS * MLA_V) ** -0.5, 0.109375, ((0, 2),)),
        "w_out_att": scatter_about(arg_keys[17], (MLA_HEADS * MLA_V, D), (RECURRENT_HEADS * HG_VDIM + MLA_HEADS * MLA_V) ** -0.5, 0.109375, ((0, 2),)),
    }


NORM_EPS = 1e-06
ROPE_BASE = 10000.0
NEG_BIG = -1e+30

def rms_scale(values):
    return values * lax.rsqrt(lax.optimization_barrier(jnp.mean(values * values, axis=-1, keepdims=True)) + NORM_EPS)

def rotate_half(values, cosine, sine_table):
    half_width = values.shape[-1] // 2
    lower_half = values[..., :half_width]
    upper_half = values[..., half_width:]
    return jnp.concatenate([lower_half * cosine - upper_half * sine_table, lower_half * sine_table + upper_half * cosine], axis=-1)

def rotary_tables(row_count, offset, rot_width):
    positions = jnp.arange(row_count, dtype=jnp.float32) + offset
    frequency = 1.0 / ROPE_BASE ** (jnp.arange(0, rot_width, 2, dtype=jnp.float32) / rot_width)
    angles = positions[:, None] * frequency[None, :]
    return (jnp.cos(angles), jnp.sin(angles))

def block_step(rec_state, inputs):
    queries, key_in, values, log_forget = inputs
    cumulative = jnp.cumsum(log_forget, axis=1)
    log_gaps = cumulative[:, :, None, :] - cumulative[:, None, :, :]
    block_len = queries.shape[1]
    lower_mask = jnp.tril(jnp.ones((block_len, block_len), jnp.float32))
    decays = jnp.exp(jnp.minimum(log_gaps, 0.0)) * lower_mask[None, :, :, None]
    scores = jnp.einsum('htsd,hsd->hts', queries[:, :, None, :] * decays, key_in, precision=lax.Precision.HIGHEST)
    block_out = jnp.einsum('hts,hsv->htv', scores, values, precision=lax.Precision.HIGHEST) + jnp.einsum('htd,hdv->htv', queries * jnp.exp(cumulative), rec_state, precision=lax.Precision.HIGHEST)
    last_cumul = cumulative[:, -1:, :]
    rec_state = jnp.exp(last_cumul[:, 0, :])[..., None] * rec_state + jnp.einsum('hsd,hsv->hdv', key_in * jnp.exp(last_cumul - cumulative), values, precision=lax.Precision.HIGHEST)
    return (rec_state, block_out)

def recurrence(queries, key_in, values, log_forget):
    seq_total, head_count, key_width = queries.shape
    block_count = seq_total // HG_BLOCK

    def to_blocks(tensor):
        return tensor.reshape(block_count, HG_BLOCK, head_count, tensor.shape[-1]).transpose(0, 2, 1, 3)
    initial = jnp.zeros((head_count, key_width, values.shape[-1]), jnp.float32)
    _, outputs = lax.scan(block_step, initial, (to_blocks(queries), to_blocks(key_in), to_blocks(values), to_blocks(log_forget)))
    return outputs.transpose(0, 2, 1, 3).reshape(seq_total, head_count, values.shape[-1])

def score_block(q_nope, q_rope, k_nope, k_rope, values, q_start, k_start):
    score_scale = 1.0 / math.sqrt(NOPE + ROPE)
    scores = (jnp.einsum('qhd,khd->hqk', q_nope.astype(jnp.float32), k_nope.astype(jnp.float32)) + jnp.einsum('qhr,kr->hqk', q_rope.astype(jnp.float32), k_rope.astype(jnp.float32))) * score_scale
    q_pos = q_start + jnp.arange(q_nope.shape[0], dtype=jnp.int32)
    k_pos = k_start + jnp.arange(k_nope.shape[0], dtype=jnp.int32)
    allowed = k_pos[None, :] <= q_pos[:, None]
    scores = jnp.where(allowed[None], scores, NEG_BIG)
    block_peak = lax.optimization_barrier(jnp.max(scores, axis=-1))
    weights = jnp.where(allowed[None], jnp.exp(scores - block_peak[..., None]), 0.0)
    block_total = lax.optimization_barrier(jnp.sum(weights, axis=-1))
    weights16 = weights.astype(jnp.bfloat16)
    block_sum = jnp.einsum('hqk,khv->hqv', weights16.astype(jnp.float32), values.astype(jnp.float32))
    return (block_peak, block_total, block_sum)

def merge_terms(earlier, later_part):
    top = jnp.maximum(earlier[0], later_part[0])
    old_factor = jnp.exp(earlier[0] - top)
    new_factor = jnp.exp(later_part[0] - top)
    return (top, earlier[1] * old_factor + later_part[1] * new_factor, earlier[2] * old_factor[..., None] + later_part[2] * new_factor[..., None])

def reference(hidden_in, w_query_rec, w_forget, w_input, forget_gap, decay_extra, rec_gain, w_q_down, w_kv_down, w_key_rope, q_gain, kv_gain, w_q_nope, w_q_rope, w_k_up, w_v_up, w_out_rec, w_out_att):
    seq_total = hidden_in.shape[0]

    def project_input(weight):
        return jnp.dot(hidden_in, weight, preferred_element_type=jnp.float32).astype(jnp.bfloat16)
    rec_query = project_input(w_query_rec).astype(jnp.float32).reshape(seq_total, RECURRENT_HEADS, HG_KDIM)
    forget_pre = project_input(w_forget).astype(jnp.float32).reshape(seq_total, RECURRENT_HEADS, HG_KDIM)
    rec_value = project_input(w_input).astype(jnp.float32).reshape(seq_total, RECURRENT_HEADS, HG_VDIM)
    gap_rows = forget_gap.reshape(RECURRENT_HEADS, HG_KDIM)
    closing = jax.nn.sigmoid(-forget_pre)
    key_in = gap_rows * closing
    log_forget = jnp.log1p(-gap_rows * closing) + decay_extra[:, :, None]
    rec_raw = recurrence(rec_query, key_in, rec_value, log_forget)
    rec_out = (rms_scale(rec_raw) * rec_gain).astype(jnp.bfloat16).reshape(seq_total, RECURRENT_HEADS * HG_VDIM)
    q_latent = project_input(w_q_down)
    kv_latent = project_input(w_kv_down)
    q_normed = (rms_scale(q_latent.astype(jnp.float32)) * q_gain).astype(jnp.bfloat16)
    latent = (rms_scale(kv_latent.astype(jnp.float32)) * kv_gain).astype(jnp.bfloat16)
    cosine, sine_table = rotary_tables(seq_total, 0.0, ROPE)
    key_rope = rotate_half(jnp.dot(hidden_in, w_key_rope, preferred_element_type=jnp.float32), cosine, sine_table).astype(jnp.bfloat16)
    q_nope = jnp.dot(q_normed, w_q_nope, preferred_element_type=jnp.float32).astype(jnp.bfloat16)
    q_nope = q_nope.reshape(seq_total, MLA_HEADS, NOPE)
    q_rope = jnp.dot(q_normed, w_q_rope, preferred_element_type=jnp.float32).reshape(seq_total, MLA_HEADS, ROPE)
    q_rope = rotate_half(q_rope, cosine[:, None, :], sine_table[:, None, :]).astype(jnp.bfloat16)
    k_nope = jnp.dot(latent, w_k_up, preferred_element_type=jnp.float32).astype(jnp.bfloat16)
    k_nope = k_nope.reshape(seq_total, MLA_HEADS, NOPE)
    att_value = jnp.dot(latent, w_v_up, preferred_element_type=jnp.float32).astype(jnp.bfloat16)
    att_value = att_value.reshape(seq_total, MLA_HEADS, MLA_V)
    block_len = TOK_DEV
    block_count = seq_total // block_len

    def per_query(query_block):
        q_start = (query_block * block_len).astype(jnp.int32)
        query_nope = lax.dynamic_slice_in_dim(q_nope, q_start, block_len, 0)
        query_rope = lax.dynamic_slice_in_dim(q_rope, q_start, block_len, 0)

        def inner(key_block, running):
            k_start = (key_block * block_len).astype(jnp.int32)
            partials = score_block(query_nope, query_rope, lax.dynamic_slice_in_dim(k_nope, k_start, block_len, 0), lax.dynamic_slice_in_dim(key_rope, k_start, block_len, 0), lax.dynamic_slice_in_dim(att_value, k_start, block_len, 0), q_start, k_start)
            return merge_terms(running, partials)
        initial = (jnp.full((MLA_HEADS, block_len), NEG_BIG, jnp.float32), jnp.zeros((MLA_HEADS, block_len), jnp.float32), jnp.zeros((MLA_HEADS, block_len, MLA_V), jnp.float32))
        top, total_w, accum = lax.fori_loop(jnp.int32(0), query_block + 1, inner, initial)
        result = accum / total_w[..., None]
        return result.transpose(1, 0, 2).reshape(block_len, MLA_HEADS * MLA_V).astype(jnp.bfloat16)
    att_out = lax.map(per_query, jnp.arange(block_count, dtype=jnp.int32)).reshape(seq_total, MLA_HEADS * MLA_V)
    mixed_out = jnp.dot(rec_out, w_out_rec, preferred_element_type=jnp.float32) + jnp.dot(att_out, w_out_att, preferred_element_type=jnp.float32)
    return mixed_out.astype(jnp.bfloat16)
```

```python
import math

import jax
import jax.numpy as jnp
from jax import lax
from jax.experimental import pallas as pl
from jax.experimental.pallas import tpu as pltpu
from jax.sharding import Mesh
from jax.sharding import PartitionSpec as P

HG_KDIM = 128
HG_VDIM = 128
HG_BLOCK = 64
NOPE = 64
ROPE = 32
MLA_V = 64


NORM_EPS = 1e-06
ROPE_BASE = 10000.0
NEG_BIG = -1e30
MESH = pl.DeviceIdType.MESH


def rotate_half(values, cosine, sine_table):
    half_width = values.shape[-1] // 2
    lower_half = values[..., :half_width]
    upper_half = values[..., half_width:]
    return jnp.concatenate(
        [
            lower_half * cosine - upper_half * sine_table,
            lower_half * sine_table + upper_half * cosine,
        ],
        axis=-1,
    )


def rotary_tables(row_count, offset, rot_width):
    positions = jnp.arange(row_count, dtype=jnp.float32) + offset
    frequency = 1.0 / ROPE_BASE ** (jnp.arange(0, rot_width, 2, dtype=jnp.float32) / rot_width)
    angles = positions[:, None] * frequency[None, :]
    return (jnp.cos(angles), jnp.sin(angles))


def dot_t(left, right, left_dim, right_dim):
    return lax.dot_general(
        left, right, (((left_dim,), (right_dim,)), ((), ())), preferred_element_type=jnp.float32
    )


def recurrence_body(rows, q_ref, k_ref, v_ref, lf_ref, s_ref, gain_ref, out_ref, state_ref):
    row_id = lax.broadcasted_iota(jnp.int32, (rows, rows), 0)
    col_id = lax.broadcasted_iota(jnp.int32, (rows, rows), 1)
    lower = row_id >= col_id
    ones = jnp.where(lower, 1.0, 0.0).astype(jnp.float32)
    state = s_ref[0]
    for step in range(k_ref.shape[0] // rows):
        here = pl.ds(step * rows, rows)
        cumulative = jnp.dot(
            ones,
            lf_ref[here, :],
            precision=lax.Precision.HIGHEST,
            preferred_element_type=jnp.float32,
        )
        last = cumulative[rows - 1 : rows, :]
        keys = k_ref[here, :]
        values = v_ref[here, :]
        if out_ref is not None:
            centre = cumulative[rows // 2 - 1 : rows // 2, :]
            queries = q_ref[here, :].astype(jnp.float32)
            q_mid = (queries * jnp.exp(cumulative - centre)).astype(jnp.bfloat16)
            k_mid = (keys * jnp.exp(centre - cumulative)).astype(jnp.bfloat16)
            scores = jnp.where(lower, dot_t(q_mid, k_mid, 1, 1), 0.0).astype(jnp.bfloat16)
            raw = dot_t(scores, values, 1, 0) + dot_t(
                (queries * jnp.exp(cumulative)).astype(jnp.bfloat16),
                state.astype(jnp.bfloat16),
                1,
                1,
            )
            scale = lax.rsqrt(jnp.mean(raw * raw, axis=-1, keepdims=True) + NORM_EPS)
            out_ref[here, :] = (raw * scale * gain_ref[...]).astype(jnp.bfloat16)
        k_last = (keys * jnp.exp(last - cumulative)).astype(jnp.bfloat16)
        state = jnp.exp(last) * state + dot_t(values, k_last, 0, 0)
    if state_ref is not None:
        state_ref[0] = state


def recurrence(queries, keys, values, log_forget, state, gain, emit):
    tokens, width = keys.shape
    heads = width // HG_KDIM
    rows = 2 * HG_BLOCK

    def body(q_ref, k_ref, v_ref, lf_ref, s_ref, gain_ref, out_ref):
        recurrence_body(
            rows,
            q_ref,
            k_ref,
            v_ref,
            lf_ref,
            s_ref,
            gain_ref,
            out_ref if emit else None,
            None if emit else out_ref,
        )

    column = pl.BlockSpec((tokens, HG_KDIM), lambda h: (0, h))
    one_state = pl.BlockSpec((1, HG_VDIM, HG_KDIM), lambda h: (h, 0, 0))
    return pl.pallas_call(
        body,
        grid=(heads,),
        in_specs=[
            column,
            column,
            column,
            column,
            one_state,
            pl.BlockSpec((1, HG_VDIM), lambda h: (0, 0)),
        ],
        out_specs=column if emit else one_state,
        out_shape=jax.ShapeDtypeStruct((tokens, width), jnp.bfloat16)
        if emit
        else jax.ShapeDtypeStruct(state.shape, jnp.float32),
        compiler_params=pltpu.CompilerParams(vmem_limit_bytes=32 * 1024 * 1024),
        cost_estimate=pl.CostEstimate(
            flops=tokens * width * 4000, bytes_accessed=tokens * width * 14, transcendentals=0
        ),
        name="rec_out" if emit else "rec_state",
    )(queries, keys, values, log_forget, state, gain)


def attention_body(
    heads, at_ref, q_ref, lat_ref, rope_ref, wk_ref, wv_ref, out_ref, top_ref, tot_ref, acc_ref
):
    step = pl.program_id(0)
    mine = at_ref[0]

    @pl.when(step == 0)
    def _():
        top_ref[...] = jnp.full(top_ref.shape, NEG_BIG, jnp.float32)
        tot_ref[...] = jnp.zeros(tot_ref.shape, jnp.float32)
        acc_ref[...] = jnp.zeros(acc_ref.shape, jnp.float32)

    def visit(masked):
        latent = lat_ref[...]
        rope = rope_ref[...]
        k_all = dot_t(wk_ref[...], latent, 1, 1).astype(jnp.bfloat16)
        v_all = dot_t(wv_ref[...], latent, 1, 1).astype(jnp.bfloat16)
        for head in range(heads):
            k_head = jnp.concatenate([k_all[head * NOPE : (head + 1) * NOPE], rope], axis=0)
            scores = dot_t(k_head, q_ref[head], 0, 0) * (1.0 / math.sqrt(NOPE + ROPE))
            if masked:
                key_id = lax.broadcasted_iota(jnp.int32, scores.shape, 0)
                query_id = lax.broadcasted_iota(jnp.int32, scores.shape, 1)
                scores = jnp.where(key_id <= query_id, scores, NEG_BIG)
            peak = jnp.max(scores, axis=0, keepdims=True)
            weights = jnp.exp(scores - peak)
            total = jnp.sum(weights, axis=0, keepdims=True)
            part = dot_t(
                v_all[head * MLA_V : (head + 1) * MLA_V], weights.astype(jnp.bfloat16), 1, 0
            )
            before = top_ref[head]
            top = jnp.maximum(before, peak)
            old = jnp.exp(before - top)
            new = jnp.exp(peak - top)
            top_ref[head] = top
            tot_ref[head] = tot_ref[head] * old + total * new
            acc_ref[head] = acc_ref[head] * old + part * new

    @pl.when(step < mine)
    def _():
        visit(False)

    @pl.when(step == mine)
    def _():
        visit(True)
        for head in range(heads):
            out_ref[head * MLA_V : (head + 1) * MLA_V, :] = (
                acc_ref[head] / tot_ref[head]
            ).astype(jnp.bfloat16)


def attention(place, queries, latent, rope, w_key, w_value):
    heads, width, rows = queries.shape
    blocks = latent.shape[0] // rows
    grid_spec = pltpu.PrefetchScalarGridSpec(
        num_scalar_prefetch=1,
        grid=(blocks,),
        in_specs=[
            pl.BlockSpec((heads, width, rows), lambda i, at: (0, 0, 0)),
            pl.BlockSpec((rows, latent.shape[1]), lambda i, at: (jnp.minimum(i, at[0]), 0)),
            pl.BlockSpec((rope.shape[0], rows), lambda i, at: (0, jnp.minimum(i, at[0]))),
            pl.BlockSpec(w_key.shape, lambda i, at: (0, 0)),
            pl.BlockSpec(w_value.shape, lambda i, at: (0, 0)),
        ],
        out_specs=pl.BlockSpec((heads * MLA_V, rows), lambda i, at: (0, 0)),
        scratch_shapes=[
            pltpu.VMEM((heads, 1, rows), jnp.float32),
            pltpu.VMEM((heads, 1, rows), jnp.float32),
            pltpu.VMEM((heads, MLA_V, rows), jnp.float32),
        ],
    )

    def body(*refs):
        attention_body(heads, *refs)

    return pl.pallas_call(
        body,
        grid_spec=grid_spec,
        out_shape=jax.ShapeDtypeStruct((heads * MLA_V, rows), jnp.bfloat16),
        compiler_params=pltpu.CompilerParams(
            dimension_semantics=("arbitrary",), vmem_limit_bytes=32 * 1024 * 1024
        ),
        cost_estimate=pl.CostEstimate(
            flops=blocks * heads * rows * rows * 2000,
            bytes_accessed=latent.size * 2,
            transcendentals=0,
        ),
        name="attend",
    )(place, queries, latent, rope, w_key, w_value)


def both_halves(part, axis):
    if lax.axis_size("tp") != 2:
        return lax.all_gather(part, "tp", axis=axis, tiled=True)
    other = lax.ppermute(part, "tp", [(0, 1), (1, 0)])
    first = lax.axis_index("tp") == 0
    return jnp.concatenate(
        [jnp.where(first, part, other), jnp.where(first, other, part)], axis=axis
    )


def shards(
    hidden_in,
    w_query_rec,
    w_forget,
    w_input,
    forget_gap,
    decay_extra,
    rec_gain,
    w_q_down,
    w_kv_down,
    w_key_rope,
    q_gain,
    kv_gain,
    w_q_nope,
    w_q_rope,
    w_k_up,
    w_v_up,
    w_out_rec,
    w_out_att,
):
    tok_dev = hidden_in.shape[0]
    group = lax.axis_size("pl")
    pl_index = lax.axis_index("pl")
    zz_index = lax.axis_index("zz")
    tp_index = lax.axis_index("tp")
    tp_size = lax.axis_size("tp")
    sp_index = zz_index * group + pl_index

    cols = w_query_rec.shape[1] // group
    heads = cols // HG_KDIM
    depth = w_query_rec.shape[0]
    packed = jnp.concatenate(
        [w.reshape(depth, group, cols) for w in (w_query_rec, w_forget, w_input)], axis=2
    )
    swapped = lax.all_to_all(packed, "pl", split_axis=1, concat_axis=0, tiled=True)
    left_weight = lax.all_gather(
        swapped.reshape(group * depth, 3 * cols), "zz", axis=0, tiled=True
    )
    feature_piece = both_halves(hidden_in, 1)
    member_rows = [feature_piece]
    for gap_to in range(1, group):
        piece = lax.ppermute(hidden_in, "pl", [(i, i ^ gap_to) for i in range(group)])
        member_rows.append(both_halves(piece, 1))
    group_decay = lax.all_gather(decay_extra, "pl", axis=0, tiled=True)
    group_decay = lax.dynamic_slice_in_dim(group_decay, pl_index * heads, heads, 1)

    right_weight = jnp.concatenate([w_q_down, w_kv_down, w_key_rope], axis=1)
    right_sum = jnp.dot(feature_piece, right_weight, preferred_element_type=jnp.float32)
    q_cols = w_q_down.shape[1]
    kv_cols = w_kv_down.shape[1]
    right_round = right_sum[:, : q_cols + kv_cols].astype(jnp.bfloat16)
    both = both_halves(right_round[None], 0).astype(jnp.float32)
    q_latent = jnp.concatenate([both[i, :, :q_cols] for i in range(tp_size)], axis=1)
    kv_latent = jnp.concatenate([both[i, :, q_cols:] for i in range(tp_size)], axis=1)
    q_normed = (
        q_latent
        * lax.rsqrt(jnp.mean(q_latent * q_latent, axis=-1, keepdims=True) + NORM_EPS)
        * q_gain
    ).astype(jnp.bfloat16)
    latent = (
        kv_latent
        * lax.rsqrt(jnp.mean(kv_latent * kv_latent, axis=-1, keepdims=True) + NORM_EPS)
        * kv_gain
    ).astype(jnp.bfloat16)
    q_start = sp_index * tok_dev
    cosine, sine_table = rotary_tables(tok_dev, q_start.astype(jnp.float32), ROPE)
    key_rope = rotate_half(right_sum[:, q_cols + kv_cols :], cosine, sine_table).astype(
        jnp.bfloat16
    )
    group_keys = lax.all_gather(
        jnp.concatenate([latent, key_rope], axis=1), "pl", axis=0, tiled=True
    )
    keys_all = lax.all_gather(group_keys, "zz", axis=0, tiled=True)
    att_heads = w_q_nope.shape[1] // NOPE
    q_nope = jnp.dot(q_normed, w_q_nope, preferred_element_type=jnp.float32).astype(jnp.bfloat16)
    q_rope = jnp.dot(q_normed, w_q_rope, preferred_element_type=jnp.float32).reshape(
        tok_dev, att_heads, ROPE
    )
    q_rope = rotate_half(q_rope, cosine[:, None, :], sine_table[:, None, :]).astype(jnp.bfloat16)
    queries = jnp.concatenate([q_nope.reshape(tok_dev, att_heads, NOPE), q_rope], axis=2)
    att_out = attention(
        sp_index.astype(jnp.int32).reshape(1),
        queries.transpose(1, 2, 0),
        keys_all[:, : latent.shape[1]],
        keys_all[:, latent.shape[1] :].T,
        w_k_up.T,
        w_v_up.T,
    )

    left_weight, att_out = lax.optimization_barrier((left_weight, att_out))
    left_round = jnp.zeros((group * tok_dev, 3 * cols), jnp.bfloat16)
    for gap_to, rows in enumerate(member_rows):
        projected = jnp.dot(rows, left_weight, preferred_element_type=jnp.float32)
        left_round = lax.dynamic_update_slice_in_dim(
            left_round, projected.astype(jnp.bfloat16), (pl_index ^ gap_to) * tok_dev, 0
        )
    rec_query = left_round[:, :cols]
    rec_value = left_round[:, 2 * cols :]
    gap = lax.dynamic_slice_in_dim(forget_gap, pl_index * cols, cols, 0)
    key_in = gap * jax.nn.sigmoid(-left_round[:, cols : 2 * cols].astype(jnp.float32))
    log_forget = jnp.log1p(-key_in) + jnp.repeat(group_decay, HG_KDIM, axis=1)
    gain = rec_gain.reshape(1, HG_VDIM)
    zero_state = jnp.zeros((heads, HG_VDIM, HG_KDIM), jnp.float32)
    local_state = recurrence(rec_query, key_in, rec_value, log_forget, zero_state, gain, False)
    decay = jnp.exp(jnp.sum(log_forget, axis=0)).reshape(heads, 1, HG_KDIM)
    reached = jnp.concatenate([local_state, decay], axis=1)
    zz_size = lax.axis_size("zz")
    into_state = zero_state
    if zz_size <= 4:
        for back in range(zz_size - 1, 0, -1):
            came = lax.ppermute(reached, "zz", [(i, i + back) for i in range(zz_size - back)])
            into_state = came[:, HG_VDIM:] * into_state + came[:, :HG_VDIM]
    else:
        reached = lax.all_gather(reached, "zz", axis=0)
        for place in range(zz_size - 1):
            later = reached[place, :, HG_VDIM:] * into_state + reached[place, :, :HG_VDIM]
            into_state = jnp.where(place < zz_index, later, into_state)
    group_out = recurrence(rec_query, key_in, rec_value, log_forget, into_state, gain, True)
    rec_out = lax.all_to_all(group_out, "pl", split_axis=0, concat_axis=1, tiled=True)

    mixed = jnp.dot(rec_out, w_out_rec, preferred_element_type=jnp.float32) + dot_t(
        att_out, w_out_att, 0, 0
    )
    if tp_size != 2:
        return lax.psum_scatter(
            mixed.astype(jnp.bfloat16), "tp", scatter_dimension=0, tiled=True
        )
    half = tok_dev // 2
    sent = lax.dynamic_slice_in_dim(mixed, (1 - tp_index) * half, half, 0).astype(jnp.bfloat16)
    kept = lax.dynamic_slice_in_dim(mixed, tp_index * half, half, 0)
    came = lax.ppermute(sent, "tp", [(0, 1), (1, 0)])
    return (kept + came.astype(jnp.float32)).astype(jnp.bfloat16)


def fast_kernel(
    sp_size,
    group,
    hid,
    wq,
    wf,
    wi,
    gap_ref,
    dec,
    gain_ref,
    wqd_h,
    wkv_h,
    wkr_h,
    qg_ref,
    kg_ref,
    wqn_h,
    wqr_h,
    wk_h,
    wv_h,
    wor_h,
    woa_h,
    cos_ref,
    sin_ref,
    out_ref,
    hb,
    wb,
    db,
    kbuf,
    lbuf,
    wqd,
    wkv,
    wkr,
    wqn,
    wqr,
    wk,
    wv,
    wor,
    woa,
    qn_ref,
    qbuf,
    top_ref,
    tot_ref,
    acc_ref,
    att_ref,
    proj,
    raw_ref,
    qdec,
    ssend,
    sdsend,
    sbuf,
    sdbuf,
    sin_state,
    ro,
    ra,
    osend,
    orecv,
    oacc,
    loc_sem,
    own_sem,
    wsend_sem,
    wsem,
    zsend_sem,
    fsend_sem,
    hsend_sem,
    hsem,
    hdsend_sem,
    hdsem,
    dsend_sem,
    dsem,
    lsend_sem,
    lsem,
    ksend_sem,
    ksem,
    kdsend_sem,
    kdsem,
    stsend_sem,
    stsem,
    rsend_sem,
    rsem,
    osend_sem,
    orecv_sem,
):
    sp = lax.axis_index("sp")
    tp = lax.axis_index("tp")
    depth = sp_size // group
    z = sp // group
    p = sp % group
    y = p // 2
    x = p % 2
    other = 1 - tp
    rows = hb.shape[2]
    half = rows // 2
    span = hb.shape[3]
    krows = wb.shape[2]
    heads = wb.shape[0]
    att_heads = qbuf.shape[0]
    kd = HG_KDIM

    def pj(j):
        return 2 * ((y + j // 2) % 2) + (x + j) % 2

    def up(k):
        return ((z + k) % depth) * group + p

    def remote(src, dst, send, recv, place, side=tp):
        return pltpu.make_async_remote_copy(
            src_ref=src,
            dst_ref=dst,
            send_sem=send,
            recv_sem=recv,
            device_id=(place, side),
            device_id_type=MESH,
        )

    def wait_in(ref, sem):
        pltpu.make_async_copy(ref, ref, sem).wait()

    loads = [
        pltpu.make_async_copy(hid, hb.at[p, tp], loc_sem.at[0]),
        pltpu.make_async_copy(wqd_h, wqd, loc_sem.at[1]),
        pltpu.make_async_copy(wkv_h, wkv, loc_sem.at[2]),
        pltpu.make_async_copy(wkr_h, wkr, loc_sem.at[3]),
        pltpu.make_async_copy(wqn_h, wqn, loc_sem.at[4]),
        pltpu.make_async_copy(wqr_h, wqr, loc_sem.at[5]),
        pltpu.make_async_copy(wk_h, wk, loc_sem.at[6]),
        pltpu.make_async_copy(wv_h, wv, loc_sem.at[7]),
        pltpu.make_async_copy(wor_h, wor, loc_sem.at[8]),
        pltpu.make_async_copy(woa_h, woa, loc_sem.at[9]),
        pltpu.make_async_copy(dec.at[p], db.at[p], loc_sem.at[10]),
    ]
    loads[0].start()
    for h in range(heads):
        for m, src in enumerate((wq, wf, wi)):
            pltpu.make_async_copy(
                src.at[:, pl.ds(pl.multiple_of((p * heads + h) * kd, kd), kd)],
                wb.at[h, sp, :, pl.ds(m * kd, kd)],
                own_sem.at[h],
            ).start()
    for load in loads[1:]:
        load.start()

    barrier = pltpu.get_barrier_semaphore()
    partners = [(z * group + pj(j), tp) for j in range(1, group)]
    partners += [(up(k), tp) for k in range(1, depth)]
    partners += [(sp, other)]
    for place in partners:
        pl.semaphore_signal(barrier, inc=1, device_id=place, device_id_type=MESH)
    pl.semaphore_wait(barrier, len(partners))

    sends = []

    def launch(copy):
        copy.start()
        sends.append(copy)

    launch(remote(hid, hb.at[p, tp], hdsend_sem.at[0], hdsem.at[p], sp, other))

    def plane_weights(h):
        for j in range(1, group):
            for m, src in enumerate((wq, wf, wi)):
                launch(
                    remote(
                        src.at[:, pl.ds(pl.multiple_of((pj(j) * heads + h) * kd, kd), kd)],
                        wb.at[h, sp, :, pl.ds(m * kd, kd)],
                        wsend_sem.at[h, j, m],
                        wsem.at[h, sp],
                        z * group + pj(j),
                    )
                )

    def around(h, j):
        slot = z * group + pj(j)
        wait_in(wb.at[h, slot], own_sem.at[h] if j == 0 else wsem.at[h, slot])
        for i, k in enumerate((1, depth - 1)):
            launch(
                remote(
                    wb.at[h, slot],
                    wb.at[h, slot],
                    zsend_sem.at[h, j, i],
                    wsem.at[h, slot],
                    up(k),
                )
            )

    def forward(h, j):
        came, to = (depth - 1, 1) if j < group // 2 else (1, depth - 1)
        slot = ((z + came) % depth) * group + pj(j)
        wait_in(wb.at[h, slot], wsem.at[h, slot])
        launch(
            remote(wb.at[h, slot], wb.at[h, slot], fsend_sem.at[h, j], wsem.at[h, slot], up(to))
        )

    plane_weights(0)
    around(0, 0)
    plane_weights(1)
    around(1, 0)
    for j in range(1, group):
        launch(
            remote(
                dec.at[pj(j)], db.at[p], dsend_sem.at[j], dsem.at[p], z * group + pj(j)
            )
        )

    loads[0].wait()
    loads[1].wait()
    loads[2].wait()
    loads[3].wait()
    wait_in(hb.at[p, other], hdsem.at[p])

    def over_features(weight):
        return jnp.dot(
            hb[p, 0], weight[:span, :], preferred_element_type=jnp.float32
        ) + jnp.dot(hb[p, 1], weight[span:, :], preferred_element_type=jnp.float32)

    q_cols = wqd.shape[1]
    kv_cols = wkv.shape[1]
    lbuf[tp, :, :q_cols] = over_features(wqd).astype(jnp.bfloat16)
    lbuf[tp, :, q_cols:] = over_features(wkv).astype(jnp.bfloat16)
    launch(remote(lbuf.at[tp], lbuf.at[tp], lsend_sem.at[0], lsem.at[0], sp, other))
    around(0, 1)
    around(0, 2)
    key_rope = dot_t(wkr[:, :span], hb[p, 0], 1, 1) + dot_t(wkr[:, span:], hb[p, 1], 1, 1)
    cosine = cos_ref[...]
    sine = sin_ref[...]
    kr = ROPE // 2
    first = key_rope[:kr] * cosine - key_rope[kr:] * sine
    second = key_rope[:kr] * sine + key_rope[kr:] * cosine
    kbuf[sp, 0, half:, :] = first.astype(jnp.bfloat16)
    kbuf[sp, 1, half:, :] = second.astype(jnp.bfloat16)
    wait_in(lbuf.at[other], lsem.at[0])
    kv_latent = jnp.concatenate(
        [lbuf[0, :, q_cols:], lbuf[1, :, q_cols:]], axis=1
    ).astype(jnp.float32)
    latent = (
        kv_latent
        * lax.rsqrt(jnp.mean(kv_latent * kv_latent, axis=-1, keepdims=True) + NORM_EPS)
        * kg_ref[...]
    ).astype(jnp.bfloat16)
    kbuf[sp, 0, :half, :] = latent[:half]
    kbuf[sp, 1, :half, :] = latent[half:]

    def key_up(k):
        return remote(
            kbuf.at[sp, tp], kbuf.at[sp, tp], ksend_sem.at[0, k], ksem.at[sp], up(k)
        )

    def key_plane(g):
        block = ((z + depth - g) % depth) * group + p
        return [
            remote(
                kbuf.at[block, tp],
                kbuf.at[block, tp],
                ksend_sem.at[1 + g, j],
                ksem.at[block],
                z * group + pj(j),
            )
            for j in range(1, group)
        ]

    def key_core(block):
        return remote(
            kbuf.at[block, tp],
            kbuf.at[block, tp],
            kdsend_sem.at[block],
            kdsem.at[block],
            sp,
            other,
        )

    for k in range(1, depth):

        @pl.when(z + k < depth)
        def _(k=k):
            key_up(k).start()

    for copy in key_plane(0):
        copy.start()

    around(0, 3)
    around(1, 1)

    q_latent = jnp.concatenate(
        [lbuf[0, :, :q_cols], lbuf[1, :, :q_cols]], axis=1
    ).astype(jnp.float32)
    qn_ref[...] = (
        q_latent
        * lax.rsqrt(jnp.mean(q_latent * q_latent, axis=-1, keepdims=True) + NORM_EPS)
        * qg_ref[...]
    ).astype(jnp.bfloat16)
    loads[4].wait()
    loads[5].wait()
    q_nope = dot_t(wqn[...], qn_ref[...], 0, 1)
    q_rope = dot_t(wqr[...], qn_ref[...], 0, 1)
    for head in range(att_heads):
        qbuf[head, :NOPE, :] = q_nope[head * NOPE : (head + 1) * NOPE].astype(jnp.bfloat16)
        lower = q_rope[head * ROPE : head * ROPE + kr]
        upper = q_rope[head * ROPE + kr : (head + 1) * ROPE]
        qbuf[head, NOPE : NOPE + kr, :] = (lower * cosine - upper * sine).astype(jnp.bfloat16)
        qbuf[head, NOPE + kr :, :] = (lower * sine + upper * cosine).astype(jnp.bfloat16)
    top_ref[...] = jnp.full(top_ref.shape, NEG_BIG, jnp.float32)
    tot_ref[...] = jnp.zeros(tot_ref.shape, jnp.float32)
    acc_ref[...] = jnp.zeros(acc_ref.shape, jnp.float32)
    around(1, 2)
    around(1, 3)

    for g in range(1, depth):

        @pl.when(z >= g)
        def _(g=g):
            block = ((z + depth - g) % depth) * group + p
            wait_in(kbuf.at[block, tp], ksem.at[block])
            for copy in key_plane(g):
                copy.start()
            key_core(block).start()

    def rows_to(j, part, slot):
        at = hb.at[slot, tp, pl.ds(part * half, half), :]
        return remote(
            at, at, hsend_sem.at[j, part, 0 if slot is p else 1], hsem.at[slot, part],
            z * group + pj(j),
        )

    launch(rows_to(1, 0, p))
    launch(rows_to(2, 1, p))
    launch(rows_to(1, 1, p))
    launch(rows_to(2, 0, p))
    for j in range(group):
        forward(0, j)
    loads[6].wait()
    loads[7].wait()

    def visit(block, masked):
        latent_all = jnp.concatenate([kbuf[block, 0, :half], kbuf[block, 1, :half]], axis=0)
        rope = jnp.concatenate([kbuf[block, 0, half:], kbuf[block, 1, half:]], axis=0)
        k_all = dot_t(wk[...], latent_all, 1, 1).astype(jnp.bfloat16)
        v_all = dot_t(wv[...], latent_all, 1, 1).astype(jnp.bfloat16)
        for head in range(att_heads):
            k_head = jnp.concatenate([k_all[head * NOPE : (head + 1) * NOPE], rope], axis=0)
            scores = dot_t(k_head, qbuf[head], 0, 0) * (1.0 / math.sqrt(NOPE + ROPE))
            if masked:
                key_id = lax.broadcasted_iota(jnp.int32, scores.shape, 0)
                query_id = lax.broadcasted_iota(jnp.int32, scores.shape, 1)
                scores = jnp.where(key_id <= query_id, scores, NEG_BIG)
            peak = jnp.max(scores, axis=0, keepdims=True)
            weights = jnp.exp(scores - peak)
            total = jnp.sum(weights, axis=0, keepdims=True)
            part = dot_t(
                v_all[head * MLA_V : (head + 1) * MLA_V], weights.astype(jnp.bfloat16), 1, 0
            )
            before = top_ref[head]
            top = jnp.maximum(before, peak)
            old = jnp.exp(before - top)
            new = jnp.exp(peak - top)
            top_ref[head] = top
            tot_ref[head] = tot_ref[head] * old + total * new
            acc_ref[head] = acc_ref[head] * old + part * new

    def visit_group(g):
        base = ((z + depth - g) % depth) * group
        for j in range(1, group):
            block = base + pj(j)
            wait_in(kbuf.at[block, tp], ksem.at[block])
            key_core(block).start()
        if g == 0:
            visit(sp, True)
        else:
            wait_in(kbuf.at[base + p, other], kdsem.at[base + p])
            visit(base + p, False)

        def step(j, carry):
            block = base + pj(j)
            wait_in(kbuf.at[block, other], kdsem.at[block])
            if g == 0:

                @pl.when(block < sp)
                def _():
                    visit(block, False)
            else:
                visit(block, False)
            return carry

        lax.fori_loop(1, group, step, 0)

    visit_group(0)
    for j in range(group):
        forward(1, j)

    @pl.when(z >= 1)
    def _():
        visit_group(1)

    def onward(j, part, to):
        wait_in(hb.at[pj(j), tp, pl.ds(part * half, half), :], hsem.at[pj(j), part])
        launch(rows_to(to, part, pj(j)))

    def across(j):
        launch(
            remote(
                hb.at[pj(j), tp], hb.at[pj(j), tp], hdsend_sem.at[j], hdsem.at[pj(j)], sp, other
            )
        )

    onward(1, 0, 2)
    onward(2, 1, 1)
    for j, part in ((1, 1), (2, 0)):
        wait_in(hb.at[pj(j), tp, pl.ds(part * half, half), :], hsem.at[pj(j), part])
        across(j)

    for g in range(2, depth):

        @pl.when(z >= g)
        def _(g=g):
            visit_group(g)

    for head in range(att_heads):
        att_ref[head * MLA_V : (head + 1) * MLA_V, :] = (acc_ref[head] / tot_ref[head]).astype(
            jnp.bfloat16
        )
    for part in range(2):
        wait_in(hb.at[pj(3), tp, pl.ds(part * half, half), :], hsem.at[pj(3), part])
    across(3)

    for h in range(heads):
        for j in range(group):
            came = 1 if j < group // 2 else depth - 1
            for k in (came, 2):
                slot = ((z + k) % depth) * group + pj(j)
                wait_in(wb.at[h, slot], wsem.at[h, slot])
    for j in range(1, group):
        wait_in(hb.at[pj(j), other], hdsem.at[pj(j)])
        wait_in(db.at[pj(j)], dsem.at[pj(j)])
    loads[10].wait()
    cut = span // krows

    def project(i, carry):
        for h in range(heads):
            low = wb[h, :cut].reshape(span, 3 * kd)
            high = wb[h, cut:].reshape(span, 3 * kd)
            proj[h, pl.ds(pl.multiple_of(i * rows, rows), rows), :] = (
                jnp.dot(hb[i, 0], low, preferred_element_type=jnp.float32)
                + jnp.dot(hb[i, 1], high, preferred_element_type=jnp.float32)
            ).astype(jnp.bfloat16)
        return carry

    lax.fori_loop(0, group, project, 0)

    block = 2 * HG_BLOCK
    row_id = lax.broadcasted_iota(jnp.int32, (block, block), 0)
    col_id = lax.broadcasted_iota(jnp.int32, (block, block), 1)
    lower_mask = row_id >= col_id
    tri = jnp.where(lower_mask, 1.0, 0.0).astype(jnp.bfloat16)
    ones = jnp.ones((block, block), jnp.bfloat16)
    per_row = rows // block

    def three(values):
        high = values.astype(jnp.bfloat16)
        rest = values - high.astype(jnp.float32)
        mid = rest.astype(jnp.bfloat16)
        low = (rest - mid.astype(jnp.float32)).astype(jnp.bfloat16)
        return high, mid, low

    def rec_step(c, carry):
        out = []
        here = pl.ds(pl.multiple_of(c * block, block), block)
        for h in range(heads):
            state, prefix = carry[2 * h], carry[2 * h + 1]
            gap = gap_ref[:, pl.ds(pl.multiple_of((p * heads + h) * kd, kd), kd)]
            queries = proj[h, here, :kd].astype(jnp.float32)
            closing = jax.nn.sigmoid(-proj[h, here, kd : 2 * kd].astype(jnp.float32))
            values = proj[h, here, 2 * kd :]
            keys = gap * closing
            logs = jnp.log1p(-keys)
            extra = db[c // per_row, h, c % per_row]
            parts = three(logs)
            extras = [
                jnp.where(lower_mask, e.astype(jnp.float32), 0.0).astype(jnp.bfloat16)
                for e in three(extra)
            ]
            cumulative = jnp.dot(
                jnp.concatenate([tri, tri, tri] + extras, axis=1),
                jnp.concatenate(list(parts) + [ones, ones, ones], axis=0),
                preferred_element_type=jnp.float32,
            )
            last = cumulative[block - 1 : block, :]
            centre = cumulative[block // 2 - 1 : block // 2, :]
            q_mid = queries * jnp.exp(cumulative - centre)
            k_mid = keys * jnp.exp(centre - cumulative)
            scores = jnp.where(
                lower_mask, dot_t(q_mid.astype(jnp.bfloat16), k_mid.astype(jnp.bfloat16), 1, 1), 0.0
            ).astype(jnp.bfloat16)
            q_in = queries * jnp.exp(cumulative)
            raw_ref[h, here, :] = dot_t(scores, values, 1, 0) + dot_t(
                q_in.astype(jnp.bfloat16), state.astype(jnp.bfloat16), 1, 1
            )
            qdec[h, here, :] = (q_in * jnp.exp(prefix)).astype(jnp.bfloat16)
            k_last = (keys * jnp.exp(last - cumulative)).astype(jnp.bfloat16)
            out.append(jnp.exp(last) * state + dot_t(values, k_last, 0, 0))
            out.append(prefix + last)
        return tuple(out)

    start = []
    for h in range(heads):
        start.append(jnp.zeros((HG_VDIM, kd), jnp.float32))
        start.append(jnp.zeros((1, kd), jnp.float32))
    ends = lax.fori_loop(0, group * per_row, rec_step, tuple(start))
    for h in range(heads):
        ssend[h] = ends[2 * h].astype(jnp.bfloat16)
        sdsend[h] = jnp.exp(ends[2 * h + 1])

    def state_up(k):
        return (
            remote(ssend, sbuf.at[z], stsend_sem.at[0, k], stsem.at[0, z], up(k)),
            remote(sdsend, sdbuf.at[z], stsend_sem.at[1, k], stsem.at[1, z], up(k)),
        )

    for k in range(1, depth):

        @pl.when(z + k < depth)
        def _(k=k):
            for copy in state_up(k):
                copy.start()

    sin_state[...] = jnp.zeros(sin_state.shape, jnp.float32)
    for place in range(depth - 1):

        @pl.when(place < z)
        def _(place=place):
            wait_in(sbuf.at[place], stsem.at[0, place])
            wait_in(sdbuf.at[place], stsem.at[1, place])
            for h in range(heads):
                sin_state[h] = sdbuf[place, h] * sin_state[h] + sbuf[place, h].astype(jnp.float32)

    gain = gain_ref[...]

    def finish(i, carry):
        for h in range(heads):
            state = sin_state[h].astype(jnp.bfloat16)
            here = pl.ds(pl.multiple_of(i * rows, rows), rows)
            raw = raw_ref[h, here, :] + dot_t(qdec[h, here, :], state, 1, 1)
            scale = lax.rsqrt(jnp.mean(raw * raw, axis=-1, keepdims=True) + NORM_EPS)
            ro[i, :, h * kd : (h + 1) * kd] = (raw * scale * gain).astype(jnp.bfloat16)
        return carry

    lax.fori_loop(0, group, finish, 0)
    for j in range(1, group):
        launch(
            remote(ro.at[pj(j)], ra.at[p], rsend_sem.at[j], rsem.at[p], z * group + pj(j))
        )
    ra[p] = ro[p]
    loads[8].wait()
    loads[9].wait()
    for j in range(1, group):
        wait_in(ra.at[pj(j)], rsem.at[pj(j)])

    def mix(side, store):
        at = pl.ds(pl.multiple_of(side * half, half), half)
        rec = jnp.concatenate([ra[i, at, :] for i in range(group)], axis=1)
        att = att_ref[:, at]
        wide = wor.shape[1] // 4
        for n in range(4):
            columns = slice(n * wide, (n + 1) * wide)
            store(
                columns,
                jnp.dot(rec, wor[:, columns], preferred_element_type=jnp.float32)
                + dot_t(att, woa[:, columns], 0, 0),
            )

    def store_send(columns, value):
        osend[:, columns] = value.astype(jnp.bfloat16)

    def store_keep(columns, value):
        oacc[:, columns] = value

    mix(other, store_send)
    launch(remote(osend, orecv, osend_sem.at[0], orecv_sem.at[0], sp, other))
    mix(tp, store_keep)
    wait_in(orecv, orecv_sem.at[0])
    out_ref[...] = (oacc[...] + orecv[...].astype(jnp.float32)).astype(jnp.bfloat16)

    for copy in sends:
        copy.wait_send()
    for copy in key_plane(0):
        copy.wait_send()
    for k in range(1, depth):

        @pl.when(z + k < depth)
        def _(k=k):
            key_up(k).wait_send()
            for copy in state_up(k):
                copy.wait_send()

        @pl.when(z >= k)
        def _(k=k):
            for copy in key_plane(k):
                copy.wait_send()

    for g in range(depth):

        @pl.when(z >= g)
        def _(g=g):
            base = ((z + depth - g) % depth) * group
            for j in range(0 if g else 1, group):
                key_core(base + pj(j)).wait_send()


def fast_shards(
    sp_size,
    group,
    hidden_in,
    w_query_rec,
    w_forget,
    w_input,
    forget_gap,
    decay_extra,
    rec_gain,
    w_q_down,
    w_kv_down,
    w_key_rope,
    q_gain,
    kv_gain,
    w_q_nope,
    w_q_rope,
    w_k_up,
    w_v_up,
    w_out_rec,
    w_out_att,
):
    rows, span = hidden_in.shape
    krows, cols = w_query_rec.shape
    all_heads = cols // HG_KDIM
    heads = all_heads // group
    att_heads = w_q_nope.shape[1] // NOPE
    kv_rank = w_k_up.shape[0]
    wide = w_out_rec.shape[1]
    half = rows // 2
    depth = sp_size // group
    block = 2 * HG_BLOCK
    offset = (lax.axis_index("sp") * rows).astype(jnp.float32)
    cosine, sine = rotary_tables(rows, offset, ROPE)
    decay = decay_extra.T.reshape(group, heads, rows // block, 1, block)
    operands = (
        hidden_in,
        w_query_rec,
        w_forget,
        w_input,
        forget_gap.reshape(1, -1),
        decay,
        rec_gain.reshape(1, -1),
        w_q_down,
        w_kv_down,
        w_key_rope.T,
        q_gain.reshape(1, -1),
        kv_gain.reshape(1, -1),
        w_q_nope,
        w_q_rope,
        w_k_up.T,
        w_v_up.T,
        w_out_rec,
        w_out_att,
        cosine.T,
        sine.T,
    )
    far = pl.BlockSpec(memory_space=pl.ANY)
    near = pl.BlockSpec(memory_space=pltpu.VMEM)
    small = (4, 6, 10, 11, 18, 19)
    bf16, f32 = jnp.bfloat16, jnp.float32
    dma = pltpu.SemaphoreType.DMA
    scratch = [
        pltpu.VMEM((group, 2, rows, span), bf16),
        pltpu.VMEM((heads, sp_size, krows, 3 * HG_KDIM), bf16),
        pltpu.VMEM(decay.shape, f32),
        pltpu.VMEM((sp_size, 2, half + ROPE // 2, kv_rank), bf16),
        pltpu.VMEM((2, rows, w_q_down.shape[1] + w_kv_down.shape[1]), bf16),
        pltpu.VMEM(w_q_down.shape, bf16),
        pltpu.VMEM(w_kv_down.shape, bf16),
        pltpu.VMEM(w_key_rope.shape[::-1], bf16),
        pltpu.VMEM(w_q_nope.shape, bf16),
        pltpu.VMEM(w_q_rope.shape, bf16),
        pltpu.VMEM(w_k_up.shape[::-1], bf16),
        pltpu.VMEM(w_v_up.shape[::-1], bf16),
        pltpu.VMEM(w_out_rec.shape, bf16),
        pltpu.VMEM(w_out_att.shape, bf16),
        pltpu.VMEM((rows, w_q_nope.shape[0]), bf16),
        pltpu.VMEM((att_heads, NOPE + ROPE, rows), bf16),
        pltpu.VMEM((att_heads, 1, rows), f32),
        pltpu.VMEM((att_heads, 1, rows), f32),
        pltpu.VMEM((att_heads, MLA_V, rows), f32),
        pltpu.VMEM((att_heads * MLA_V, rows), bf16),
        pltpu.VMEM((heads, group * rows, 3 * HG_KDIM), bf16),
        pltpu.VMEM((heads, group * rows, HG_VDIM), f32),
        pltpu.VMEM((heads, group * rows, HG_KDIM), bf16),
        pltpu.VMEM((heads, HG_VDIM, HG_KDIM), bf16),
        pltpu.VMEM((heads, 1, HG_KDIM), f32),
        pltpu.VMEM((depth, heads, HG_VDIM, HG_KDIM), bf16),
        pltpu.VMEM((depth, heads, 1, HG_KDIM), f32),
        pltpu.VMEM((heads, HG_VDIM, HG_KDIM), f32),
        pltpu.VMEM((group, rows, heads * HG_VDIM), bf16),
        pltpu.VMEM((group, rows, heads * HG_VDIM), bf16),
        pltpu.VMEM((half, wide), bf16),
        pltpu.VMEM((half, wide), bf16),
        pltpu.VMEM((half, wide), f32),
        dma((11,)),
        dma((heads,)),
        dma((heads, group, 3)),
        dma((heads, sp_size)),
        dma((heads, group, 2)),
        dma((heads, group)),
        dma((group, 2, 2)),
        dma((group, 2)),
        dma((group,)),
        dma((group,)),
        dma((group,)),
        dma((group,)),
        dma((1,)),
        dma((1,)),
        dma((depth + 1, max(group, depth))),
        dma((sp_size,)),
        dma((sp_size,)),
        dma((sp_size,)),
        dma((2, depth)),
        dma((2, depth)),
        dma((group,)),
        dma((group,)),
        dma((1,)),
        dma((1,)),
    ]

    def body(*refs):
        fast_kernel(sp_size, group, *refs)

    return pl.pallas_call(
        body,
        in_specs=[near if i in small else far for i in range(len(operands))],
        out_specs=near,
        out_shape=jax.ShapeDtypeStruct((half, wide), bf16),
        scratch_shapes=scratch,
        compiler_params=pltpu.CompilerParams(
            collective_id=0, has_side_effects=True, vmem_limit_bytes=56 * 1024 * 1024
        ),
        name="layer",
    )(*operands)


def solution(mesh):
    placed = (
        P(("zz", "pl"), "tp"),
        P(("zz", "pl"), "tp"),
        P(("zz", "pl"), "tp"),
        P(("zz", "pl"), "tp"),
        P("tp"),
        P(("zz", "pl"), "tp"),
        P(),
        P(None, "tp"),
        P(None, "tp"),
        P(),
        P(),
        P(),
        P(None, "tp"),
        P(None, "tp"),
        P(None, "tp"),
        P(None, "tp"),
        P("tp", None),
        P("tp", None),
    )
    sp_size, tp_size = mesh.shape["sp"], mesh.shape["tp"]

    def run(hidden_in, w_query_rec, *rest):
        heads_dev = w_query_rec.shape[1] // HG_KDIM // tp_size
        if tp_size == 2 and sp_size == 16 and heads_dev % 4 == 0:

            def body(*arrays):
                return fast_shards(sp_size, 4, *arrays)

            flat = [
                P(*("sp" if axis == ("zz", "pl") else axis for axis in spec)) for spec in placed
            ]
            return jax.shard_map(
                body,
                mesh=mesh,
                in_specs=tuple(flat),
                out_specs=P(("sp", "tp"), None),
                check_vma=False,
            )(hidden_in, w_query_rec, *rest)
        group = math.gcd(math.gcd(heads_dev, 4), sp_size)
        split_mesh = Mesh(
            mesh.devices.reshape(sp_size // group, group, tp_size), ("zz", "pl", "tp")
        )
        return jax.shard_map(
            shards,
            mesh=split_mesh,
            in_specs=placed,
            out_specs=P(("zz", "pl", "tp"), None),
            check_vma=False,
        )(hidden_in, w_query_rec, *rest)

    return run
```

```python
import math

import jax
import jax.numpy as jnp
from jax import lax
from jax.experimental import pallas as pl
from jax.experimental.pallas import tpu as pltpu
from jax.sharding import Mesh
from jax.sharding import PartitionSpec as P

HG_KDIM = 128
HG_VDIM = 128
HG_BLOCK = 64
NOPE = 64
ROPE = 32
MLA_V = 64


NORM_EPS = 1e-06
ROPE_BASE = 10000.0
NEG_BIG = -1e30
MESH = pl.DeviceIdType.MESH


def rotate_half(values, cosine, sine_table):
    half_width = values.shape[-1] // 2
    lower_half = values[..., :half_width]
    upper_half = values[..., half_width:]
    return jnp.concatenate(
        [
            lower_half * cosine - upper_half * sine_table,
            lower_half * sine_table + upper_half * cosine,
        ],
        axis=-1,
    )


def rotary_tables(row_count, offset, rot_width):
    positions = jnp.arange(row_count, dtype=jnp.float32) + offset
    frequency = 1.0 / ROPE_BASE ** (jnp.arange(0, rot_width, 2, dtype=jnp.float32) / rot_width)
    angles = positions[:, None] * frequency[None, :]
    return (jnp.cos(angles), jnp.sin(angles))


def dot_t(left, right, left_dim, right_dim):
    return lax.dot_general(
        left, right, (((left_dim,), (right_dim,)), ((), ())), preferred_element_type=jnp.float32
    )


def recurrence_body(rows, q_ref, k_ref, v_ref, lf_ref, s_ref, gain_ref, out_ref, state_ref):
    row_id = lax.broadcasted_iota(jnp.int32, (rows, rows), 0)
    col_id = lax.broadcasted_iota(jnp.int32, (rows, rows), 1)
    lower = row_id >= col_id
    ones = jnp.where(lower, 1.0, 0.0).astype(jnp.float32)
    state = s_ref[0]
    for step in range(k_ref.shape[0] // rows):
        here = pl.ds(step * rows, rows)
        cumulative = jnp.dot(
            ones,
            lf_ref[here, :],
            precision=lax.Precision.HIGHEST,
            preferred_element_type=jnp.float32,
        )
        last = cumulative[rows - 1 : rows, :]
        keys = k_ref[here, :]
        values = v_ref[here, :]
        if out_ref is not None:
            centre = cumulative[rows // 2 - 1 : rows // 2, :]
            queries = q_ref[here, :].astype(jnp.float32)
            q_mid = (queries * jnp.exp(cumulative - centre)).astype(jnp.bfloat16)
            k_mid = (keys * jnp.exp(centre - cumulative)).astype(jnp.bfloat16)
            scores = jnp.where(lower, dot_t(q_mid, k_mid, 1, 1), 0.0).astype(jnp.bfloat16)
            raw = dot_t(scores, values, 1, 0) + dot_t(
                (queries * jnp.exp(cumulative)).astype(jnp.bfloat16),
                state.astype(jnp.bfloat16),
                1,
                1,
            )
            scale = lax.rsqrt(jnp.mean(raw * raw, axis=-1, keepdims=True) + NORM_EPS)
            out_ref[here, :] = (raw * scale * gain_ref[...]).astype(jnp.bfloat16)
        k_last = (keys * jnp.exp(last - cumulative)).astype(jnp.bfloat16)
        state = jnp.exp(last) * state + dot_t(values, k_last, 0, 0)
    if state_ref is not None:
        state_ref[0] = state


def recurrence(queries, keys, values, log_forget, state, gain, emit):
    tokens, width = keys.shape
    heads = width // HG_KDIM
    rows = 2 * HG_BLOCK

    def body(q_ref, k_ref, v_ref, lf_ref, s_ref, gain_ref, out_ref):
        recurrence_body(
            rows,
            q_ref,
            k_ref,
            v_ref,
            lf_ref,
            s_ref,
            gain_ref,
            out_ref if emit else None,
            None if emit else out_ref,
        )

    column = pl.BlockSpec((tokens, HG_KDIM), lambda h: (0, h))
    one_state = pl.BlockSpec((1, HG_VDIM, HG_KDIM), lambda h: (h, 0, 0))
    return pl.pallas_call(
        body,
        grid=(heads,),
        in_specs=[
            column,
            column,
            column,
            column,
            one_state,
            pl.BlockSpec((1, HG_VDIM), lambda h: (0, 0)),
        ],
        out_specs=column if emit else one_state,
        out_shape=jax.ShapeDtypeStruct((tokens, width), jnp.bfloat16)
        if emit
        else jax.ShapeDtypeStruct(state.shape, jnp.float32),
        compiler_params=pltpu.CompilerParams(vmem_limit_bytes=32 * 1024 * 1024),
        cost_estimate=pl.CostEstimate(
            flops=tokens * width * 4000, bytes_accessed=tokens * width * 14, transcendentals=0
        ),
        name="rec_out" if emit else "rec_state",
    )(queries, keys, values, log_forget, state, gain)


def attention_body(
    heads, at_ref, q_ref, lat_ref, rope_ref, wk_ref, wv_ref, out_ref, top_ref, tot_ref, acc_ref
):
    step = pl.program_id(0)
    mine = at_ref[0]

    @pl.when(step == 0)
    def _():
        top_ref[...] = jnp.full(top_ref.shape, NEG_BIG, jnp.float32)
        tot_ref[...] = jnp.zeros(tot_ref.shape, jnp.float32)
        acc_ref[...] = jnp.zeros(acc_ref.shape, jnp.float32)

    def visit(masked):
        latent = lat_ref[...]
        rope = rope_ref[...]
        k_all = dot_t(wk_ref[...], latent, 1, 1).astype(jnp.bfloat16)
        v_all = dot_t(wv_ref[...], latent, 1, 1).astype(jnp.bfloat16)
        for head in range(heads):
            k_head = jnp.concatenate([k_all[head * NOPE : (head + 1) * NOPE], rope], axis=0)
            scores = dot_t(k_head, q_ref[head], 0, 0) * (1.0 / math.sqrt(NOPE + ROPE))
            if masked:
                key_id = lax.broadcasted_iota(jnp.int32, scores.shape, 0)
                query_id = lax.broadcasted_iota(jnp.int32, scores.shape, 1)
                scores = jnp.where(key_id <= query_id, scores, NEG_BIG)
            peak = jnp.max(scores, axis=0, keepdims=True)
            weights = jnp.exp(scores - peak)
            total = jnp.sum(weights, axis=0, keepdims=True)
            part = dot_t(
                v_all[head * MLA_V : (head + 1) * MLA_V], weights.astype(jnp.bfloat16), 1, 0
            )
            before = top_ref[head]
            top = jnp.maximum(before, peak)
            old = jnp.exp(before - top)
            new = jnp.exp(peak - top)
            top_ref[head] = top
            tot_ref[head] = tot_ref[head] * old + total * new
            acc_ref[head] = acc_ref[head] * old + part * new

    @pl.when(step < mine)
    def _():
        visit(False)

    @pl.when(step == mine)
    def _():
        visit(True)
        for head in range(heads):
            out_ref[head * MLA_V : (head + 1) * MLA_V, :] = (
                acc_ref[head] / tot_ref[head]
            ).astype(jnp.bfloat16)


def attention(place, queries, latent, rope, w_key, w_value):
    heads, width, rows = queries.shape
    blocks = latent.shape[0] // rows
    grid_spec = pltpu.PrefetchScalarGridSpec(
        num_scalar_prefetch=1,
        grid=(blocks,),
        in_specs=[
            pl.BlockSpec((heads, width, rows), lambda i, at: (0, 0, 0)),
            pl.BlockSpec((rows, latent.shape[1]), lambda i, at: (jnp.minimum(i, at[0]), 0)),
            pl.BlockSpec((rope.shape[0], rows), lambda i, at: (0, jnp.minimum(i, at[0]))),
            pl.BlockSpec(w_key.shape, lambda i, at: (0, 0)),
            pl.BlockSpec(w_value.shape, lambda i, at: (0, 0)),
        ],
        out_specs=pl.BlockSpec((heads * MLA_V, rows), lambda i, at: (0, 0)),
        scratch_shapes=[
            pltpu.VMEM((heads, 1, rows), jnp.float32),
            pltpu.VMEM((heads, 1, rows), jnp.float32),
            pltpu.VMEM((heads, MLA_V, rows), jnp.float32),
        ],
    )

    def body(*refs):
        attention_body(heads, *refs)

    return pl.pallas_call(
        body,
        grid_spec=grid_spec,
        out_shape=jax.ShapeDtypeStruct((heads * MLA_V, rows), jnp.bfloat16),
        compiler_params=pltpu.CompilerParams(
            dimension_semantics=("arbitrary",), vmem_limit_bytes=32 * 1024 * 1024
        ),
        cost_estimate=pl.CostEstimate(
            flops=blocks * heads * rows * rows * 2000,
            bytes_accessed=latent.size * 2,
            transcendentals=0,
        ),
        name="attend",
    )(place, queries, latent, rope, w_key, w_value)


def both_halves(part, axis):
    if lax.axis_size("tp") != 2:
        return lax.all_gather(part, "tp", axis=axis, tiled=True)
    other = lax.ppermute(part, "tp", [(0, 1), (1, 0)])
    first = lax.axis_index("tp") == 0
    return jnp.concatenate(
        [jnp.where(first, part, other), jnp.where(first, other, part)], axis=axis
    )


def shards(
    hidden_in,
    w_query_rec,
    w_forget,
    w_input,
    forget_gap,
    decay_extra,
    rec_gain,
    w_q_down,
    w_kv_down,
    w_key_rope,
    q_gain,
    kv_gain,
    w_q_nope,
    w_q_rope,
    w_k_up,
    w_v_up,
    w_out_rec,
    w_out_att,
):
    tok_dev = hidden_in.shape[0]
    group = lax.axis_size("pl")
    pl_index = lax.axis_index("pl")
    zz_index = lax.axis_index("zz")
    tp_index = lax.axis_index("tp")
    tp_size = lax.axis_size("tp")
    sp_index = zz_index * group + pl_index

    cols = w_query_rec.shape[1] // group
    heads = cols // HG_KDIM
    depth = w_query_rec.shape[0]
    packed = jnp.concatenate(
        [w.reshape(depth, group, cols) for w in (w_query_rec, w_forget, w_input)], axis=2
    )
    swapped = lax.all_to_all(packed, "pl", split_axis=1, concat_axis=0, tiled=True)
    left_weight = lax.all_gather(
        swapped.reshape(group * depth, 3 * cols), "zz", axis=0, tiled=True
    )
    feature_piece = both_halves(hidden_in, 1)
    member_rows = [feature_piece]
    for gap_to in range(1, group):
        piece = lax.ppermute(hidden_in, "pl", [(i, i ^ gap_to) for i in range(group)])
        member_rows.append(both_halves(piece, 1))
    group_decay = lax.all_gather(decay_extra, "pl", axis=0, tiled=True)
    group_decay = lax.dynamic_slice_in_dim(group_decay, pl_index * heads, heads, 1)

    right_weight = jnp.concatenate([w_q_down, w_kv_down, w_key_rope], axis=1)
    right_sum = jnp.dot(feature_piece, right_weight, preferred_element_type=jnp.float32)
    q_cols = w_q_down.shape[1]
    kv_cols = w_kv_down.shape[1]
    right_round = right_sum[:, : q_cols + kv_cols].astype(jnp.bfloat16)
    both = both_halves(right_round[None], 0).astype(jnp.float32)
    q_latent = jnp.concatenate([both[i, :, :q_cols] for i in range(tp_size)], axis=1)
    kv_latent = jnp.concatenate([both[i, :, q_cols:] for i in range(tp_size)], axis=1)
    q_normed = (
        q_latent
        * lax.rsqrt(jnp.mean(q_latent * q_latent, axis=-1, keepdims=True) + NORM_EPS)
        * q_gain
    ).astype(jnp.bfloat16)
    latent = (
        kv_latent
        * lax.rsqrt(jnp.mean(kv_latent * kv_latent, axis=-1, keepdims=True) + NORM_EPS)
        * kv_gain
    ).astype(jnp.bfloat16)
    q_start = sp_index * tok_dev
    cosine, sine_table = rotary_tables(tok_dev, q_start.astype(jnp.float32), ROPE)
    key_rope = rotate_half(right_sum[:, q_cols + kv_cols :], cosine, sine_table).astype(
        jnp.bfloat16
    )
    group_keys = lax.all_gather(
        jnp.concatenate([latent, key_rope], axis=1), "pl", axis=0, tiled=True
    )
    keys_all = lax.all_gather(group_keys, "zz", axis=0, tiled=True)
    att_heads = w_q_nope.shape[1] // NOPE
    q_nope = jnp.dot(q_normed, w_q_nope, preferred_element_type=jnp.float32).astype(jnp.bfloat16)
    q_rope = jnp.dot(q_normed, w_q_rope, preferred_element_type=jnp.float32).reshape(
        tok_dev, att_heads, ROPE
    )
    q_rope = rotate_half(q_rope, cosine[:, None, :], sine_table[:, None, :]).astype(jnp.bfloat16)
    queries = jnp.concatenate([q_nope.reshape(tok_dev, att_heads, NOPE), q_rope], axis=2)
    att_out = attention(
        sp_index.astype(jnp.int32).reshape(1),
        queries.transpose(1, 2, 0),
        keys_all[:, : latent.shape[1]],
        keys_all[:, latent.shape[1] :].T,
        w_k_up.T,
        w_v_up.T,
    )

    left_weight, att_out = lax.optimization_barrier((left_weight, att_out))
    left_round = jnp.zeros((group * tok_dev, 3 * cols), jnp.bfloat16)
    for gap_to, rows in enumerate(member_rows):
        projected = jnp.dot(rows, left_weight, preferred_element_type=jnp.float32)
        left_round = lax.dynamic_update_slice_in_dim(
            left_round, projected.astype(jnp.bfloat16), (pl_index ^ gap_to) * tok_dev, 0
        )
    rec_query = left_round[:, :cols]
    rec_value = left_round[:, 2 * cols :]
    gap = lax.dynamic_slice_in_dim(forget_gap, pl_index * cols, cols, 0)
    key_in = gap * jax.nn.sigmoid(-left_round[:, cols : 2 * cols].astype(jnp.float32))
    log_forget = jnp.log1p(-key_in) + jnp.repeat(group_decay, HG_KDIM, axis=1)
    gain = rec_gain.reshape(1, HG_VDIM)
    zero_state = jnp.zeros((heads, HG_VDIM, HG_KDIM), jnp.float32)
    local_state = recurrence(rec_query, key_in, rec_value, log_forget, zero_state, gain, False)
    decay = jnp.exp(jnp.sum(log_forget, axis=0)).reshape(heads, 1, HG_KDIM)
    reached = jnp.concatenate([local_state, decay], axis=1)
    zz_size = lax.axis_size("zz")
    into_state = zero_state
    if zz_size <= 4:
        for back in range(zz_size - 1, 0, -1):
            came = lax.ppermute(reached, "zz", [(i, i + back) for i in range(zz_size - back)])
            into_state = came[:, HG_VDIM:] * into_state + came[:, :HG_VDIM]
    else:
        reached = lax.all_gather(reached, "zz", axis=0)
        for place in range(zz_size - 1):
            later = reached[place, :, HG_VDIM:] * into_state + reached[place, :, :HG_VDIM]
            into_state = jnp.where(place < zz_index, later, into_state)
    group_out = recurrence(rec_query, key_in, rec_value, log_forget, into_state, gain, True)
    rec_out = lax.all_to_all(group_out, "pl", split_axis=0, concat_axis=1, tiled=True)

    mixed = jnp.dot(rec_out, w_out_rec, preferred_element_type=jnp.float32) + dot_t(
        att_out, w_out_att, 0, 0
    )
    if tp_size != 2:
        return lax.psum_scatter(
            mixed.astype(jnp.bfloat16), "tp", scatter_dimension=0, tiled=True
        )
    half = tok_dev // 2
    sent = lax.dynamic_slice_in_dim(mixed, (1 - tp_index) * half, half, 0).astype(jnp.bfloat16)
    kept = lax.dynamic_slice_in_dim(mixed, tp_index * half, half, 0)
    came = lax.ppermute(sent, "tp", [(0, 1), (1, 0)])
    return (kept + came.astype(jnp.float32)).astype(jnp.bfloat16)


def fast_kernel(
    sp_size,
    group,
    hid,
    wq,
    wf,
    wi,
    gap_ref,
    dec,
    gain_ref,
    wqd_h,
    wkv_h,
    wkr_h,
    qg_ref,
    kg_ref,
    wqn_h,
    wqr_h,
    wk_h,
    wv_h,
    wor_h,
    woa_h,
    cos_ref,
    sin_ref,
    out_ref,
    hb,
    wb_all,
    wb_gate,
    wb_query,
    db,
    kbuf,
    lbuf,
    wqd,
    wkv,
    wkr,
    wqn,
    wqr,
    wk,
    wv,
    wor,
    woa,
    wkx,
    wvt,
    qn_ref,
    qbuf,
    top_ref,
    tot_ref,
    acc_ref,
    att_ref,
    pacc,
    proj,
    key_ref,
    log_ref,
    kmid,
    gain_state,
    fade,
    state_ref,
    dsrc,
    ssend,
    sdsend,
    sbuf,
    sdbuf,
    sin_state,
    ro,
    ra,
    osend,
    orecv,
    oacc,
    loc_sem,
    wor_sem,
    own_sem,
    wsend_sem,
    wsem,
    zsend_sem,
    fsend_sem,
    hsend_sem,
    hsem,
    hdsend_sem,
    hdsem,
    dsend_sem,
    dsem,
    lsend_sem,
    lsem,
    ksend_sem,
    ksem,
    kdsend_sem,
    kdsem,
    stsend_sem,
    stsem,
    rsend_sem,
    rsem,
    osend_sem,
    orecv_sem,
):
    sp = lax.axis_index("sp")
    tp = lax.axis_index("tp")
    depth = sp_size // group
    z = sp // group
    p = sp % group
    y = p // 2
    x = p % 2
    other = 1 - tp
    rows = hb.shape[2]
    half = rows // 2
    span = hb.shape[3]
    krows = wb_all.shape[1]
    heads = sin_state.shape[0]
    wb = (wb_all, wb_gate, wb_query)
    sources = (wq, wf, wi)
    streams = ((0, (0, 1, 2)), (1, (1, 2)), (1, (0,)))
    att_heads = qbuf.shape[0]
    kd = HG_KDIM
    pad = qbuf.shape[1]


    def pj(j):
        return 2 * ((y + j // 2) % 2) + (x + j) % 2

    toward = 1 - 2 * (z // 2)
    inner = ((z + 1) // 2) % 2
    near = z + toward
    far = z + 2 * toward
    last_from = inner * (z - toward) + (1 - inner) * (z + 3 * toward)

    def column(place):
        return place * group + p

    def up(k):
        return ((z + k) % depth) * group + p

    def remote(src, dst, send, recv, place, side=tp):
        return pltpu.make_async_remote_copy(
            src_ref=src,
            dst_ref=dst,
            send_sem=send,
            recv_sem=recv,
            device_id=(place, side),
            device_id_type=MESH,
        )

    def wait_in(ref, sem):
        pltpu.make_async_copy(ref, ref, sem).wait()

    loads = [
        pltpu.make_async_copy(hid, hb.at[p, tp], loc_sem.at[0]),
        pltpu.make_async_copy(wqd_h, wqd, loc_sem.at[1]),
        pltpu.make_async_copy(wkv_h, wkv, loc_sem.at[2]),
        pltpu.make_async_copy(wkr_h, wkr, loc_sem.at[3]),
        pltpu.make_async_copy(wqn_h, wqn, loc_sem.at[4]),
        pltpu.make_async_copy(wqr_h, wqr, loc_sem.at[5]),
        pltpu.make_async_copy(wk_h, wk, loc_sem.at[6]),
        pltpu.make_async_copy(wv_h, wv, loc_sem.at[7]),
        pltpu.make_async_copy(woa_h, woa, loc_sem.at[8]),
    ]
    loads[0].start()
    for s, (h, kinds) in enumerate(streams):
        for n, kind in enumerate(kinds):
            pltpu.make_async_copy(
                sources[kind].at[:, pl.ds(pl.multiple_of((p * heads + h) * kd, kd), kd)],
                wb[s].at[sp, :, pl.ds(n * kd, kd)],
                own_sem.at[s],
            ).start()
    for load in [loads[i] for i in (1, 2, 3, 6, 7, 4, 5, 8)]:
        load.start()
    for h in range(heads):
        for i in range(group):
            pltpu.make_async_copy(
                wor_h.at[pl.ds((i * heads + h) * kd, kd), :],
                wor.at[h, pl.ds(i * kd, kd), :],
                wor_sem.at[h],
            ).start()

    barrier = pltpu.get_barrier_semaphore()
    partners = [(z * group + pj(j), tp) for j in range(1, group)]
    partners += [(up(k), tp) for k in range(1, depth)]
    partners += [(sp, other)]
    for place in partners:
        pl.semaphore_signal(barrier, inc=1, device_id=place, device_id_type=MESH)
    pl.semaphore_wait(barrier, len(partners))

    sends = []

    def launch(copy):
        copy.start()
        sends.append(copy)

    launch(remote(hid, hb.at[p, tp], hdsend_sem.at[0], hdsem.at[p], sp, other))

    def plane_copies(s):
        h, kinds = streams[s]
        return [
            remote(
                sources[kind].at[:, pl.ds(pl.multiple_of((pj(j) * heads + h) * kd, kd), kd)],
                wb[s].at[sp, :, pl.ds(n * kd, kd)],
                wsend_sem.at[s, j, n],
                wsem.at[s, sp],
                z * group + pj(j),
            )
            for j in range(1, group)
            for n, kind in enumerate(kinds)
        ]

    def plane_weights(s):
        for copy in plane_copies(s):
            launch(copy)

    def weights_in(s, slot):
        wait_in(wb[s].at[slot], wsem.at[s, slot])

    def around(s, j):
        slot = z * group + pj(j)
        if j == 0:
            wait_in(wb[s].at[slot], own_sem.at[s])
        else:
            weights_in(s, slot)
        for copy in around_copies(s, j):
            copy.start()

    def around_copies(s, j):
        slot = z * group + pj(j)
        return [
            remote(
                wb[s].at[slot],
                wb[s].at[slot],
                zsend_sem.at[s, j, i],
                wsem.at[s, slot],
                column(place),
            )
            for i, place in enumerate((inner * (z - toward) + (1 - inner) * far, near))
        ]

    def forward(s, j, k, begin=True):
        slot = (near if k == 0 else far) * group + pj(j)

        @pl.when(inner == 1)
        def _():
            copy = remote(
                wb[s].at[slot],
                wb[s].at[slot],
                fsend_sem.at[s, j, k],
                wsem.at[s, slot],
                column(z - toward),
            )
            if begin:
                weights_in(s, slot)
                copy.start()
            else:
                copy.wait_send()

    plane_weights(0)
    around(0, 0)
    def three(values):
        high = values.astype(jnp.bfloat16)
        rest = values - high.astype(jnp.float32)
        mid = rest.astype(jnp.bfloat16)
        low = (rest - mid.astype(jnp.float32)).astype(jnp.bfloat16)
        return high, mid, low

    turned = dec[...]
    block = 2 * HG_BLOCK
    per_row = rows // block
    for i in range(group):
        for h in range(heads):
            for n in range(per_row):
                row = i * heads + h
                dsrc[i, h, n] = turned[row : row + 1, n * block : (n + 1) * block]
    db[p] = dsrc[p]
    for j in range(1, group):
        launch(
            remote(dsrc.at[pj(j)], db.at[p], dsend_sem.at[j], dsem.at[p], z * group + pj(j))
        )
    loads[6].wait()
    loads[7].wait()
    for head in range(att_heads):
        wkx[:, head * pad : head * pad + NOPE] = wk[
            :, head * NOPE : (head + 1) * NOPE
        ]
        wkx[:, head * pad + NOPE : (head + 1) * pad] = jnp.zeros(
            (wk.shape[0], pad - NOPE), jnp.bfloat16
        )
        qbuf[head, NOPE + ROPE :, :] = jnp.zeros((pad - NOPE - ROPE, rows), jnp.bfloat16)
    wvt[...] = jnp.transpose(wv[...].astype(jnp.float32)).astype(jnp.bfloat16)
    loads[0].wait()
    loads[1].wait()
    loads[2].wait()
    loads[3].wait()
    wait_in(hb.at[p, other], hdsem.at[p])

    def over_features(weight):
        return jnp.dot(
            hb[p, 0], weight[:span, :], preferred_element_type=jnp.float32
        ) + jnp.dot(hb[p, 1], weight[span:, :], preferred_element_type=jnp.float32)

    q_cols = wqd.shape[1]
    kv_cols = wkv.shape[1]
    lbuf[tp, :, :q_cols] = over_features(wqd).astype(jnp.bfloat16)
    lbuf[tp, :, q_cols:] = over_features(wkv).astype(jnp.bfloat16)
    launch(remote(lbuf.at[tp], lbuf.at[tp], lsend_sem.at[0], lsem.at[0], sp, other))
    key_rope = dot_t(wkr[:, :span], hb[p, 0], 1, 1) + dot_t(wkr[:, span:], hb[p, 1], 1, 1)
    cosine = cos_ref[...]
    sine = sin_ref[...]
    kr = ROPE // 2
    first = key_rope[:kr] * cosine - key_rope[kr:] * sine
    second = key_rope[:kr] * sine + key_rope[kr:] * cosine
    kbuf[sp, 0, half:, :] = first.astype(jnp.bfloat16)
    kbuf[sp, 1, half:, :] = second.astype(jnp.bfloat16)
    wait_in(lbuf.at[other], lsem.at[0])
    kv_latent = jnp.concatenate(
        [lbuf[0, :, q_cols:], lbuf[1, :, q_cols:]], axis=1
    ).astype(jnp.float32)
    latent = (
        kv_latent
        * lax.rsqrt(jnp.mean(kv_latent * kv_latent, axis=-1, keepdims=True) + NORM_EPS)
        * kg_ref[...]
    ).astype(jnp.bfloat16)
    kbuf[sp, 0, :half, :] = latent[:half]
    kbuf[sp, 1, :half, :] = latent[half:]

    def key_up(k):
        return remote(
            kbuf.at[sp, tp], kbuf.at[sp, tp], ksend_sem.at[0, k], ksem.at[sp], up(k)
        )

    def key_plane(g):
        block = ((z + depth - g) % depth) * group + p
        return [
            remote(
                kbuf.at[block, tp],
                kbuf.at[block, tp],
                ksend_sem.at[1 + g, j],
                ksem.at[block],
                z * group + pj(j),
            )
            for j in range(1, group)
        ]

    def key_core(block):
        return remote(
            kbuf.at[block, tp],
            kbuf.at[block, tp],
            kdsend_sem.at[block],
            kdsem.at[block],
            sp,
            other,
        )

    for k in range(1, depth):

        @pl.when(z + k < depth)
        def _(k=k):
            key_up(k).start()

    for copy in key_plane(0):
        copy.start()

    plane_weights(1)
    around(0, 1)
    around(0, 2)

    q_latent = jnp.concatenate(
        [lbuf[0, :, :q_cols], lbuf[1, :, :q_cols]], axis=1
    ).astype(jnp.float32)
    qn_ref[...] = (
        q_latent
        * lax.rsqrt(jnp.mean(q_latent * q_latent, axis=-1, keepdims=True) + NORM_EPS)
        * qg_ref[...]
    ).astype(jnp.bfloat16)
    loads[4].wait()
    loads[5].wait()
    q_nope = dot_t(wqn[...], qn_ref[...], 0, 1)
    q_rope = dot_t(wqr[...], qn_ref[...], 0, 1)
    for head in range(att_heads):
        qbuf[head, :NOPE, :] = q_nope[head * NOPE : (head + 1) * NOPE].astype(jnp.bfloat16)
        lower = q_rope[head * ROPE : head * ROPE + kr]
        upper = q_rope[head * ROPE + kr : (head + 1) * ROPE]
        qbuf[head, NOPE : NOPE + kr, :] = (lower * cosine - upper * sine).astype(jnp.bfloat16)
        qbuf[head, NOPE + kr : NOPE + ROPE, :] = (lower * sine + upper * cosine).astype(jnp.bfloat16)
    top_ref[...] = jnp.full(top_ref.shape, NEG_BIG, jnp.float32)
    tot_ref[...] = jnp.zeros(tot_ref.shape, jnp.float32)
    acc_ref[...] = jnp.zeros(acc_ref.shape, jnp.float32)
    around(0, 3)

    def rows_to(j, part, slot):
        at = hb.at[slot, tp, pl.ds(part * half, half), :]
        return remote(
            at, at, hsend_sem.at[j, part, 0 if slot is p else 1], hsem.at[slot, part],
            z * group + pj(j),
        )

    def onward(j, part, to):
        wait_in(hb.at[pj(j), tp, pl.ds(part * half, half), :], hsem.at[pj(j), part])
        return rows_to(to, part, pj(j))

    def across(j, part=None):
        if part is not None:
            rows_in(j, part)
        return remote(
            hb.at[pj(j), tp], hb.at[pj(j), tp], hdsend_sem.at[j], hdsem.at[pj(j)], sp, other
        )

    def rows_in(j, part):
        wait_in(hb.at[pj(j), tp, pl.ds(part * half, half), :], hsem.at[pj(j), part])

    scale = math.log2(math.e) / math.sqrt(NOPE + ROPE)
    lane = lax.broadcasted_iota(jnp.int32, (rows, pad), 1)

    def visit(block, masked):
        latent_all = jnp.concatenate([kbuf[block, 0, :half], kbuf[block, 1, :half]], axis=0)
        rope = jnp.concatenate([kbuf[block, 0, half:], kbuf[block, 1, half:]], axis=0)
        v_all = dot_t(wvt[...], latent_all, 1, 1).astype(jnp.bfloat16)
        rope_wide = jnp.transpose(
            jnp.concatenate(
                [
                    jnp.zeros((NOPE, rows), jnp.float32),
                    rope.astype(jnp.float32),
                    jnp.zeros((pad - NOPE - ROPE, rows), jnp.float32),
                ],
                axis=0,
            )
        ).astype(jnp.bfloat16)
        pairs = {}

        def scored(head):
            pair = head // 2
            if pair not in pairs:
                pairs[pair] = jnp.dot(
                    latent_all,
                    wkx[:, pair * 2 * pad : (pair + 1) * 2 * pad],
                    preferred_element_type=jnp.float32,
                ).astype(jnp.bfloat16)
            nope = pairs[pair][:, (head % 2) * pad : (head % 2 + 1) * pad]
            keys = jnp.where(lane < NOPE, nope, rope_wide)
            scores = jnp.dot(keys, qbuf[head], preferred_element_type=jnp.float32)
            if masked:
                key_id = lax.broadcasted_iota(jnp.int32, scores.shape, 0)
                query_id = lax.broadcasted_iota(jnp.int32, scores.shape, 1)
                scores = jnp.where(key_id <= query_id, scores, NEG_BIG)
            return scores

        ahead = [scored(0), scored(1)]
        for head in range(att_heads):
            if head + 2 < att_heads:
                ahead.append(scored(head + 2))
            scores = ahead[head]
            before = top_ref[head]
            top = jnp.maximum(before, jnp.max(scores, axis=0, keepdims=True))
            weights = jnp.exp2(scores * scale - top * scale)
            old = jnp.exp2((before - top) * scale)
            top_ref[head] = top
            tot_ref[head] = tot_ref[head] * old + jnp.sum(weights, axis=0, keepdims=True)
            acc_ref[head] = acc_ref[head] * old + dot_t(
                v_all[head * MLA_V : (head + 1) * MLA_V], weights.astype(jnp.bfloat16), 1, 0
            )

    def block_at(i):
        return ((z + depth - i // group) % depth) * group + pj(i % group)

    def fetch(i):
        wait_in(kbuf.at[block_at(i), tp], ksem.at[block_at(i)])
        key_core(block_at(i)).start()

    count = (z + 1) * group
    fetch(1)
    visit(sp, True)
    around(1, 0)
    around(1, 1)
    around(1, 2)

    def act(copy):
        copy.start()

    def column_keys(g):
        @pl.when(z >= g)
        def _():
            at = ((z + depth - g) % depth) * group + p
            wait_in(kbuf.at[at, tp], ksem.at[at])
            for copy in key_plane(g):
                copy.start()
            key_core(at).start()

    def start_bulk():
        for copy in plane_copies(2) + [
            rows_to(j, part, p) for j, part in ((1, 0), (2, 1), (1, 1), (2, 0))
        ]:
            copy.start()

    def diagonal_rows():
        for part in range(2):
            rows_in(group - 1, part)
        across(group - 1).start()

    def pass_on(h, k):
        return [lambda j=j: forward(h, j, k) for j in range(group)]

    late = {n: [] for n in range(1, sp_size)}
    for n, actions in (
        (2, [lambda g=g: column_keys(g) for g in range(1, depth)]),
        (3, [start_bulk, lambda: around(1, 3), lambda: around(2, 0)]),
        (7, pass_on(0, 0)),
        (9, pass_on(0, 1)),
        (10, [lambda j=j: around(2, j) for j in range(1, group)]),
        (11, [lambda: act(onward(1, 0, 2)), lambda: act(onward(2, 1, 1))]),
        (12, pass_on(1, 0)),
        (13, [lambda: act(across(1, 1)), lambda: act(across(2, 0))]),
        (14, pass_on(1, 1)),
        (15, [diagonal_rows]),
    ):
        late[n] += actions

    def step(i, carry):
        for n, actions in late.items():
            for action in actions:
                pl.when(i == n)(action)

        @pl.when(((i + 1) % group != 0) & (i + 1 < count))
        def _():
            fetch(i + 1)

        @pl.when(i < count)
        def _():
            wait_in(kbuf.at[block_at(i), other], kdsem.at[block_at(i)])

            @pl.when(block_at(i) < sp)
            def _():
                visit(block_at(i), False)

        return carry

    lax.fori_loop(1, sp_size, step, 0)
    for head in range(att_heads):
        att_ref[head * MLA_V : (head + 1) * MLA_V, :] = (acc_ref[head] / tot_ref[head]).astype(
            jnp.bfloat16
        )
    slab = group * krows
    place_count = span // slab

    def weights_of(s, place):
        return wb[s][pl.ds(place * group, group)].reshape(slab, wb[s].shape[2])

    def features(i, place):
        columns = pl.ds(pl.multiple_of((place % place_count) * slab, slab), slab)
        return hb[i, place // place_count, :, columns]

    def rows_of(i):
        return pl.ds(pl.multiple_of(i * rows, rows), rows)

    def project_part(s):
        @pl.when(inner == 0)
        def _():
            for j in range(group):
                for place in (near, far):
                    weights_in(s, place * group + pj(j))

        def one(j, carry):
            i = pj(j)
            if s == 0:

                @pl.when(j > 0)
                def _():
                    wait_in(hb.at[i, other], hdsem.at[i])
                    wait_in(db.at[i], dsem.at[i])

            pacc[rows_of(i), : wb[s].shape[2]] = sum(
                jnp.dot(
                    features(i, place), weights_of(s, place), preferred_element_type=jnp.float32
                )
                for place in (z, near, far)
            )
            return carry

        lax.fori_loop(0, group, one, 0)

    def project_last(s):
        h, kinds = streams[s]
        for j in range(group):
            weights_in(s, last_from * group + pj(j))

        def one(i, carry):
            here = rows_of(i)
            both = (
                pacc[here, : wb[s].shape[2]]
                + jnp.dot(
                    features(i, last_from),
                    weights_of(s, last_from),
                    preferred_element_type=jnp.float32,
                )
            ).astype(jnp.bfloat16)
            for n, kind in enumerate(kinds):
                piece = both[:, n * kd : (n + 1) * kd]
                if kind == 1:
                    gap = gap_ref[:, pl.ds(pl.multiple_of((p * heads + h) * kd, kd), kd)]
                    keys = gap * jax.nn.sigmoid(-piece.astype(jnp.float32))
                    key_ref[h, here, :] = keys
                    log_ref[h, here, :] = jnp.log1p(-keys)
                else:
                    proj[h, kind // 2, here, :] = piece
            return carry

        lax.fori_loop(0, group, one, 0)

    row_id = lax.broadcasted_iota(jnp.int32, (block, block), 0)
    col_id = lax.broadcasted_iota(jnp.int32, (block, block), 1)
    lower_mask = row_id >= col_id
    tri = jnp.where(lower_mask, 1.0, 0.0).astype(jnp.bfloat16)
    ones = jnp.ones((block, block), jnp.bfloat16)
    steps = group * per_row

    def chunk(c):
        return pl.ds(pl.multiple_of(c * block, block), block)

    def keys_pass(h):
        def one(c, carry):
            here = chunk(c)
            keys = key_ref[h, here, :]
            extras = [
                jnp.where(lower_mask, e.astype(jnp.float32), 0.0).astype(jnp.bfloat16)
                for e in three(db[c // per_row, h, c % per_row])
            ]
            cumulative = jnp.dot(
                jnp.concatenate([tri, tri, tri] + extras, axis=1),
                jnp.concatenate(list(three(log_ref[h, here, :])) + [ones, ones, ones], axis=0),
                preferred_element_type=jnp.float32,
            )
            last = cumulative[block - 1 : block, :]
            centre = cumulative[block // 2 - 1 : block // 2, :]
            log_ref[h, here, :] = cumulative
            kmid[h, here, :] = (keys * jnp.exp(centre - cumulative)).astype(jnp.bfloat16)
            k_last = (keys * jnp.exp(last - cumulative)).astype(jnp.bfloat16)
            gain_state[h, c] = dot_t(proj[h, 1, here, :], k_last, 0, 0)
            fade[h, c] = jnp.exp(last)
            return carry

        lax.fori_loop(0, steps, one, 0, unroll=4)
        state = gain_state[h, 0]
        whole = fade[h, 0]
        for c in range(1, steps):
            state = fade[h, c] * state + gain_state[h, c]
            whole = whole * fade[h, c]
        ssend[h] = state.astype(jnp.bfloat16)
        sdsend[h] = whole

    def state_up(h, k):
        return (
            remote(
                ssend.at[h], sbuf.at[z, h], stsend_sem.at[0, h, k], stsem.at[0, h, z], up(k)
            ),
            remote(
                sdsend.at[h], sdbuf.at[z, h], stsend_sem.at[1, h, k], stsem.at[1, h, z], up(k)
            ),
        )

    def send_state(h):
        for k in range(1, depth):

            @pl.when(z + k < depth)
            def _(k=k):
                for copy in state_up(h, k):
                    copy.start()

    def take_state(h):
        sin_state[h] = jnp.zeros(sin_state.shape[1:], jnp.float32)
        for place in range(depth - 1):

            @pl.when(place < z)
            def _(place=place):
                wait_in(sbuf.at[place, h], stsem.at[0, h, place])
                wait_in(sdbuf.at[place, h], stsem.at[1, h, place])
                sin_state[h] = sdbuf[place, h] * sin_state[h] + sbuf[place, h].astype(jnp.float32)

    gain = gain_ref[...]

    def carry_states(h):
        state = sin_state[h]
        for c in range(steps):
            state_ref[h, c] = state.astype(jnp.bfloat16)
            state = fade[h, c] * state + gain_state[h, c]

    def query_pass(h):
        for j in range(group - 1, -1, -1):
            i = pj(j)
            for n in range(per_row):
                c = i * per_row + n
                here = chunk(c)
                queries = proj[h, 0, here, :].astype(jnp.float32)
                cumulative = log_ref[h, here, :]
                centre = cumulative[block // 2 - 1 : block // 2, :]
                q_mid = (queries * jnp.exp(cumulative - centre)).astype(jnp.bfloat16)
                q_in = (queries * jnp.exp(cumulative)).astype(jnp.bfloat16)
                scores = jnp.where(
                    lower_mask, dot_t(q_mid, kmid[h, here, :], 1, 1), 0.0
                ).astype(jnp.bfloat16)
                raw = dot_t(scores, proj[h, 1, here, :], 1, 0) + dot_t(
                    q_in, state_ref[h, c], 1, 1
                )
                size = lax.rsqrt(jnp.mean(raw * raw, axis=-1, keepdims=True) + NORM_EPS)
                normed = (raw * size * gain).astype(jnp.bfloat16)
                if j:
                    ro[h, i, n * block : (n + 1) * block, :] = normed
                else:
                    ra[h, p, n * block : (n + 1) * block, :] = normed
            if j:
                launch(
                    remote(
                        ro.at[h, i],
                        ra.at[h, p],
                        rsend_sem.at[h, j],
                        rsem.at[h, p],
                        z * group + i,
                    )
                )

    tiles = osend.shape[0]
    wide = osend.shape[2]

    def spot(side):
        return pl.ds(pl.multiple_of(side * half, half), half)

    def tile(n):
        return slice(n * wide, (n + 1) * wide)

    def gathered(h, at):
        return jnp.concatenate([ra[h, i, at, :] for i in range(group)], axis=1)

    project_part(0)
    project_last(0)
    keys_pass(0)
    send_state(0)
    loads[8].wait()
    for n in range(tiles):
        oacc[n] = dot_t(att_ref[...], woa[:, tile(n)], 0, 0)
    for k in range(2):
        for j in range(group):
            forward(2, j, k)
    project_part(1)
    project_last(1)
    keys_pass(1)
    send_state(1)
    take_state(0)
    carry_states(0)
    query_pass(0)
    project_part(2)
    for h in range(heads):
        wait_in(wor.at[h], wor_sem.at[h])
    for j in range(1, group):
        wait_in(ra.at[0, pj(j)], rsem.at[0, pj(j)])
    for n in range(tiles):
        oacc[n] += jnp.dot(
            gathered(0, slice(None)), wor[0, :, tile(n)], preferred_element_type=jnp.float32
        )
    take_state(1)
    carry_states(1)
    project_last(2)
    query_pass(1)
    for j in range(1, group):
        wait_in(ra.at[1, pj(j)], rsem.at[1, pj(j)])

    def mix(side, n):
        return oacc[n, spot(side), :] + jnp.dot(
            gathered(1, spot(side)), wor[1, :, tile(n)], preferred_element_type=jnp.float32
        )

    for n in range(tiles):
        osend[n] = mix(other, n).astype(jnp.bfloat16)
        launch(remote(osend.at[n], orecv.at[n], osend_sem.at[n], orecv_sem.at[n], sp, other))
    for n in range(tiles):
        oacc[n, spot(tp), :] = mix(tp, n)
    for n in range(tiles):
        wait_in(orecv.at[n], orecv_sem.at[n])
        out_ref[:, tile(n)] = (
            oacc[n, spot(tp), :] + orecv[n].astype(jnp.float32)
        ).astype(jnp.bfloat16)

    for copy in sends:
        copy.wait_send()
    for s in range(len(streams)):
        for j in range(group):
            for copy in around_copies(s, j):
                copy.wait_send()
            for k in range(2):
                forward(s, j, k, False)
    for copy in plane_copies(2) + [
        rows_to(j, part, p) for j, part in ((1, 0), (2, 1), (1, 1), (2, 0))
    ]:
        copy.wait_send()
    for j, part, to in ((1, 0, 2), (2, 1, 1)):
        rows_to(to, part, pj(j)).wait_send()
    for j in range(1, group):
        across(j).wait_send()
    for copy in key_plane(0):
        copy.wait_send()
    for k in range(1, depth):

        @pl.when(z + k < depth)
        def _(k=k):
            key_up(k).wait_send()
            for h in range(heads):
                for copy in state_up(h, k):
                    copy.wait_send()

        @pl.when(z >= k)
        def _(k=k):
            for copy in key_plane(k):
                copy.wait_send()

    for g in range(depth):

        @pl.when(z >= g)
        def _(g=g):
            base = ((z + depth - g) % depth) * group
            for j in range(0 if g else 1, group):
                key_core(base + pj(j)).wait_send()


def fast_shards(
    sp_size,
    group,
    hidden_in,
    w_query_rec,
    w_forget,
    w_input,
    forget_gap,
    decay_extra,
    rec_gain,
    w_q_down,
    w_kv_down,
    w_key_rope,
    q_gain,
    kv_gain,
    w_q_nope,
    w_q_rope,
    w_k_up,
    w_v_up,
    w_out_rec,
    w_out_att,
):
    rows, span = hidden_in.shape
    krows, cols = w_query_rec.shape
    all_heads = cols // HG_KDIM
    heads = all_heads // group
    att_heads = w_q_nope.shape[1] // NOPE
    kv_rank = w_k_up.shape[0]
    wide = w_out_rec.shape[1]
    half = rows // 2
    depth = sp_size // group
    block = 2 * HG_BLOCK
    pad = 128 * math.ceil((NOPE + ROPE) / 128)
    tiles = 4
    offset = (lax.axis_index("sp") * rows).astype(jnp.float32)
    cosine, sine = rotary_tables(rows, offset, ROPE)
    blocks = (group, heads, rows // block, 1, block)
    operands = (
        hidden_in,
        w_query_rec,
        w_forget,
        w_input,
        forget_gap.reshape(1, -1),
        decay_extra.T,
        rec_gain.reshape(1, -1),
        w_q_down,
        w_kv_down,
        w_key_rope.T,
        q_gain.reshape(1, -1),
        kv_gain.reshape(1, -1),
        w_q_nope,
        w_q_rope,
        w_k_up,
        w_v_up,
        w_out_rec,
        w_out_att,
        cosine.T,
        sine.T,
    )
    far = pl.BlockSpec(memory_space=pl.ANY)
    near = pl.BlockSpec(memory_space=pltpu.VMEM)
    small = (4, 5, 6, 10, 11, 18, 19)
    bf16, f32 = jnp.bfloat16, jnp.float32
    dma = pltpu.SemaphoreType.DMA
    scratch = [
        pltpu.VMEM((group, 2, rows, span), bf16),
        pltpu.VMEM((sp_size, krows, 3 * HG_KDIM), bf16),
        pltpu.VMEM((sp_size, krows, 2 * HG_KDIM), bf16),
        pltpu.VMEM((sp_size, krows, HG_KDIM), bf16),
        pltpu.VMEM(blocks, f32),
        pltpu.VMEM((sp_size, 2, half + ROPE // 2, kv_rank), bf16),
        pltpu.VMEM((2, rows, w_q_down.shape[1] + w_kv_down.shape[1]), bf16),
        pltpu.VMEM(w_q_down.shape, bf16),
        pltpu.VMEM(w_kv_down.shape, bf16),
        pltpu.VMEM(w_key_rope.shape[::-1], bf16),
        pltpu.VMEM(w_q_nope.shape, bf16),
        pltpu.VMEM(w_q_rope.shape, bf16),
        pltpu.VMEM(w_k_up.shape, bf16),
        pltpu.VMEM(w_v_up.shape, bf16),
        pltpu.VMEM((heads, group * HG_VDIM, wide), bf16),
        pltpu.VMEM(w_out_att.shape, bf16),
        pltpu.VMEM((kv_rank, att_heads * pad), bf16),
        pltpu.VMEM(w_v_up.shape[::-1], bf16),
        pltpu.VMEM((rows, w_q_nope.shape[0]), bf16),
        pltpu.VMEM((att_heads, pad, rows), bf16),
        pltpu.VMEM((att_heads, 1, rows), f32),
        pltpu.VMEM((att_heads, 1, rows), f32),
        pltpu.VMEM((att_heads, MLA_V, rows), f32),
        pltpu.VMEM((att_heads * MLA_V, rows), bf16),
        pltpu.VMEM((group * rows, 3 * HG_KDIM), f32),
        pltpu.VMEM((heads, 2, group * rows, HG_KDIM), bf16),
        pltpu.VMEM((heads, group * rows, HG_KDIM), f32),
        pltpu.VMEM((heads, group * rows, HG_KDIM), f32),
        pltpu.VMEM((heads, group * rows, HG_KDIM), bf16),
        pltpu.VMEM((heads, group * rows // block, HG_VDIM, HG_KDIM), f32),
        pltpu.VMEM((heads, group * rows // block, 1, HG_KDIM), f32),
        pltpu.VMEM((heads, group * rows // block, HG_VDIM, HG_KDIM), bf16),
        pltpu.VMEM(blocks, f32),
        pltpu.VMEM((heads, HG_VDIM, HG_KDIM), bf16),
        pltpu.VMEM((heads, 1, HG_KDIM), f32),
        pltpu.VMEM((depth, heads, HG_VDIM, HG_KDIM), bf16),
        pltpu.VMEM((depth, heads, 1, HG_KDIM), f32),
        pltpu.VMEM((heads, HG_VDIM, HG_KDIM), f32),
        pltpu.VMEM((heads, group, rows, HG_VDIM), bf16),
        pltpu.VMEM((heads, group, rows, HG_VDIM), bf16),
        pltpu.VMEM((tiles, half, wide // tiles), bf16),
        pltpu.VMEM((tiles, half, wide // tiles), bf16),
        pltpu.VMEM((tiles, rows, wide // tiles), f32),
        dma((9,)),
        dma((heads,)),
        dma((3,)),
        dma((3, group, 3)),
        dma((3, sp_size)),
        dma((3, group, 2)),
        dma((3, group, 2)),
        dma((group, 2, 2)),
        dma((group, 2)),
        dma((group,)),
        dma((group,)),
        dma((group,)),
        dma((group,)),
        dma((1,)),
        dma((1,)),
        dma((depth + 1, max(group, depth))),
        dma((sp_size,)),
        dma((sp_size,)),
        dma((sp_size,)),
        dma((2, heads, depth)),
        dma((2, heads, depth)),
        dma((heads, group)),
        dma((heads, group)),
        dma((tiles,)),
        dma((tiles,)),
    ]

    def body(*refs):
        fast_kernel(sp_size, group, *refs)

    return pl.pallas_call(
        body,
        in_specs=[near if i in small else far for i in range(len(operands))],
        out_specs=near,
        out_shape=jax.ShapeDtypeStruct((half, wide), bf16),
        scratch_shapes=scratch,
        compiler_params=pltpu.CompilerParams(
            collective_id=0, has_side_effects=True, vmem_limit_bytes=56 * 1024 * 1024
        ),
        name="layer",
    )(*operands)


def solution(mesh):
    placed = (
        P(("zz", "pl"), "tp"),
        P(("zz", "pl"), "tp"),
        P(("zz", "pl"), "tp"),
        P(("zz", "pl"), "tp"),
        P("tp"),
        P(("zz", "pl"), "tp"),
        P(),
        P(None, "tp"),
        P(None, "tp"),
        P(),
        P(),
        P(),
        P(None, "tp"),
        P(None, "tp"),
        P(None, "tp"),
        P(None, "tp"),
        P("tp", None),
        P("tp", None),
    )
    sp_size, tp_size = mesh.shape["sp"], mesh.shape["tp"]

    def run(hidden_in, w_query_rec, *rest):
        heads_dev = w_query_rec.shape[1] // HG_KDIM // tp_size
        if tp_size == 2 and sp_size == 16 and heads_dev == 8:

            def body(*arrays):
                return fast_shards(sp_size, 4, *arrays)

            flat = [
                P(*("sp" if axis == ("zz", "pl") else axis for axis in spec)) for spec in placed
            ]
            return jax.shard_map(
                body,
                mesh=mesh,
                in_specs=tuple(flat),
                out_specs=P(("sp", "tp"), None),
                check_vma=False,
            )(hidden_in, w_query_rec, *rest)
        group = math.gcd(math.gcd(heads_dev, 4), sp_size)
        split_mesh = Mesh(
            mesh.devices.reshape(sp_size // group, group, tp_size), ("zz", "pl", "tp")
        )
        return jax.shard_map(
            shards,
            mesh=split_mesh,
            in_specs=placed,
            out_specs=P(("zz", "pl", "tp"), None),
            check_vma=False,
        )(hidden_in, w_query_rec, *rest)

    return run
```

```python
import math

import jax
import jax.numpy as jnp
from jax import lax
from jax.experimental import pallas as pl
from jax.experimental.pallas import tpu as pltpu
from jax.sharding import Mesh
from jax.sharding import PartitionSpec as P

HG_KDIM = 128
HG_VDIM = 128
HG_BLOCK = 64
NOPE = 64
ROPE = 32
MLA_V = 64


NORM_EPS = 1e-06
ROPE_BASE = 10000.0
NEG_BIG = -1e30
MESH = pl.DeviceIdType.MESH


def rotate_half(values, cosine, sine_table):
    half_width = values.shape[-1] // 2
    lower_half = values[..., :half_width]
    upper_half = values[..., half_width:]
    return jnp.concatenate(
        [
            lower_half * cosine - upper_half * sine_table,
            lower_half * sine_table + upper_half * cosine,
        ],
        axis=-1,
    )


def rotary_tables(row_count, offset, rot_width):
    positions = jnp.arange(row_count, dtype=jnp.float32) + offset
    frequency = 1.0 / ROPE_BASE ** (jnp.arange(0, rot_width, 2, dtype=jnp.float32) / rot_width)
    angles = positions[:, None] * frequency[None, :]
    return (jnp.cos(angles), jnp.sin(angles))


def dot_t(left, right, left_dim, right_dim):
    return lax.dot_general(
        left, right, (((left_dim,), (right_dim,)), ((), ())), preferred_element_type=jnp.float32
    )


def recurrence_body(rows, q_ref, k_ref, v_ref, lf_ref, s_ref, gain_ref, out_ref, state_ref):
    row_id = lax.broadcasted_iota(jnp.int32, (rows, rows), 0)
    col_id = lax.broadcasted_iota(jnp.int32, (rows, rows), 1)
    lower = row_id >= col_id
    ones = jnp.where(lower, 1.0, 0.0).astype(jnp.float32)
    state = s_ref[0]
    for step in range(k_ref.shape[0] // rows):
        here = pl.ds(step * rows, rows)
        cumulative = jnp.dot(
            ones,
            lf_ref[here, :],
            precision=lax.Precision.HIGHEST,
            preferred_element_type=jnp.float32,
        )
        last = cumulative[rows - 1 : rows, :]
        keys = k_ref[here, :]
        values = v_ref[here, :]
        if out_ref is not None:
            centre = cumulative[rows // 2 - 1 : rows // 2, :]
            queries = q_ref[here, :].astype(jnp.float32)
            q_mid = (queries * jnp.exp(cumulative - centre)).astype(jnp.bfloat16)
            k_mid = (keys * jnp.exp(centre - cumulative)).astype(jnp.bfloat16)
            scores = jnp.where(lower, dot_t(q_mid, k_mid, 1, 1), 0.0).astype(jnp.bfloat16)
            raw = dot_t(scores, values, 1, 0) + dot_t(
                (queries * jnp.exp(cumulative)).astype(jnp.bfloat16),
                state.astype(jnp.bfloat16),
                1,
                1,
            )
            scale = lax.rsqrt(jnp.mean(raw * raw, axis=-1, keepdims=True) + NORM_EPS)
            out_ref[here, :] = (raw * scale * gain_ref[...]).astype(jnp.bfloat16)
        k_last = (keys * jnp.exp(last - cumulative)).astype(jnp.bfloat16)
        state = jnp.exp(last) * state + dot_t(values, k_last, 0, 0)
    if state_ref is not None:
        state_ref[0] = state


def recurrence(queries, keys, values, log_forget, state, gain, emit):
    tokens, width = keys.shape
    heads = width // HG_KDIM
    rows = 2 * HG_BLOCK

    def body(q_ref, k_ref, v_ref, lf_ref, s_ref, gain_ref, out_ref):
        recurrence_body(
            rows,
            q_ref,
            k_ref,
            v_ref,
            lf_ref,
            s_ref,
            gain_ref,
            out_ref if emit else None,
            None if emit else out_ref,
        )

    column = pl.BlockSpec((tokens, HG_KDIM), lambda h: (0, h))
    one_state = pl.BlockSpec((1, HG_VDIM, HG_KDIM), lambda h: (h, 0, 0))
    return pl.pallas_call(
        body,
        grid=(heads,),
        in_specs=[
            column,
            column,
            column,
            column,
            one_state,
            pl.BlockSpec((1, HG_VDIM), lambda h: (0, 0)),
        ],
        out_specs=column if emit else one_state,
        out_shape=jax.ShapeDtypeStruct((tokens, width), jnp.bfloat16)
        if emit
        else jax.ShapeDtypeStruct(state.shape, jnp.float32),
        compiler_params=pltpu.CompilerParams(vmem_limit_bytes=32 * 1024 * 1024),
        cost_estimate=pl.CostEstimate(
            flops=tokens * width * 4000, bytes_accessed=tokens * width * 14, transcendentals=0
        ),
        name="rec_out" if emit else "rec_state",
    )(queries, keys, values, log_forget, state, gain)


def attention_body(
    heads, at_ref, q_ref, lat_ref, rope_ref, wk_ref, wv_ref, out_ref, top_ref, tot_ref, acc_ref
):
    step = pl.program_id(0)
    mine = at_ref[0]

    @pl.when(step == 0)
    def _():
        top_ref[...] = jnp.full(top_ref.shape, NEG_BIG, jnp.float32)
        tot_ref[...] = jnp.zeros(tot_ref.shape, jnp.float32)
        acc_ref[...] = jnp.zeros(acc_ref.shape, jnp.float32)

    def visit(masked):
        latent = lat_ref[...]
        rope = rope_ref[...]
        k_all = dot_t(wk_ref[...], latent, 1, 1).astype(jnp.bfloat16)
        v_all = dot_t(wv_ref[...], latent, 1, 1).astype(jnp.bfloat16)
        for head in range(heads):
            k_head = jnp.concatenate([k_all[head * NOPE : (head + 1) * NOPE], rope], axis=0)
            scores = dot_t(k_head, q_ref[head], 0, 0) * (1.0 / math.sqrt(NOPE + ROPE))
            if masked:
                key_id = lax.broadcasted_iota(jnp.int32, scores.shape, 0)
                query_id = lax.broadcasted_iota(jnp.int32, scores.shape, 1)
                scores = jnp.where(key_id <= query_id, scores, NEG_BIG)
            peak = jnp.max(scores, axis=0, keepdims=True)
            weights = jnp.exp(scores - peak)
            total = jnp.sum(weights, axis=0, keepdims=True)
            part = dot_t(
                v_all[head * MLA_V : (head + 1) * MLA_V], weights.astype(jnp.bfloat16), 1, 0
            )
            before = top_ref[head]
            top = jnp.maximum(before, peak)
            old = jnp.exp(before - top)
            new = jnp.exp(peak - top)
            top_ref[head] = top
            tot_ref[head] = tot_ref[head] * old + total * new
            acc_ref[head] = acc_ref[head] * old + part * new

    @pl.when(step < mine)
    def _():
        visit(False)

    @pl.when(step == mine)
    def _():
        visit(True)
        for head in range(heads):
            out_ref[head * MLA_V : (head + 1) * MLA_V, :] = (
                acc_ref[head] / tot_ref[head]
            ).astype(jnp.bfloat16)


def attention(place, queries, latent, rope, w_key, w_value):
    heads, width, rows = queries.shape
    blocks = latent.shape[0] // rows
    grid_spec = pltpu.PrefetchScalarGridSpec(
        num_scalar_prefetch=1,
        grid=(blocks,),
        in_specs=[
            pl.BlockSpec((heads, width, rows), lambda i, at: (0, 0, 0)),
            pl.BlockSpec((rows, latent.shape[1]), lambda i, at: (jnp.minimum(i, at[0]), 0)),
            pl.BlockSpec((rope.shape[0], rows), lambda i, at: (0, jnp.minimum(i, at[0]))),
            pl.BlockSpec(w_key.shape, lambda i, at: (0, 0)),
            pl.BlockSpec(w_value.shape, lambda i, at: (0, 0)),
        ],
        out_specs=pl.BlockSpec((heads * MLA_V, rows), lambda i, at: (0, 0)),
        scratch_shapes=[
            pltpu.VMEM((heads, 1, rows), jnp.float32),
            pltpu.VMEM((heads, 1, rows), jnp.float32),
            pltpu.VMEM((heads, MLA_V, rows), jnp.float32),
        ],
    )

    def body(*refs):
        attention_body(heads, *refs)

    return pl.pallas_call(
        body,
        grid_spec=grid_spec,
        out_shape=jax.ShapeDtypeStruct((heads * MLA_V, rows), jnp.bfloat16),
        compiler_params=pltpu.CompilerParams(
            dimension_semantics=("arbitrary",), vmem_limit_bytes=32 * 1024 * 1024
        ),
        cost_estimate=pl.CostEstimate(
            flops=blocks * heads * rows * rows * 2000,
            bytes_accessed=latent.size * 2,
            transcendentals=0,
        ),
        name="attend",
    )(place, queries, latent, rope, w_key, w_value)


def both_halves(part, axis):
    if lax.axis_size("tp") != 2:
        return lax.all_gather(part, "tp", axis=axis, tiled=True)
    other = lax.ppermute(part, "tp", [(0, 1), (1, 0)])
    first = lax.axis_index("tp") == 0
    return jnp.concatenate(
        [jnp.where(first, part, other), jnp.where(first, other, part)], axis=axis
    )


def shards(
    hidden_in,
    w_query_rec,
    w_forget,
    w_input,
    forget_gap,
    decay_extra,
    rec_gain,
    w_q_down,
    w_kv_down,
    w_key_rope,
    q_gain,
    kv_gain,
    w_q_nope,
    w_q_rope,
    w_k_up,
    w_v_up,
    w_out_rec,
    w_out_att,
):
    tok_dev = hidden_in.shape[0]
    group = lax.axis_size("pl")
    pl_index = lax.axis_index("pl")
    zz_index = lax.axis_index("zz")
    tp_index = lax.axis_index("tp")
    tp_size = lax.axis_size("tp")
    sp_index = zz_index * group + pl_index

    cols = w_query_rec.shape[1] // group
    heads = cols // HG_KDIM
    depth = w_query_rec.shape[0]
    packed = jnp.concatenate(
        [w.reshape(depth, group, cols) for w in (w_query_rec, w_forget, w_input)], axis=2
    )
    swapped = lax.all_to_all(packed, "pl", split_axis=1, concat_axis=0, tiled=True)
    left_weight = lax.all_gather(
        swapped.reshape(group * depth, 3 * cols), "zz", axis=0, tiled=True
    )
    feature_piece = both_halves(hidden_in, 1)
    member_rows = [feature_piece]
    for gap_to in range(1, group):
        piece = lax.ppermute(hidden_in, "pl", [(i, i ^ gap_to) for i in range(group)])
        member_rows.append(both_halves(piece, 1))
    group_decay = lax.all_gather(decay_extra, "pl", axis=0, tiled=True)
    group_decay = lax.dynamic_slice_in_dim(group_decay, pl_index * heads, heads, 1)

    right_weight = jnp.concatenate([w_q_down, w_kv_down, w_key_rope], axis=1)
    right_sum = jnp.dot(feature_piece, right_weight, preferred_element_type=jnp.float32)
    q_cols = w_q_down.shape[1]
    kv_cols = w_kv_down.shape[1]
    right_round = right_sum[:, : q_cols + kv_cols].astype(jnp.bfloat16)
    both = both_halves(right_round[None], 0).astype(jnp.float32)
    q_latent = jnp.concatenate([both[i, :, :q_cols] for i in range(tp_size)], axis=1)
    kv_latent = jnp.concatenate([both[i, :, q_cols:] for i in range(tp_size)], axis=1)
    q_normed = (
        q_latent
        * lax.rsqrt(jnp.mean(q_latent * q_latent, axis=-1, keepdims=True) + NORM_EPS)
        * q_gain
    ).astype(jnp.bfloat16)
    latent = (
        kv_latent
        * lax.rsqrt(jnp.mean(kv_latent * kv_latent, axis=-1, keepdims=True) + NORM_EPS)
        * kv_gain
    ).astype(jnp.bfloat16)
    q_start = sp_index * tok_dev
    cosine, sine_table = rotary_tables(tok_dev, q_start.astype(jnp.float32), ROPE)
    key_rope = rotate_half(right_sum[:, q_cols + kv_cols :], cosine, sine_table).astype(
        jnp.bfloat16
    )
    group_keys = lax.all_gather(
        jnp.concatenate([latent, key_rope], axis=1), "pl", axis=0, tiled=True
    )
    keys_all = lax.all_gather(group_keys, "zz", axis=0, tiled=True)
    att_heads = w_q_nope.shape[1] // NOPE
    q_nope = jnp.dot(q_normed, w_q_nope, preferred_element_type=jnp.float32).astype(jnp.bfloat16)
    q_rope = jnp.dot(q_normed, w_q_rope, preferred_element_type=jnp.float32).reshape(
        tok_dev, att_heads, ROPE
    )
    q_rope = rotate_half(q_rope, cosine[:, None, :], sine_table[:, None, :]).astype(jnp.bfloat16)
    queries = jnp.concatenate([q_nope.reshape(tok_dev, att_heads, NOPE), q_rope], axis=2)
    att_out = attention(
        sp_index.astype(jnp.int32).reshape(1),
        queries.transpose(1, 2, 0),
        keys_all[:, : latent.shape[1]],
        keys_all[:, latent.shape[1] :].T,
        w_k_up.T,
        w_v_up.T,
    )

    left_weight, att_out = lax.optimization_barrier((left_weight, att_out))
    left_round = jnp.zeros((group * tok_dev, 3 * cols), jnp.bfloat16)
    for gap_to, rows in enumerate(member_rows):
        projected = jnp.dot(rows, left_weight, preferred_element_type=jnp.float32)
        left_round = lax.dynamic_update_slice_in_dim(
            left_round, projected.astype(jnp.bfloat16), (pl_index ^ gap_to) * tok_dev, 0
        )
    rec_query = left_round[:, :cols]
    rec_value = left_round[:, 2 * cols :]
    gap = lax.dynamic_slice_in_dim(forget_gap, pl_index * cols, cols, 0)
    key_in = gap * jax.nn.sigmoid(-left_round[:, cols : 2 * cols].astype(jnp.float32))
    log_forget = jnp.log1p(-key_in) + jnp.repeat(group_decay, HG_KDIM, axis=1)
    gain = rec_gain.reshape(1, HG_VDIM)
    zero_state = jnp.zeros((heads, HG_VDIM, HG_KDIM), jnp.float32)
    local_state = recurrence(rec_query, key_in, rec_value, log_forget, zero_state, gain, False)
    decay = jnp.exp(jnp.sum(log_forget, axis=0)).reshape(heads, 1, HG_KDIM)
    reached = jnp.concatenate([local_state, decay], axis=1)
    zz_size = lax.axis_size("zz")
    into_state = zero_state
    if zz_size <= 4:
        for back in range(zz_size - 1, 0, -1):
            came = lax.ppermute(reached, "zz", [(i, i + back) for i in range(zz_size - back)])
            into_state = came[:, HG_VDIM:] * into_state + came[:, :HG_VDIM]
    else:
        reached = lax.all_gather(reached, "zz", axis=0)
        for place in range(zz_size - 1):
            later = reached[place, :, HG_VDIM:] * into_state + reached[place, :, :HG_VDIM]
            into_state = jnp.where(place < zz_index, later, into_state)
    group_out = recurrence(rec_query, key_in, rec_value, log_forget, into_state, gain, True)
    rec_out = lax.all_to_all(group_out, "pl", split_axis=0, concat_axis=1, tiled=True)

    mixed = jnp.dot(rec_out, w_out_rec, preferred_element_type=jnp.float32) + dot_t(
        att_out, w_out_att, 0, 0
    )
    if tp_size != 2:
        return lax.psum_scatter(
            mixed.astype(jnp.bfloat16), "tp", scatter_dimension=0, tiled=True
        )
    half = tok_dev // 2
    sent = lax.dynamic_slice_in_dim(mixed, (1 - tp_index) * half, half, 0).astype(jnp.bfloat16)
    kept = lax.dynamic_slice_in_dim(mixed, tp_index * half, half, 0)
    came = lax.ppermute(sent, "tp", [(0, 1), (1, 0)])
    return (kept + came.astype(jnp.float32)).astype(jnp.bfloat16)


def fast_kernel(
    sp_size,
    group,
    hid,
    wq,
    wf,
    wi,
    gap_ref,
    dec,
    gain_ref,
    wqd_h,
    wkv_h,
    wkr_h,
    qg_ref,
    kg_ref,
    wqn_h,
    wqr_h,
    wk_h,
    wv_h,
    wor_h,
    woa_h,
    cos_ref,
    sin_ref,
    out_ref,
    hb,
    wb_all,
    wb_gate,
    wb_query,
    db,
    kbuf,
    lbuf,
    wqd,
    wkv,
    wkr,
    wqn,
    wqr,
    wk,
    wv,
    wor,
    woa,
    wkx,
    wvt,
    qn_ref,
    qbuf,
    top_ref,
    tot_ref,
    acc_ref,
    att_ref,
    pacc,
    proj,
    key_ref,
    log_ref,
    kmid,
    gain_state,
    fade,
    state_ref,
    dsrc,
    ssend,
    sbuf,
    sin_state,
    ro,
    ra,
    osend,
    orecv,
    oacc,
    odone,
    loc_sem,
    wor_sem,
    own_sem,
    wsend_sem,
    wsem,
    zsend_sem,
    fsend_sem,
    hsend_sem,
    hsem,
    hdsend_sem,
    hdsem,
    dsend_sem,
    dsem,
    lsend_sem,
    lsem,
    ksend_sem,
    ksem,
    kdsend_sem,
    kdsem,
    stsend_sem,
    stsem,
    rsend_sem,
    rsem,
    osend_sem,
    orecv_sem,
    out_sem,
):
    sp = lax.axis_index("sp")
    tp = lax.axis_index("tp")
    depth = sp_size // group
    z = sp // group
    p = sp % group
    y = p // 2
    x = p % 2
    other = 1 - tp
    rows = hb.shape[2]
    half = rows // 2
    span = hb.shape[3]
    krows = wb_all.shape[1]
    heads = sin_state.shape[0]
    wb = (wb_all, wb_gate, wb_query)
    sources = (wq, wf, wi)
    streams = ((0, (0, 1, 2)), (1, (1, 2)), (1, (0,)))
    att_heads = qbuf.shape[0]
    kd = HG_KDIM
    pad = qbuf.shape[1]


    def pj(j):
        return 2 * ((y + j // 2) % 2) + (x + j) % 2

    toward = 1 - 2 * (z // 2)
    inner = ((z + 1) // 2) % 2
    near = z + toward
    far = z + 2 * toward
    last_from = inner * (z - toward) + (1 - inner) * (z + 3 * toward)

    def column(place):
        return place * group + p

    def up(k):
        return ((z + k) % depth) * group + p

    def remote(src, dst, send, recv, place, side=tp):
        return pltpu.make_async_remote_copy(
            src_ref=src,
            dst_ref=dst,
            send_sem=send,
            recv_sem=recv,
            device_id=(place, side),
            device_id_type=MESH,
        )

    def wait_in(ref, sem):
        pltpu.make_async_copy(ref, ref, sem).wait()

    loads = [
        pltpu.make_async_copy(hid, hb.at[p, tp], loc_sem.at[0]),
        pltpu.make_async_copy(wqd_h, wqd, loc_sem.at[1]),
        pltpu.make_async_copy(wkv_h, wkv, loc_sem.at[2]),
        pltpu.make_async_copy(wkr_h, wkr, loc_sem.at[3]),
        pltpu.make_async_copy(wqn_h, wqn, loc_sem.at[4]),
        pltpu.make_async_copy(wqr_h, wqr, loc_sem.at[5]),
        pltpu.make_async_copy(wk_h, wk, loc_sem.at[6]),
        pltpu.make_async_copy(wv_h, wv, loc_sem.at[7]),
        pltpu.make_async_copy(woa_h, woa, loc_sem.at[8]),
    ]
    loads[0].start()
    for s, (h, kinds) in enumerate(streams):
        for n, kind in enumerate(kinds):
            pltpu.make_async_copy(
                sources[kind].at[:, pl.ds(pl.multiple_of((p * heads + h) * kd, kd), kd)],
                wb[s].at[sp, :, pl.ds(n * kd, kd)],
                own_sem.at[s],
            ).start()
    for load in [loads[i] for i in (1, 2, 3, 6, 7, 4, 5, 8)]:
        load.start()
    for h in range(heads):
        for i in range(group):
            pltpu.make_async_copy(
                wor_h.at[pl.ds((i * heads + h) * kd, kd), :],
                wor.at[h, pl.ds(i * kd, kd), :],
                wor_sem.at[h],
            ).start()

    barrier = pltpu.get_barrier_semaphore()
    partners = [(z * group + pj(j), tp) for j in range(1, group)]
    partners += [(up(k), tp) for k in range(1, depth)]
    partners += [(sp, other)]
    for place in partners:
        pl.semaphore_signal(barrier, inc=1, device_id=place, device_id_type=MESH)
    pl.semaphore_wait(barrier, len(partners))

    def launch(copy):
        copy.start()

    launch(remote(hid, hb.at[p, tp], hdsend_sem.at[0], hdsem.at[p], sp, other))

    def plane_copies(s):
        h, kinds = streams[s]
        return [
            remote(
                sources[kind].at[:, pl.ds(pl.multiple_of((pj(j) * heads + h) * kd, kd), kd)],
                wb[s].at[sp, :, pl.ds(n * kd, kd)],
                wsend_sem.at[s],
                wsem.at[s, sp],
                z * group + pj(j),
            )
            for j in range(1, group)
            for n, kind in enumerate(kinds)
        ]

    def plane_weights(s):
        for copy in plane_copies(s):
            launch(copy)

    def weights_in(s, slot):
        wait_in(wb[s].at[slot], wsem.at[s, slot])

    def around(s, j):
        slot = z * group + pj(j)
        if j == 0:
            wait_in(wb[s].at[slot], own_sem.at[s])
        else:
            weights_in(s, slot)
        for copy in around_copies(s, j):
            copy.start()

    def around_copies(s, j):
        slot = z * group + pj(j)
        return [
            remote(
                wb[s].at[slot],
                wb[s].at[slot],
                zsend_sem.at[s],
                wsem.at[s, slot],
                column(place),
            )
            for place in (inner * (z - toward) + (1 - inner) * far, near)
        ]

    def forward(s, j, k):
        slot = (near if k == 0 else far) * group + pj(j)

        @pl.when(inner == 1)
        def _():
            weights_in(s, slot)
            remote(
                wb[s].at[slot],
                wb[s].at[slot],
                fsend_sem.at[s],
                wsem.at[s, slot],
                column(z - toward),
            ).start()

    plane_weights(0)
    around(0, 0)
    def three(values):
        high = values.astype(jnp.bfloat16)
        rest = values - high.astype(jnp.float32)
        mid = rest.astype(jnp.bfloat16)
        low = (rest - mid.astype(jnp.float32)).astype(jnp.bfloat16)
        return high, mid, low

    turned = dec[...]
    block = 2 * HG_BLOCK
    per_row = rows // block
    for i in range(group):
        for h in range(heads):
            for n in range(per_row):
                row = i * heads + h
                dsrc[i, h, n] = turned[row : row + 1, n * block : (n + 1) * block]
    db[p] = dsrc[p]
    for j in range(1, group):
        launch(
            remote(dsrc.at[pj(j)], db.at[p], dsend_sem.at[0], dsem.at[0], z * group + pj(j))
        )
    loads[6].wait()
    loads[7].wait()
    for head in range(att_heads):
        wkx[:, head * pad : head * pad + NOPE] = wk[
            :, head * NOPE : (head + 1) * NOPE
        ]
        wkx[:, head * pad + NOPE : (head + 1) * pad] = jnp.zeros(
            (wk.shape[0], pad - NOPE), jnp.bfloat16
        )
        qbuf[head, NOPE + ROPE :, :] = jnp.zeros((pad - NOPE - ROPE, rows), jnp.bfloat16)
    wvt[...] = jnp.transpose(wv[...].astype(jnp.float32)).astype(jnp.bfloat16)
    loads[0].wait()
    loads[1].wait()
    loads[2].wait()
    loads[3].wait()
    wait_in(hb.at[p, other], hdsem.at[p])

    def over_features(weight):
        return jnp.dot(
            hb[p, 0], weight[:span, :], preferred_element_type=jnp.float32
        ) + jnp.dot(hb[p, 1], weight[span:, :], preferred_element_type=jnp.float32)

    q_cols = wqd.shape[1]
    kv_cols = wkv.shape[1]
    lbuf[tp, :, :q_cols] = over_features(wqd).astype(jnp.bfloat16)
    lbuf[tp, :, q_cols:] = over_features(wkv).astype(jnp.bfloat16)
    launch(remote(lbuf.at[tp], lbuf.at[tp], lsend_sem.at[0], lsem.at[0], sp, other))
    key_rope = dot_t(wkr[:, :span], hb[p, 0], 1, 1) + dot_t(wkr[:, span:], hb[p, 1], 1, 1)
    cosine = cos_ref[...]
    sine = sin_ref[...]
    kr = ROPE // 2
    first = key_rope[:kr] * cosine - key_rope[kr:] * sine
    second = key_rope[:kr] * sine + key_rope[kr:] * cosine
    kbuf[sp, 0, half:, :] = first.astype(jnp.bfloat16)
    kbuf[sp, 1, half:, :] = second.astype(jnp.bfloat16)
    wait_in(lbuf.at[other], lsem.at[0])
    kv_latent = jnp.concatenate(
        [lbuf[0, :, q_cols:], lbuf[1, :, q_cols:]], axis=1
    ).astype(jnp.float32)
    latent = (
        kv_latent
        * lax.rsqrt(jnp.mean(kv_latent * kv_latent, axis=-1, keepdims=True) + NORM_EPS)
        * kg_ref[...]
    ).astype(jnp.bfloat16)
    kbuf[sp, 0, :half, :] = latent[:half]
    kbuf[sp, 1, :half, :] = latent[half:]

    def key_up(k):
        return remote(
            kbuf.at[sp, tp], kbuf.at[sp, tp], ksend_sem.at[depth + k - 1], ksem.at[sp], up(k)
        )

    def key_plane(g):
        block = ((z + depth - g) % depth) * group + p
        return [
            remote(
                kbuf.at[block, tp],
                kbuf.at[block, tp],
                ksend_sem.at[g],
                ksem.at[block],
                z * group + pj(j),
            )
            for j in range(1, group)
        ]

    def key_core(block, g):
        return remote(
            kbuf.at[block, tp],
            kbuf.at[block, tp],
            kdsend_sem.at[g],
            kdsem.at[block],
            sp,
            other,
        )

    for k in range(1, depth):

        @pl.when(z + k < depth)
        def _(k=k):
            key_up(k).start()

    for copy in key_plane(0):
        copy.start()

    plane_weights(1)
    around(0, 1)
    around(0, 2)

    q_latent = jnp.concatenate(
        [lbuf[0, :, :q_cols], lbuf[1, :, :q_cols]], axis=1
    ).astype(jnp.float32)
    qn_ref[...] = (
        q_latent
        * lax.rsqrt(jnp.mean(q_latent * q_latent, axis=-1, keepdims=True) + NORM_EPS)
        * qg_ref[...]
    ).astype(jnp.bfloat16)
    loads[4].wait()
    loads[5].wait()
    q_nope = dot_t(wqn[...], qn_ref[...], 0, 1)
    q_rope = dot_t(wqr[...], qn_ref[...], 0, 1)
    for head in range(att_heads):
        qbuf[head, :NOPE, :] = q_nope[head * NOPE : (head + 1) * NOPE].astype(jnp.bfloat16)
        lower = q_rope[head * ROPE : head * ROPE + kr]
        upper = q_rope[head * ROPE + kr : (head + 1) * ROPE]
        qbuf[head, NOPE : NOPE + kr, :] = (lower * cosine - upper * sine).astype(jnp.bfloat16)
        qbuf[head, NOPE + kr : NOPE + ROPE, :] = (lower * sine + upper * cosine).astype(jnp.bfloat16)
    top_ref[...] = jnp.full(top_ref.shape, NEG_BIG, jnp.float32)
    tot_ref[...] = jnp.zeros(tot_ref.shape, jnp.float32)
    acc_ref[...] = jnp.zeros(acc_ref.shape, jnp.float32)
    around(0, 3)

    def rows_to(j, part, slot):
        at = hb.at[slot, tp, pl.ds(part * half, half), :]
        return remote(
            at, at, hsend_sem.at[0 if slot is p else 1], hsem.at[slot, part],
            z * group + pj(j),
        )

    def onward(j, part, to):
        wait_in(hb.at[pj(j), tp, pl.ds(part * half, half), :], hsem.at[pj(j), part])
        return rows_to(to, part, pj(j))

    def across(j, part=None):
        if part is not None:
            rows_in(j, part)
        return remote(
            hb.at[pj(j), tp], hb.at[pj(j), tp], hdsend_sem.at[0], hdsem.at[pj(j)], sp, other
        )

    def rows_in(j, part):
        wait_in(hb.at[pj(j), tp, pl.ds(part * half, half), :], hsem.at[pj(j), part])

    scale = math.log2(math.e) / math.sqrt(NOPE + ROPE)
    lane = lax.broadcasted_iota(jnp.int32, (rows, pad), 1)

    def visit(block, masked):
        latent_all = jnp.concatenate([kbuf[block, 0, :half], kbuf[block, 1, :half]], axis=0)
        rope = jnp.concatenate([kbuf[block, 0, half:], kbuf[block, 1, half:]], axis=0)
        v_all = dot_t(wvt[...], latent_all, 1, 1).astype(jnp.bfloat16)
        rope_wide = jnp.transpose(
            jnp.concatenate(
                [
                    jnp.zeros((NOPE, rows), jnp.float32),
                    rope.astype(jnp.float32),
                    jnp.zeros((pad - NOPE - ROPE, rows), jnp.float32),
                ],
                axis=0,
            )
        ).astype(jnp.bfloat16)
        pairs = {}

        def scored(head):
            pair = head // 2
            if pair not in pairs:
                pairs[pair] = jnp.dot(
                    latent_all,
                    wkx[:, pair * 2 * pad : (pair + 1) * 2 * pad],
                    preferred_element_type=jnp.float32,
                ).astype(jnp.bfloat16)
            nope = pairs[pair][:, (head % 2) * pad : (head % 2 + 1) * pad]
            keys = jnp.where(lane < NOPE, nope, rope_wide)
            scores = jnp.dot(keys, qbuf[head], preferred_element_type=jnp.float32)
            if masked:
                key_id = lax.broadcasted_iota(jnp.int32, scores.shape, 0)
                query_id = lax.broadcasted_iota(jnp.int32, scores.shape, 1)
                scores = jnp.where(key_id <= query_id, scores, NEG_BIG)
            return scores

        ahead = [scored(0), scored(1)]
        for head in range(att_heads):
            if head + 2 < att_heads:
                ahead.append(scored(head + 2))
            scores = ahead[head]
            before = top_ref[head]
            top = jnp.maximum(before, jnp.max(scores, axis=0, keepdims=True))
            weights = jnp.exp2(scores * scale - top * scale)
            old = jnp.exp2((before - top) * scale)
            top_ref[head] = top
            tot_ref[head] = tot_ref[head] * old + jnp.sum(weights, axis=0, keepdims=True)
            acc_ref[head] = acc_ref[head] * old + dot_t(
                v_all[head * MLA_V : (head + 1) * MLA_V], weights.astype(jnp.bfloat16), 1, 0
            )

    def block_at(i):
        return ((z + depth - i // group) % depth) * group + pj(i % group)

    def fetch(i):
        wait_in(kbuf.at[block_at(i), tp], ksem.at[block_at(i)])
        key_core(block_at(i), i // group).start()

    count = (z + 1) * group
    fetch(1)
    visit(sp, True)
    around(1, 0)
    around(1, 1)
    around(1, 2)

    def act(copy):
        copy.start()

    def column_keys(g):
        @pl.when(z >= g)
        def _():
            at = ((z + depth - g) % depth) * group + p
            wait_in(kbuf.at[at, tp], ksem.at[at])
            for copy in key_plane(g):
                copy.start()
            key_core(at, g).start()

    def start_bulk():
        for copy in plane_copies(2) + [
            rows_to(j, part, p) for j, part in ((1, 0), (2, 1), (1, 1), (2, 0))
        ]:
            copy.start()

    def spread(side, j):
        @pl.when(inner == side)
        def _():
            around(2, j)

    def diagonal_rows():
        for part in range(2):
            rows_in(group - 1, part)
        across(group - 1).start()

    def pass_on(h, k):
        return [lambda j=j: forward(h, j, k) for j in range(group)]

    late = {n: [] for n in range(1, sp_size)}
    for n, actions in (
        (2, [lambda g=g: column_keys(g) for g in range(1, depth)]),
        (3, [start_bulk, lambda: around(1, 3), lambda: around(2, 0)]),
        (7, pass_on(0, 0)),
        (9, pass_on(0, 1)),
        (6, [lambda j=j: spread(1, j) for j in range(1, group)]),
        (10, [lambda j=j: spread(0, j) for j in range(1, group)]),
        (11, [lambda: act(onward(1, 0, 2)), lambda: act(onward(2, 1, 1))]),
        (12, pass_on(1, 0)),
        (13, [lambda: act(across(1, 1)), lambda: act(across(2, 0))]),
        (15, [diagonal_rows]),
    ):
        late[n] += actions

    def step(i, carry):
        for n, actions in late.items():
            for action in actions:
                pl.when(i == n)(action)

        @pl.when(((i + 1) % group != 0) & (i + 1 < count))
        def _():
            fetch(i + 1)

        @pl.when(i < count)
        def _():
            wait_in(kbuf.at[block_at(i), other], kdsem.at[block_at(i)])

            @pl.when(block_at(i) < sp)
            def _():
                visit(block_at(i), False)

        return carry

    lax.fori_loop(1, sp_size, step, 0)
    for head in range(att_heads):
        att_ref[head * MLA_V : (head + 1) * MLA_V, :] = (acc_ref[head] / tot_ref[head]).astype(
            jnp.bfloat16
        )
    slab = group * krows
    place_count = span // slab

    def weights_of(s, place):
        return wb[s][pl.ds(place * group, group)].reshape(slab, wb[s].shape[2])

    def features(i, place):
        columns = pl.ds(pl.multiple_of((place % place_count) * slab, slab), slab)
        return hb[i, place // place_count, :, columns]

    def rows_of(i):
        return pl.ds(pl.multiple_of(i * rows, rows), rows)

    def early_weights(s):
        @pl.when(inner == 0)
        def _():
            for j in range(group):
                for place in (near, far):
                    weights_in(s, place * group + pj(j))

    def project_part(s):
        early_weights(s)
        if s == 0:
            wait_in(db.at[pl.ds(0, group - 1)], dsem.at[0])

        def one(j, carry):
            i = pj(j)
            if s == 0:

                @pl.when(j > 0)
                def _():
                    wait_in(hb.at[i, other], hdsem.at[i])

            pacc[rows_of(i), : wb[s].shape[2]] = sum(
                jnp.dot(
                    features(i, place), weights_of(s, place), preferred_element_type=jnp.float32
                )
                for place in (z, near, far)
            )
            return carry

        lax.fori_loop(0, group, one, 0)

    def project_last(s):
        h, kinds = streams[s]
        for j in range(group):
            weights_in(s, last_from * group + pj(j))

        def one(i, carry):
            here = rows_of(i)
            both = (
                pacc[here, : wb[s].shape[2]]
                + jnp.dot(
                    features(i, last_from),
                    weights_of(s, last_from),
                    preferred_element_type=jnp.float32,
                )
            ).astype(jnp.bfloat16)
            for n, kind in enumerate(kinds):
                piece = both[:, n * kd : (n + 1) * kd]
                if kind == 1:
                    gap = gap_ref[:, pl.ds(pl.multiple_of((p * heads + h) * kd, kd), kd)]
                    keys = gap * jax.nn.sigmoid(-piece.astype(jnp.float32))
                    key_ref[h, here, :] = keys
                    log_ref[h, here, :] = jnp.log1p(-keys)
                else:
                    proj[h, kind // 2, here, :] = piece
            return carry

        lax.fori_loop(0, group, one, 0)

    row_id = lax.broadcasted_iota(jnp.int32, (block, block), 0)
    col_id = lax.broadcasted_iota(jnp.int32, (block, block), 1)
    lower_mask = row_id >= col_id
    tri = jnp.where(lower_mask, 1.0, 0.0).astype(jnp.bfloat16)
    ones = jnp.ones((block, block), jnp.bfloat16)
    steps = group * per_row

    def chunk(c):
        return pl.ds(pl.multiple_of(c * block, block), block)

    def keys_pass(h):
        def one(c, carry):
            here = chunk(c)
            keys = key_ref[h, here, :]
            extras = [
                jnp.where(lower_mask, e.astype(jnp.float32), 0.0).astype(jnp.bfloat16)
                for e in three(db[c // per_row, h, c % per_row])
            ]
            cumulative = jnp.dot(
                jnp.concatenate([tri, tri, tri] + extras, axis=1),
                jnp.concatenate(list(three(log_ref[h, here, :])) + [ones, ones, ones], axis=0),
                preferred_element_type=jnp.float32,
            )
            last = cumulative[block - 1 : block, :]
            centre = cumulative[block // 2 - 1 : block // 2, :]
            log_ref[h, here, :] = cumulative
            kmid[h, here, :] = (keys * jnp.exp(centre - cumulative)).astype(jnp.bfloat16)
            k_last = (keys * jnp.exp(last - cumulative)).astype(jnp.bfloat16)
            gain_state[h, c] = dot_t(proj[h, 1, here, :], k_last, 0, 0)
            fade[h, c] = jnp.exp(last)
            return carry

        lax.fori_loop(0, steps, one, 0, unroll=4)
        state = gain_state[h, 0]
        whole = fade[h, 0]
        for c in range(1, steps):
            state = fade[h, c] * state + gain_state[h, c]
            whole = whole * fade[h, c]
        ssend[h, :HG_VDIM, :] = state.astype(jnp.bfloat16)
        ssend[h, HG_VDIM:, :] = jnp.concatenate(
            list(three(whole)) + [jnp.zeros((ssend.shape[1] - HG_VDIM - 3, kd), jnp.bfloat16)],
            axis=0,
        )

    def state_up(h, k):
        return remote(
            ssend.at[h], sbuf.at[z, h], stsend_sem.at[h, k - 1], stsem.at[h, z], up(k)
        )

    def send_state(h):
        for k in range(1, depth):

            @pl.when(z + k < depth)
            def _(k=k):
                state_up(h, k).start()

    def take_state(h):
        sin_state[h] = jnp.zeros(sin_state.shape[1:], jnp.float32)
        for place in range(depth - 1):

            @pl.when(place < z)
            def _(place=place):
                wait_in(sbuf.at[place, h], stsem.at[h, place])
                came = sbuf[place, h].astype(jnp.float32)
                whole = sum(came[HG_VDIM + n : HG_VDIM + n + 1] for n in range(3))
                sin_state[h] = whole * sin_state[h] + came[:HG_VDIM]

    gain = gain_ref[...]

    def carry_states(h):
        state = sin_state[h]
        for c in range(steps):
            state_ref[h, c] = state.astype(jnp.bfloat16)
            state = fade[h, c] * state + gain_state[h, c]

    def query_pass(h):
        for j in range(group - 1, -1, -1):
            i = pj(j)
            for n in range(per_row):
                c = i * per_row + n
                here = chunk(c)
                queries = proj[h, 0, here, :].astype(jnp.float32)
                cumulative = log_ref[h, here, :]
                centre = cumulative[block // 2 - 1 : block // 2, :]
                q_mid = (queries * jnp.exp(cumulative - centre)).astype(jnp.bfloat16)
                q_in = (queries * jnp.exp(cumulative)).astype(jnp.bfloat16)
                scores = jnp.where(
                    lower_mask, dot_t(q_mid, kmid[h, here, :], 1, 1), 0.0
                ).astype(jnp.bfloat16)
                raw = dot_t(scores, proj[h, 1, here, :], 1, 0) + dot_t(
                    q_in, state_ref[h, c], 1, 1
                )
                size = lax.rsqrt(jnp.mean(raw * raw, axis=-1, keepdims=True) + NORM_EPS)
                normed = (raw * size * gain).astype(jnp.bfloat16)
                piece = pl.ds(n * block, block)
                if j:
                    ro[h, i, piece, :] = normed
                    launch(
                        remote(
                            ro.at[h, i, piece],
                            ra.at[h, p, piece],
                            rsend_sem.at[h],
                            rsem.at[h],
                            z * group + i,
                        )
                    )
                else:
                    ra[h, p, piece, :] = normed

    tiles = osend.shape[0]
    wide = osend.shape[2]

    def spot(side):
        return pl.ds(pl.multiple_of(side * half, half), half)

    def tile(n):
        return slice(n * wide, (n + 1) * wide)

    def gathered(h, at):
        return jnp.concatenate([ra[h, i, at, :] for i in range(group)], axis=1)

    project_part(0)
    project_last(0)
    keys_pass(0)
    send_state(0)
    loads[8].wait()
    for n in range(tiles):
        oacc[n] = dot_t(att_ref[...], woa[:, tile(n)], 0, 0)
    for j in range(group):
        forward(1, j, 1)

    project_part(1)
    for k in range(2):
        for j in range(group):
            forward(2, j, k)
    take_state(0)
    carry_states(0)
    query_pass(0)
    project_last(1)
    keys_pass(1)
    send_state(1)
    project_part(2)
    take_state(1)
    carry_states(1)
    project_last(2)
    query_pass(1)
    for h in range(heads):
        wait_in(wor.at[h], wor_sem.at[h])
    wait_in(ra.at[0, pl.ds(0, group - 1)], rsem.at[0])
    for n in range(tiles):
        oacc[n] += jnp.dot(
            gathered(0, slice(None)), wor[0, :, tile(n)], preferred_element_type=jnp.float32
        )
    wait_in(ra.at[1, pl.ds(0, group - 1)], rsem.at[1])

    def out_copy(n):
        return pltpu.make_async_copy(odone.at[n], out_ref.at[:, tile(n)], out_sem.at[0])

    def mix(side, n):
        return oacc[n, spot(side), :] + jnp.dot(
            gathered(1, spot(side)), wor[1, :, tile(n)], preferred_element_type=jnp.float32
        )

    for n in range(tiles):
        osend[n] = mix(other, n).astype(jnp.bfloat16)
        launch(remote(osend.at[n], orecv.at[n], osend_sem.at[0], orecv_sem.at[n], sp, other))
    for n in range(tiles):
        oacc[n, spot(tp), :] = mix(tp, n)
    for n in range(tiles):
        wait_in(orecv.at[n], orecv_sem.at[n])
        odone[n] = (oacc[n, spot(tp), :] + orecv[n].astype(jnp.float32)).astype(jnp.bfloat16)
        out_copy(n).start()

    wait_in(odone, out_sem.at[0])
    wait_in(osend, osend_sem.at[0])
    wait_in(hb.at[:, 0], hdsend_sem.at[0])
    wait_in(hb.at[pl.ds(0, 2), 0], hsend_sem.at[0])
    wait_in(hb.at[0, 0], hsend_sem.at[1])
    wait_in(dsrc.at[pl.ds(0, group - 1)], dsend_sem.at[0])
    wait_in(lbuf.at[0], lsend_sem.at[0])
    for s in range(len(streams)):
        wait_in(wb[s].at[pl.ds(0, group - 1)], wsend_sem.at[s])
        wait_in(wb[s].at[pl.ds(0, 2 * group)], zsend_sem.at[s])

    @pl.when(inner == 1)
    def _():
        for s in range(len(streams)):
            wait_in(wb[s].at[pl.ds(0, 2 * group)], fsend_sem.at[s])

    for h in range(heads):
        wait_in(ro.at[h, pl.ds(0, group - 1)], rsend_sem.at[h])
    for k in range(1, depth):

        @pl.when(z + k < depth)
        def _(k=k):
            key_up(k).wait_send()
            for h in range(heads):
                state_up(h, k).wait_send()

    for g in range(depth):

        @pl.when(z >= g)
        def _(g=g):
            wait_in(kbuf.at[pl.ds(0, group - 1), 0], ksend_sem.at[g])
            wait_in(kbuf.at[pl.ds(0, group if g else group - 1), 0], kdsend_sem.at[g])


def fast_shards(
    sp_size,
    group,
    hidden_in,
    w_query_rec,
    w_forget,
    w_input,
    forget_gap,
    decay_extra,
    rec_gain,
    w_q_down,
    w_kv_down,
    w_key_rope,
    q_gain,
    kv_gain,
    w_q_nope,
    w_q_rope,
    w_k_up,
    w_v_up,
    w_out_rec,
    w_out_att,
):
    rows, span = hidden_in.shape
    krows, cols = w_query_rec.shape
    all_heads = cols // HG_KDIM
    heads = all_heads // group
    att_heads = w_q_nope.shape[1] // NOPE
    kv_rank = w_k_up.shape[0]
    wide = w_out_rec.shape[1]
    half = rows // 2
    depth = sp_size // group
    block = 2 * HG_BLOCK
    pad = 128 * math.ceil((NOPE + ROPE) / 128)
    tiles = 4
    offset = (lax.axis_index("sp") * rows).astype(jnp.float32)
    cosine, sine = rotary_tables(rows, offset, ROPE)
    blocks = (group, heads, rows // block, 1, block)
    operands = (
        hidden_in,
        w_query_rec,
        w_forget,
        w_input,
        forget_gap.reshape(1, -1),
        decay_extra.T,
        rec_gain.reshape(1, -1),
        w_q_down,
        w_kv_down,
        w_key_rope.T,
        q_gain.reshape(1, -1),
        kv_gain.reshape(1, -1),
        w_q_nope,
        w_q_rope,
        w_k_up,
        w_v_up,
        w_out_rec,
        w_out_att,
        cosine.T,
        sine.T,
    )
    far = pl.BlockSpec(memory_space=pl.ANY)
    near = pl.BlockSpec(memory_space=pltpu.VMEM)
    small = (4, 5, 6, 10, 11, 18, 19)
    bf16, f32 = jnp.bfloat16, jnp.float32
    dma = pltpu.SemaphoreType.DMA
    scratch = [
        pltpu.VMEM((group, 2, rows, span), bf16),
        pltpu.VMEM((sp_size, krows, 3 * HG_KDIM), bf16),
        pltpu.VMEM((sp_size, krows, 2 * HG_KDIM), bf16),
        pltpu.VMEM((sp_size, krows, HG_KDIM), bf16),
        pltpu.VMEM(blocks, f32),
        pltpu.VMEM((sp_size, 2, half + ROPE // 2, kv_rank), bf16),
        pltpu.VMEM((2, rows, w_q_down.shape[1] + w_kv_down.shape[1]), bf16),
        pltpu.VMEM(w_q_down.shape, bf16),
        pltpu.VMEM(w_kv_down.shape, bf16),
        pltpu.VMEM(w_key_rope.shape[::-1], bf16),
        pltpu.VMEM(w_q_nope.shape, bf16),
        pltpu.VMEM(w_q_rope.shape, bf16),
        pltpu.VMEM(w_k_up.shape, bf16),
        pltpu.VMEM(w_v_up.shape, bf16),
        pltpu.VMEM((heads, group * HG_VDIM, wide), bf16),
        pltpu.VMEM(w_out_att.shape, bf16),
        pltpu.VMEM((kv_rank, att_heads * pad), bf16),
        pltpu.VMEM(w_v_up.shape[::-1], bf16),
        pltpu.VMEM((rows, w_q_nope.shape[0]), bf16),
        pltpu.VMEM((att_heads, pad, rows), bf16),
        pltpu.VMEM((att_heads, 1, rows), f32),
        pltpu.VMEM((att_heads, 1, rows), f32),
        pltpu.VMEM((att_heads, MLA_V, rows), f32),
        pltpu.VMEM((att_heads * MLA_V, rows), bf16),
        pltpu.VMEM((group * rows, 3 * HG_KDIM), f32),
        pltpu.VMEM((heads, 2, group * rows, HG_KDIM), bf16),
        pltpu.VMEM((heads, group * rows, HG_KDIM), f32),
        pltpu.VMEM((heads, group * rows, HG_KDIM), f32),
        pltpu.VMEM((heads, group * rows, HG_KDIM), bf16),
        pltpu.VMEM((heads, group * rows // block, HG_VDIM, HG_KDIM), f32),
        pltpu.VMEM((heads, group * rows // block, 1, HG_KDIM), f32),
        pltpu.VMEM((heads, group * rows // block, HG_VDIM, HG_KDIM), bf16),
        pltpu.VMEM(blocks, f32),
        pltpu.VMEM((heads, HG_VDIM + 16, HG_KDIM), bf16),
        pltpu.VMEM((depth, heads, HG_VDIM + 16, HG_KDIM), bf16),
        pltpu.VMEM((heads, HG_VDIM, HG_KDIM), f32),
        pltpu.VMEM((heads, group, rows, HG_VDIM), bf16),
        pltpu.VMEM((heads, group, rows, HG_VDIM), bf16),
        pltpu.VMEM((tiles, half, wide // tiles), bf16),
        pltpu.VMEM((tiles, half, wide // tiles), bf16),
        pltpu.VMEM((tiles, rows, wide // tiles), f32),
        pltpu.VMEM((tiles, half, wide // tiles), bf16),
        dma((9,)),
        dma((heads,)),
        dma((3,)),
        dma((3,)),
        dma((3, sp_size)),
        dma((3,)),
        dma((3,)),
        dma((2,)),
        dma((group, 2)),
        dma((1,)),
        dma((group,)),
        dma((1,)),
        dma((1,)),
        dma((1,)),
        dma((1,)),
        dma((2 * depth - 1,)),
        dma((sp_size,)),
        dma((depth,)),
        dma((sp_size,)),
        dma((heads, depth - 1)),
        dma((heads, depth - 1)),
        dma((heads,)),
        dma((heads,)),
        dma((1,)),
        dma((tiles,)),
        dma((1,)),
    ]

    def body(*refs):
        fast_kernel(sp_size, group, *refs)

    return pl.pallas_call(
        body,
        in_specs=[near if i in small else far for i in range(len(operands))],
        out_specs=far,
        out_shape=jax.ShapeDtypeStruct((half, wide), bf16),
        scratch_shapes=scratch,
        compiler_params=pltpu.CompilerParams(
            collective_id=0, has_side_effects=True, vmem_limit_bytes=56 * 1024 * 1024
        ),
        name="layer",
    )(*operands)


def solution(mesh):
    placed = (
        P(("zz", "pl"), "tp"),
        P(("zz", "pl"), "tp"),
        P(("zz", "pl"), "tp"),
        P(("zz", "pl"), "tp"),
        P("tp"),
        P(("zz", "pl"), "tp"),
        P(),
        P(None, "tp"),
        P(None, "tp"),
        P(),
        P(),
        P(),
        P(None, "tp"),
        P(None, "tp"),
        P(None, "tp"),
        P(None, "tp"),
        P("tp", None),
        P("tp", None),
    )
    sp_size, tp_size = mesh.shape["sp"], mesh.shape["tp"]

    def run(hidden_in, w_query_rec, *rest):
        heads_dev = w_query_rec.shape[1] // HG_KDIM // tp_size
        if tp_size == 2 and sp_size == 16 and heads_dev == 8:

            def body(*arrays):
                return fast_shards(sp_size, 4, *arrays)

            flat = [
                P(*("sp" if axis == ("zz", "pl") else axis for axis in spec)) for spec in placed
            ]
            return jax.shard_map(
                body,
                mesh=mesh,
                in_specs=tuple(flat),
                out_specs=P(("sp", "tp"), None),
                check_vma=False,
            )(hidden_in, w_query_rec, *rest)
        group = math.gcd(math.gcd(heads_dev, 4), sp_size)
        split_mesh = Mesh(
            mesh.devices.reshape(sp_size // group, group, tp_size), ("zz", "pl", "tp")
        )
        return jax.shard_map(
            shards,
            mesh=split_mesh,
            in_specs=placed,
            out_specs=P(("zz", "pl", "tp"), None),
            check_vma=False,
        )(hidden_in, w_query_rec, *rest)

    return run
```

```python
import math

import jax
import jax.numpy as jnp
from jax import lax
from jax.experimental import pallas as pl
from jax.experimental.pallas import tpu as pltpu
from jax.sharding import Mesh
from jax.sharding import PartitionSpec as P

HG_KDIM = 128
HG_VDIM = 128
HG_BLOCK = 64
NOPE = 64
ROPE = 32
MLA_V = 64


NORM_EPS = 1e-06
ROPE_BASE = 10000.0
NEG_BIG = -1e30
MESH = pl.DeviceIdType.MESH


def rotate_half(values, cosine, sine_table):
    half_width = values.shape[-1] // 2
    lower_half = values[..., :half_width]
    upper_half = values[..., half_width:]
    return jnp.concatenate(
        [
            lower_half * cosine - upper_half * sine_table,
            lower_half * sine_table + upper_half * cosine,
        ],
        axis=-1,
    )


def rotary_tables(row_count, offset, rot_width):
    positions = jnp.arange(row_count, dtype=jnp.float32) + offset
    frequency = 1.0 / ROPE_BASE ** (jnp.arange(0, rot_width, 2, dtype=jnp.float32) / rot_width)
    angles = positions[:, None] * frequency[None, :]
    return (jnp.cos(angles), jnp.sin(angles))


def dot_t(left, right, left_dim, right_dim):
    return lax.dot_general(
        left, right, (((left_dim,), (right_dim,)), ((), ())), preferred_element_type=jnp.float32
    )


def recurrence_body(rows, q_ref, k_ref, v_ref, lf_ref, s_ref, gain_ref, out_ref, state_ref):
    row_id = lax.broadcasted_iota(jnp.int32, (rows, rows), 0)
    col_id = lax.broadcasted_iota(jnp.int32, (rows, rows), 1)
    lower = row_id >= col_id
    ones = jnp.where(lower, 1.0, 0.0).astype(jnp.float32)
    state = s_ref[0]
    for step in range(k_ref.shape[0] // rows):
        here = pl.ds(step * rows, rows)
        cumulative = jnp.dot(
            ones,
            lf_ref[here, :],
            precision=lax.Precision.HIGHEST,
            preferred_element_type=jnp.float32,
        )
        last = cumulative[rows - 1 : rows, :]
        keys = k_ref[here, :]
        values = v_ref[here, :]
        if out_ref is not None:
            centre = cumulative[rows // 2 - 1 : rows // 2, :]
            queries = q_ref[here, :].astype(jnp.float32)
            q_mid = (queries * jnp.exp(cumulative - centre)).astype(jnp.bfloat16)
            k_mid = (keys * jnp.exp(centre - cumulative)).astype(jnp.bfloat16)
            scores = jnp.where(lower, dot_t(q_mid, k_mid, 1, 1), 0.0).astype(jnp.bfloat16)
            raw = dot_t(scores, values, 1, 0) + dot_t(
                (queries * jnp.exp(cumulative)).astype(jnp.bfloat16),
                state.astype(jnp.bfloat16),
                1,
                1,
            )
            scale = lax.rsqrt(jnp.mean(raw * raw, axis=-1, keepdims=True) + NORM_EPS)
            out_ref[here, :] = (raw * scale * gain_ref[...]).astype(jnp.bfloat16)
        k_last = (keys * jnp.exp(last - cumulative)).astype(jnp.bfloat16)
        state = jnp.exp(last) * state + dot_t(values, k_last, 0, 0)
    if state_ref is not None:
        state_ref[0] = state


def recurrence(queries, keys, values, log_forget, state, gain, emit):
    tokens, width = keys.shape
    heads = width // HG_KDIM
    rows = 2 * HG_BLOCK

    def body(q_ref, k_ref, v_ref, lf_ref, s_ref, gain_ref, out_ref):
        recurrence_body(
            rows,
            q_ref,
            k_ref,
            v_ref,
            lf_ref,
            s_ref,
            gain_ref,
            out_ref if emit else None,
            None if emit else out_ref,
        )

    column = pl.BlockSpec((tokens, HG_KDIM), lambda h: (0, h))
    one_state = pl.BlockSpec((1, HG_VDIM, HG_KDIM), lambda h: (h, 0, 0))
    return pl.pallas_call(
        body,
        grid=(heads,),
        in_specs=[
            column,
            column,
            column,
            column,
            one_state,
            pl.BlockSpec((1, HG_VDIM), lambda h: (0, 0)),
        ],
        out_specs=column if emit else one_state,
        out_shape=jax.ShapeDtypeStruct((tokens, width), jnp.bfloat16)
        if emit
        else jax.ShapeDtypeStruct(state.shape, jnp.float32),
        compiler_params=pltpu.CompilerParams(vmem_limit_bytes=32 * 1024 * 1024),
        cost_estimate=pl.CostEstimate(
            flops=tokens * width * 4000, bytes_accessed=tokens * width * 14, transcendentals=0
        ),
        name="rec_out" if emit else "rec_state",
    )(queries, keys, values, log_forget, state, gain)


def attention_body(
    heads, at_ref, q_ref, lat_ref, rope_ref, wk_ref, wv_ref, out_ref, top_ref, tot_ref, acc_ref
):
    step = pl.program_id(0)
    mine = at_ref[0]

    @pl.when(step == 0)
    def _():
        top_ref[...] = jnp.full(top_ref.shape, NEG_BIG, jnp.float32)
        tot_ref[...] = jnp.zeros(tot_ref.shape, jnp.float32)
        acc_ref[...] = jnp.zeros(acc_ref.shape, jnp.float32)

    def visit(masked):
        latent = lat_ref[...]
        rope = rope_ref[...]
        k_all = dot_t(wk_ref[...], latent, 1, 1).astype(jnp.bfloat16)
        v_all = dot_t(wv_ref[...], latent, 1, 1).astype(jnp.bfloat16)
        for head in range(heads):
            k_head = jnp.concatenate([k_all[head * NOPE : (head + 1) * NOPE], rope], axis=0)
            scores = dot_t(k_head, q_ref[head], 0, 0) * (1.0 / math.sqrt(NOPE + ROPE))
            if masked:
                key_id = lax.broadcasted_iota(jnp.int32, scores.shape, 0)
                query_id = lax.broadcasted_iota(jnp.int32, scores.shape, 1)
                scores = jnp.where(key_id <= query_id, scores, NEG_BIG)
            peak = jnp.max(scores, axis=0, keepdims=True)
            weights = jnp.exp(scores - peak)
            total = jnp.sum(weights, axis=0, keepdims=True)
            part = dot_t(
                v_all[head * MLA_V : (head + 1) * MLA_V], weights.astype(jnp.bfloat16), 1, 0
            )
            before = top_ref[head]
            top = jnp.maximum(before, peak)
            old = jnp.exp(before - top)
            new = jnp.exp(peak - top)
            top_ref[head] = top
            tot_ref[head] = tot_ref[head] * old + total * new
            acc_ref[head] = acc_ref[head] * old + part * new

    @pl.when(step < mine)
    def _():
        visit(False)

    @pl.when(step == mine)
    def _():
        visit(True)
        for head in range(heads):
            out_ref[head * MLA_V : (head + 1) * MLA_V, :] = (
                acc_ref[head] / tot_ref[head]
            ).astype(jnp.bfloat16)


def attention(place, queries, latent, rope, w_key, w_value):
    heads, width, rows = queries.shape
    blocks = latent.shape[0] // rows
    grid_spec = pltpu.PrefetchScalarGridSpec(
        num_scalar_prefetch=1,
        grid=(blocks,),
        in_specs=[
            pl.BlockSpec((heads, width, rows), lambda i, at: (0, 0, 0)),
            pl.BlockSpec((rows, latent.shape[1]), lambda i, at: (jnp.minimum(i, at[0]), 0)),
            pl.BlockSpec((rope.shape[0], rows), lambda i, at: (0, jnp.minimum(i, at[0]))),
            pl.BlockSpec(w_key.shape, lambda i, at: (0, 0)),
            pl.BlockSpec(w_value.shape, lambda i, at: (0, 0)),
        ],
        out_specs=pl.BlockSpec((heads * MLA_V, rows), lambda i, at: (0, 0)),
        scratch_shapes=[
            pltpu.VMEM((heads, 1, rows), jnp.float32),
            pltpu.VMEM((heads, 1, rows), jnp.float32),
            pltpu.VMEM((heads, MLA_V, rows), jnp.float32),
        ],
    )

    def body(*refs):
        attention_body(heads, *refs)

    return pl.pallas_call(
        body,
        grid_spec=grid_spec,
        out_shape=jax.ShapeDtypeStruct((heads * MLA_V, rows), jnp.bfloat16),
        compiler_params=pltpu.CompilerParams(
            dimension_semantics=("arbitrary",), vmem_limit_bytes=32 * 1024 * 1024
        ),
        cost_estimate=pl.CostEstimate(
            flops=blocks * heads * rows * rows * 2000,
            bytes_accessed=latent.size * 2,
            transcendentals=0,
        ),
        name="attend",
    )(place, queries, latent, rope, w_key, w_value)


def both_halves(part, axis):
    if lax.axis_size("tp") != 2:
        return lax.all_gather(part, "tp", axis=axis, tiled=True)
    other = lax.ppermute(part, "tp", [(0, 1), (1, 0)])
    first = lax.axis_index("tp") == 0
    return jnp.concatenate(
        [jnp.where(first, part, other), jnp.where(first, other, part)], axis=axis
    )


def shards(
    hidden_in,
    w_query_rec,
    w_forget,
    w_input,
    forget_gap,
    decay_extra,
    rec_gain,
    w_q_down,
    w_kv_down,
    w_key_rope,
    q_gain,
    kv_gain,
    w_q_nope,
    w_q_rope,
    w_k_up,
    w_v_up,
    w_out_rec,
    w_out_att,
):
    tok_dev = hidden_in.shape[0]
    group = lax.axis_size("pl")
    pl_index = lax.axis_index("pl")
    zz_index = lax.axis_index("zz")
    tp_index = lax.axis_index("tp")
    tp_size = lax.axis_size("tp")
    sp_index = zz_index * group + pl_index

    cols = w_query_rec.shape[1] // group
    heads = cols // HG_KDIM
    depth = w_query_rec.shape[0]
    packed = jnp.concatenate(
        [w.reshape(depth, group, cols) for w in (w_query_rec, w_forget, w_input)], axis=2
    )
    swapped = lax.all_to_all(packed, "pl", split_axis=1, concat_axis=0, tiled=True)
    left_weight = lax.all_gather(
        swapped.reshape(group * depth, 3 * cols), "zz", axis=0, tiled=True
    )
    feature_piece = both_halves(hidden_in, 1)
    member_rows = [feature_piece]
    for gap_to in range(1, group):
        piece = lax.ppermute(hidden_in, "pl", [(i, i ^ gap_to) for i in range(group)])
        member_rows.append(both_halves(piece, 1))
    group_decay = lax.all_gather(decay_extra, "pl", axis=0, tiled=True)
    group_decay = lax.dynamic_slice_in_dim(group_decay, pl_index * heads, heads, 1)

    right_weight = jnp.concatenate([w_q_down, w_kv_down, w_key_rope], axis=1)
    right_sum = jnp.dot(feature_piece, right_weight, preferred_element_type=jnp.float32)
    q_cols = w_q_down.shape[1]
    kv_cols = w_kv_down.shape[1]
    right_round = right_sum[:, : q_cols + kv_cols].astype(jnp.bfloat16)
    both = both_halves(right_round[None], 0).astype(jnp.float32)
    q_latent = jnp.concatenate([both[i, :, :q_cols] for i in range(tp_size)], axis=1)
    kv_latent = jnp.concatenate([both[i, :, q_cols:] for i in range(tp_size)], axis=1)
    q_normed = (
        q_latent
        * lax.rsqrt(jnp.mean(q_latent * q_latent, axis=-1, keepdims=True) + NORM_EPS)
        * q_gain
    ).astype(jnp.bfloat16)
    latent = (
        kv_latent
        * lax.rsqrt(jnp.mean(kv_latent * kv_latent, axis=-1, keepdims=True) + NORM_EPS)
        * kv_gain
    ).astype(jnp.bfloat16)
    q_start = sp_index * tok_dev
    cosine, sine_table = rotary_tables(tok_dev, q_start.astype(jnp.float32), ROPE)
    key_rope = rotate_half(right_sum[:, q_cols + kv_cols :], cosine, sine_table).astype(
        jnp.bfloat16
    )
    group_keys = lax.all_gather(
        jnp.concatenate([latent, key_rope], axis=1), "pl", axis=0, tiled=True
    )
    keys_all = lax.all_gather(group_keys, "zz", axis=0, tiled=True)
    att_heads = w_q_nope.shape[1] // NOPE
    q_nope = jnp.dot(q_normed, w_q_nope, preferred_element_type=jnp.float32).astype(jnp.bfloat16)
    q_rope = jnp.dot(q_normed, w_q_rope, preferred_element_type=jnp.float32).reshape(
        tok_dev, att_heads, ROPE
    )
    q_rope = rotate_half(q_rope, cosine[:, None, :], sine_table[:, None, :]).astype(jnp.bfloat16)
    queries = jnp.concatenate([q_nope.reshape(tok_dev, att_heads, NOPE), q_rope], axis=2)
    att_out = attention(
        sp_index.astype(jnp.int32).reshape(1),
        queries.transpose(1, 2, 0),
        keys_all[:, : latent.shape[1]],
        keys_all[:, latent.shape[1] :].T,
        w_k_up.T,
        w_v_up.T,
    )

    left_weight, att_out = lax.optimization_barrier((left_weight, att_out))
    left_round = jnp.zeros((group * tok_dev, 3 * cols), jnp.bfloat16)
    for gap_to, rows in enumerate(member_rows):
        projected = jnp.dot(rows, left_weight, preferred_element_type=jnp.float32)
        left_round = lax.dynamic_update_slice_in_dim(
            left_round, projected.astype(jnp.bfloat16), (pl_index ^ gap_to) * tok_dev, 0
        )
    rec_query = left_round[:, :cols]
    rec_value = left_round[:, 2 * cols :]
    gap = lax.dynamic_slice_in_dim(forget_gap, pl_index * cols, cols, 0)
    key_in = gap * jax.nn.sigmoid(-left_round[:, cols : 2 * cols].astype(jnp.float32))
    log_forget = jnp.log1p(-key_in) + jnp.repeat(group_decay, HG_KDIM, axis=1)
    gain = rec_gain.reshape(1, HG_VDIM)
    zero_state = jnp.zeros((heads, HG_VDIM, HG_KDIM), jnp.float32)
    local_state = recurrence(rec_query, key_in, rec_value, log_forget, zero_state, gain, False)
    decay = jnp.exp(jnp.sum(log_forget, axis=0)).reshape(heads, 1, HG_KDIM)
    reached = jnp.concatenate([local_state, decay], axis=1)
    zz_size = lax.axis_size("zz")
    into_state = zero_state
    if zz_size <= 4:
        for back in range(zz_size - 1, 0, -1):
            came = lax.ppermute(reached, "zz", [(i, i + back) for i in range(zz_size - back)])
            into_state = came[:, HG_VDIM:] * into_state + came[:, :HG_VDIM]
    else:
        reached = lax.all_gather(reached, "zz", axis=0)
        for place in range(zz_size - 1):
            later = reached[place, :, HG_VDIM:] * into_state + reached[place, :, :HG_VDIM]
            into_state = jnp.where(place < zz_index, later, into_state)
    group_out = recurrence(rec_query, key_in, rec_value, log_forget, into_state, gain, True)
    rec_out = lax.all_to_all(group_out, "pl", split_axis=0, concat_axis=1, tiled=True)

    mixed = jnp.dot(rec_out, w_out_rec, preferred_element_type=jnp.float32) + dot_t(
        att_out, w_out_att, 0, 0
    )
    if tp_size != 2:
        return lax.psum_scatter(
            mixed.astype(jnp.bfloat16), "tp", scatter_dimension=0, tiled=True
        )
    half = tok_dev // 2
    sent = lax.dynamic_slice_in_dim(mixed, (1 - tp_index) * half, half, 0).astype(jnp.bfloat16)
    kept = lax.dynamic_slice_in_dim(mixed, tp_index * half, half, 0)
    came = lax.ppermute(sent, "tp", [(0, 1), (1, 0)])
    return (kept + came.astype(jnp.float32)).astype(jnp.bfloat16)


def fast_kernel(
    sp_size,
    group,
    hid,
    wq,
    wf,
    wi,
    gap_ref,
    dec,
    gain_ref,
    wqd_h,
    wkv_h,
    wkr_h,
    qg_ref,
    kg_ref,
    wqn_h,
    wqr_h,
    wk_h,
    wv_h,
    wor_h,
    woa_h,
    out_ref,
    hb,
    wb_all,
    wb_gate,
    wb_query,
    db,
    kbuf,
    lbuf,
    wqd,
    wkv,
    wkr,
    wqn,
    wqr,
    wk,
    wv,
    wor,
    woa,
    wkx,
    wvt,
    qn_ref,
    qbuf,
    top_ref,
    tot_ref,
    acc_ref,
    att_ref,
    pacc,
    proj,
    key_ref,
    log_ref,
    kmid,
    gain_state,
    fade,
    state_ref,
    dsrc,
    ssend,
    sbuf,
    sin_state,
    last_state,
    last_fade,
    ro,
    ra,
    osend,
    orecv,
    oacc,
    odone,
    loc_sem,
    wor_sem,
    own_sem,
    wsend_sem,
    wsem,
    zsend_sem,
    fsend_sem,
    hsend_sem,
    hsem,
    hdsend_sem,
    hdsem,
    dsend_sem,
    dsem,
    lsend_sem,
    lsem,
    ksend_sem,
    ksem,
    kdsend_sem,
    kdsem,
    stsend_sem,
    stsem,
    rsend_sem,
    rsem,
    osend_sem,
    orecv_sem,
    out_sem,
):
    sp = lax.axis_index("sp")
    tp = lax.axis_index("tp")
    depth = sp_size // group
    z = sp // group
    p = sp % group
    y = p // 2
    x = p % 2
    other = 1 - tp
    rows = hb.shape[2]
    half = rows // 2
    span = hb.shape[3]
    krows = wb_all.shape[1]
    heads = sin_state.shape[0]
    wb = (wb_all, wb_gate, wb_query)
    sources = (wq, wf, wi)
    streams = ((0, (0, 1, 2)), (1, (1, 2)), (1, (0,)))
    att_heads = qbuf.shape[0]
    kd = HG_KDIM
    pad = qbuf.shape[1]


    def pj(j):
        return 2 * ((y + j // 2) % 2) + (x + j) % 2

    toward = 1 - 2 * (z // 2)
    inner = ((z + 1) // 2) % 2
    near = z + toward
    far = z + 2 * toward
    last_from = inner * (z - toward) + (1 - inner) * (z + 3 * toward)

    def column(place):
        return place * group + p

    def up(k):
        return ((z + k) % depth) * group + p

    def remote(src, dst, send, recv, place, side=tp):
        return pltpu.make_async_remote_copy(
            src_ref=src,
            dst_ref=dst,
            send_sem=send,
            recv_sem=recv,
            device_id=(place, side),
            device_id_type=MESH,
        )

    def wait_in(ref, sem):
        pltpu.make_async_copy(ref, ref, sem).wait()

    loads = [
        pltpu.make_async_copy(hid, hb.at[p, tp], loc_sem.at[0]),
        pltpu.make_async_copy(wqd_h, wqd, loc_sem.at[1]),
        pltpu.make_async_copy(wkv_h, wkv, loc_sem.at[2]),
        pltpu.make_async_copy(wkr_h, wkr, loc_sem.at[3]),
        pltpu.make_async_copy(wqn_h, wqn, loc_sem.at[4]),
        pltpu.make_async_copy(wqr_h, wqr, loc_sem.at[5]),
        pltpu.make_async_copy(wk_h, wk, loc_sem.at[6]),
        pltpu.make_async_copy(wv_h, wv, loc_sem.at[7]),
        pltpu.make_async_copy(woa_h, woa, loc_sem.at[8]),
    ]
    loads[0].start()
    for s, (h, kinds) in enumerate(streams):
        for n, kind in enumerate(kinds):
            pltpu.make_async_copy(
                sources[kind].at[:, pl.ds(pl.multiple_of((p * heads + h) * kd, kd), kd)],
                wb[s].at[sp, :, pl.ds(n * kd, kd)],
                own_sem.at[s],
            ).start()
    for load in [loads[i] for i in (1, 2, 3, 6, 7, 4, 5, 8)]:
        load.start()
    for h in range(heads):
        for i in range(group):
            pltpu.make_async_copy(
                wor_h.at[pl.ds((i * heads + h) * kd, kd), :],
                wor.at[h, pl.ds(i * kd, kd), :],
                wor_sem.at[h],
            ).start()

    barrier = pltpu.get_barrier_semaphore()
    partners = [(z * group + pj(j), tp) for j in range(1, group)]
    partners += [(up(k), tp) for k in range(1, depth)]
    partners += [(sp, other)]
    for place in partners:
        pl.semaphore_signal(barrier, inc=1, device_id=place, device_id_type=MESH)
    pl.semaphore_wait(barrier, len(partners))

    def launch(copy):
        copy.start()

    launch(remote(hid, hb.at[p, tp], hdsend_sem.at[0], hdsem.at[p], sp, other))

    def plane_copies(s):
        h, kinds = streams[s]
        return [
            remote(
                sources[kind].at[:, pl.ds(pl.multiple_of((pj(j) * heads + h) * kd, kd), kd)],
                wb[s].at[sp, :, pl.ds(n * kd, kd)],
                wsend_sem.at[s],
                wsem.at[s, sp],
                z * group + pj(j),
            )
            for j in range(1, group)
            for n, kind in enumerate(kinds)
        ]

    def plane_weights(s):
        for copy in plane_copies(s):
            launch(copy)

    def weights_in(s, slot):
        wait_in(wb[s].at[slot], wsem.at[s, slot])

    def around(s, j):
        slot = z * group + pj(j)
        if j == 0:
            wait_in(wb[s].at[slot], own_sem.at[s])
        else:
            weights_in(s, slot)
        for copy in around_copies(s, j):
            copy.start()

    def around_copies(s, j):
        slot = z * group + pj(j)
        return [
            remote(
                wb[s].at[slot],
                wb[s].at[slot],
                zsend_sem.at[s],
                wsem.at[s, slot],
                column(place),
            )
            for place in (inner * (z - toward) + (1 - inner) * far, near)
        ]

    def forward(s, j, k, place):
        slot = (near if k == 0 else far) * group + pj(j)

        @pl.when(z == place)
        def _():
            weights_in(s, slot)
            remote(
                wb[s].at[slot],
                wb[s].at[slot],
                fsend_sem.at[s],
                wsem.at[s, slot],
                column(z - toward),
            ).start()

    plane_weights(0)
    around(0, 0)
    def three(values):
        high = values.astype(jnp.bfloat16)
        rest = values - high.astype(jnp.float32)
        mid = rest.astype(jnp.bfloat16)
        low = (rest - mid.astype(jnp.float32)).astype(jnp.bfloat16)
        return high, mid, low

    turned = dec[...]
    block = 2 * HG_BLOCK
    per_row = rows // block
    for i in range(group):
        for h in range(heads):
            for n in range(per_row):
                row = i * heads + h
                dsrc[i, h, n] = turned[row : row + 1, n * block : (n + 1) * block]
    db[p] = dsrc[p]
    for j in range(1, group):
        launch(
            remote(dsrc.at[pj(j)], db.at[p], dsend_sem.at[0], dsem.at[0], z * group + pj(j))
        )
    kr = ROPE // 2
    where = (sp * rows + lax.broadcasted_iota(jnp.int32, (kr, rows), 1)).astype(jnp.float32)
    order = lax.broadcasted_iota(jnp.int32, (kr, rows), 0).astype(jnp.float32)
    angles = where * jnp.exp(order * (-math.log(ROPE_BASE) / kr))
    cosine = jnp.cos(angles)
    sine = jnp.sin(angles)
    loads[6].wait()
    loads[7].wait()
    for head in range(att_heads):
        wkx[:, head * pad : head * pad + NOPE] = wk[
            :, head * NOPE : (head + 1) * NOPE
        ]
        wkx[:, head * pad + NOPE : (head + 1) * pad] = jnp.zeros(
            (wk.shape[0], pad - NOPE), jnp.bfloat16
        )
        qbuf[head, NOPE + ROPE :, :] = jnp.zeros((pad - NOPE - ROPE, rows), jnp.bfloat16)
    wvt[...] = jnp.transpose(wv[...].astype(jnp.float32)).astype(jnp.bfloat16)
    loads[0].wait()
    loads[1].wait()
    loads[2].wait()
    loads[3].wait()
    wait_in(hb.at[p, other], hdsem.at[p])

    def over_features(weight):
        return jnp.dot(
            hb[p, 0], weight[:span, :], preferred_element_type=jnp.float32
        ) + jnp.dot(hb[p, 1], weight[span:, :], preferred_element_type=jnp.float32)

    q_cols = wqd.shape[1]
    kv_cols = wkv.shape[1]
    lbuf[tp, :, :q_cols] = over_features(wqd).astype(jnp.bfloat16)
    lbuf[tp, :, q_cols:] = over_features(wkv).astype(jnp.bfloat16)
    launch(remote(lbuf.at[tp], lbuf.at[tp], lsend_sem.at[0], lsem.at[0], sp, other))
    key_rope = dot_t(wkr[:, :span], hb[p, 0], 1, 1) + dot_t(wkr[:, span:], hb[p, 1], 1, 1)
    first = key_rope[:kr] * cosine - key_rope[kr:] * sine
    second = key_rope[:kr] * sine + key_rope[kr:] * cosine
    kbuf[sp, 0, half:, :] = first.astype(jnp.bfloat16)
    kbuf[sp, 1, half:, :] = second.astype(jnp.bfloat16)
    wait_in(lbuf.at[other], lsem.at[0])
    kv_latent = jnp.concatenate(
        [lbuf[0, :, q_cols:], lbuf[1, :, q_cols:]], axis=1
    ).astype(jnp.float32)
    latent = (
        kv_latent
        * lax.rsqrt(jnp.mean(kv_latent * kv_latent, axis=-1, keepdims=True) + NORM_EPS)
        * kg_ref[...]
    ).astype(jnp.bfloat16)
    kbuf[sp, 0, :half, :] = latent[:half]
    kbuf[sp, 1, :half, :] = latent[half:]

    def key_up(k):
        return remote(
            kbuf.at[sp, tp], kbuf.at[sp, tp], ksend_sem.at[depth + k - 1], ksem.at[sp], up(k)
        )

    def key_plane(g):
        block = ((z + depth - g) % depth) * group + p
        return [
            remote(
                kbuf.at[block, tp],
                kbuf.at[block, tp],
                ksend_sem.at[g],
                ksem.at[block],
                z * group + pj(j),
            )
            for j in range(1, group)
        ]

    def key_core(block, g):
        return remote(
            kbuf.at[block, tp],
            kbuf.at[block, tp],
            kdsend_sem.at[g],
            kdsem.at[block],
            sp,
            other,
        )

    for k in range(1, depth):

        @pl.when(z + k < depth)
        def _(k=k):
            key_up(k).start()

    for copy in key_plane(0):
        copy.start()

    plane_weights(1)
    around(0, 1)
    around(0, 2)

    q_latent = jnp.concatenate(
        [lbuf[0, :, :q_cols], lbuf[1, :, :q_cols]], axis=1
    ).astype(jnp.float32)
    qn_ref[...] = (
        q_latent
        * lax.rsqrt(jnp.mean(q_latent * q_latent, axis=-1, keepdims=True) + NORM_EPS)
        * qg_ref[...]
    ).astype(jnp.bfloat16)
    loads[4].wait()
    loads[5].wait()
    q_nope = dot_t(wqn[...], qn_ref[...], 0, 1)
    q_rope = dot_t(wqr[...], qn_ref[...], 0, 1)
    for head in range(att_heads):
        qbuf[head, :NOPE, :] = q_nope[head * NOPE : (head + 1) * NOPE].astype(jnp.bfloat16)
        lower = q_rope[head * ROPE : head * ROPE + kr]
        upper = q_rope[head * ROPE + kr : (head + 1) * ROPE]
        qbuf[head, NOPE : NOPE + kr, :] = (lower * cosine - upper * sine).astype(jnp.bfloat16)
        qbuf[head, NOPE + kr : NOPE + ROPE, :] = (lower * sine + upper * cosine).astype(jnp.bfloat16)
    top_ref[...] = jnp.full(top_ref.shape, NEG_BIG, jnp.float32)
    tot_ref[...] = jnp.zeros(tot_ref.shape, jnp.float32)
    acc_ref[...] = jnp.zeros(acc_ref.shape, jnp.float32)
    around(0, 3)

    def rows_to(j, part, slot):
        at = hb.at[slot, tp, pl.ds(part * half, half), :]
        return remote(
            at, at, hsend_sem.at[0 if slot is p else 1], hsem.at[slot, part],
            z * group + pj(j),
        )

    def onward(j, part, to):
        wait_in(hb.at[pj(j), tp, pl.ds(part * half, half), :], hsem.at[pj(j), part])
        return rows_to(to, part, pj(j))

    def across(j, part=None):
        if part is not None:
            rows_in(j, part)
        return remote(
            hb.at[pj(j), tp], hb.at[pj(j), tp], hdsend_sem.at[0], hdsem.at[pj(j)], sp, other
        )

    def rows_in(j, part):
        wait_in(hb.at[pj(j), tp, pl.ds(part * half, half), :], hsem.at[pj(j), part])

    scale = math.log2(math.e) / math.sqrt(NOPE + ROPE)
    lane = lax.broadcasted_iota(jnp.int32, (rows, pad), 1)

    def visit(block, masked):
        latent_all = jnp.concatenate([kbuf[block, 0, :half], kbuf[block, 1, :half]], axis=0)
        rope = jnp.concatenate([kbuf[block, 0, half:], kbuf[block, 1, half:]], axis=0)
        v_all = dot_t(wvt[...], latent_all, 1, 1).astype(jnp.bfloat16)
        rope_wide = jnp.transpose(
            jnp.concatenate(
                [
                    jnp.zeros((NOPE, rows), jnp.float32),
                    rope.astype(jnp.float32),
                    jnp.zeros((pad - NOPE - ROPE, rows), jnp.float32),
                ],
                axis=0,
            )
        ).astype(jnp.bfloat16)
        pairs = {}

        def scored(head):
            pair = head // 2
            if pair not in pairs:
                pairs[pair] = jnp.dot(
                    latent_all,
                    wkx[:, pair * 2 * pad : (pair + 1) * 2 * pad],
                    preferred_element_type=jnp.float32,
                ).astype(jnp.bfloat16)
            nope = pairs[pair][:, (head % 2) * pad : (head % 2 + 1) * pad]
            keys = jnp.where(lane < NOPE, nope, rope_wide)
            scores = jnp.dot(keys, qbuf[head], preferred_element_type=jnp.float32)
            if masked:
                key_id = lax.broadcasted_iota(jnp.int32, scores.shape, 0)
                query_id = lax.broadcasted_iota(jnp.int32, scores.shape, 1)
                scores = jnp.where(key_id <= query_id, scores, NEG_BIG)
            return scores

        ahead = [scored(0), scored(1)]
        for head in range(att_heads):
            if head + 2 < att_heads:
                ahead.append(scored(head + 2))
            scores = ahead[head]
            before = top_ref[head]
            top = jnp.maximum(before, jnp.max(scores, axis=0, keepdims=True))
            weights = jnp.exp2(scores * scale - top * scale)
            old = jnp.exp2((before - top) * scale)
            top_ref[head] = top
            tot_ref[head] = tot_ref[head] * old + jnp.sum(weights, axis=0, keepdims=True)
            acc_ref[head] = acc_ref[head] * old + dot_t(
                v_all[head * MLA_V : (head + 1) * MLA_V], weights.astype(jnp.bfloat16), 1, 0
            )

    def block_at(i):
        return ((z + depth - i // group) % depth) * group + pj(i % group)

    def fetch(i):
        wait_in(kbuf.at[block_at(i), tp], ksem.at[block_at(i)])
        key_core(block_at(i), i // group).start()

    count = (z + 1) * group
    fetch(1)
    visit(sp, True)
    around(1, 0)
    around(1, 1)
    around(1, 2)

    def act(copy):
        copy.start()

    def column_keys(g):
        @pl.when(z >= g)
        def _():
            at = ((z + depth - g) % depth) * group + p
            wait_in(kbuf.at[at, tp], ksem.at[at])
            for copy in key_plane(g):
                copy.start()
            key_core(at, g).start()

    def start_bulk():
        for copy in plane_copies(2) + [
            rows_to(j, part, p) for j, part in ((1, 0), (2, 1), (1, 1), (2, 0))
        ]:
            copy.start()

    def spread(side, j):
        @pl.when(inner == side)
        def _():
            around(2, j)

    def diagonal_rows():
        for part in range(2):
            rows_in(group - 1, part)
        across(group - 1).start()

    def pass_on(h, k, *places):
        return [
            lambda j=j, place=place: forward(h, j, k, place)
            for j in range(group)
            for place in places
        ]

    late = {n: [] for n in range(1, sp_size)}
    for n, actions in (
        (2, [lambda g=g: column_keys(g) for g in range(1, depth)]),
        (3, [start_bulk, lambda: around(1, 3), lambda: around(2, 0)]),
        (5, pass_on(0, 0, 1)),
        (7, pass_on(0, 0, 2)),
        (8, pass_on(0, 1, 1)),
        (9, pass_on(0, 1, 2)),
        (6, [lambda j=j: spread(1, j) for j in range(1, group)]),
        (10, [lambda j=j: spread(0, j) for j in range(1, group)]),
        (11, [lambda: act(onward(1, 0, 2)), lambda: act(onward(2, 1, 1))]),
        (12, pass_on(1, 0, 1, 2)),
        (13, [lambda: act(across(1, 1)), lambda: act(across(2, 0))]),
        (14, pass_on(1, 1, 1)),
        (15, [diagonal_rows] + pass_on(2, 0, 1) + pass_on(2, 1, 1)),
    ):
        late[n] += actions

    def step(i, carry):
        for n, actions in late.items():
            for action in actions:
                pl.when(i == n)(action)

        @pl.when(((i + 1) % group != 0) & (i + 1 < count))
        def _():
            fetch(i + 1)

        @pl.when(i < count)
        def _():
            wait_in(kbuf.at[block_at(i), other], kdsem.at[block_at(i)])

            @pl.when(block_at(i) < sp)
            def _():
                visit(block_at(i), False)

        return carry

    lax.fori_loop(1, sp_size, step, 0)
    for head in range(att_heads):
        att_ref[head * MLA_V : (head + 1) * MLA_V, :] = (acc_ref[head] / tot_ref[head]).astype(
            jnp.bfloat16
        )
    slab = group * krows
    place_count = span // slab

    def weights_of(s, place):
        return wb[s][pl.ds(place * group, group)].reshape(slab, wb[s].shape[2])

    def features(i, place):
        columns = pl.ds(pl.multiple_of((place % place_count) * slab, slab), slab)
        return hb[i, place // place_count, :, columns]

    def rows_of(i):
        return pl.ds(pl.multiple_of(i * rows, rows), rows)

    def early_weights(s):
        @pl.when(inner == 0)
        def _():
            for j in range(group):
                for place in (near, far):
                    weights_in(s, place * group + pj(j))

    def project_part(s):
        early_weights(s)
        if s == 0:
            wait_in(db.at[pl.ds(0, group - 1)], dsem.at[0])

        def one(j, carry):
            i = pj(j)
            if s == 0:

                @pl.when(j > 0)
                def _():
                    wait_in(hb.at[i, other], hdsem.at[i])

            pacc[rows_of(i), : wb[s].shape[2]] = sum(
                jnp.dot(
                    features(i, place), weights_of(s, place), preferred_element_type=jnp.float32
                )
                for place in (z, near, far)
            )
            return carry

        lax.fori_loop(0, group, one, 0)

    def project_last(s):
        h, kinds = streams[s]
        for j in range(group):
            weights_in(s, last_from * group + pj(j))

        def one(i, carry):
            here = rows_of(i)
            both = (
                pacc[here, : wb[s].shape[2]]
                + jnp.dot(
                    features(i, last_from),
                    weights_of(s, last_from),
                    preferred_element_type=jnp.float32,
                )
            ).astype(jnp.bfloat16)
            for n, kind in enumerate(kinds):
                piece = both[:, n * kd : (n + 1) * kd]
                if kind == 1:
                    gap = gap_ref[:, pl.ds(pl.multiple_of((p * heads + h) * kd, kd), kd)]
                    keys = gap * jax.nn.sigmoid(-piece.astype(jnp.float32))
                    key_ref[h, here, :] = keys
                    log_ref[h, here, :] = jnp.log1p(-keys)
                else:
                    proj[h, kind // 2, here, :] = piece
            return carry

        lax.fori_loop(0, group, one, 0)

    row_id = lax.broadcasted_iota(jnp.int32, (block, block), 0)
    col_id = lax.broadcasted_iota(jnp.int32, (block, block), 1)
    lower_mask = row_id >= col_id
    tri = jnp.where(lower_mask, 1.0, 0.0).astype(jnp.bfloat16)
    ones = jnp.ones((block, block), jnp.bfloat16)
    steps = group * per_row

    def chunk(c):
        return pl.ds(pl.multiple_of(c * block, block), block)

    def keys_pass(h):
        def one(c, carry):
            here = chunk(c)
            keys = key_ref[h, here, :]
            extras = [
                jnp.where(lower_mask, e.astype(jnp.float32), 0.0).astype(jnp.bfloat16)
                for e in three(db[c // per_row, h, c % per_row])
            ]
            cumulative = jnp.dot(
                jnp.concatenate([tri, tri, tri] + extras, axis=1),
                jnp.concatenate(list(three(log_ref[h, here, :])) + [ones, ones, ones], axis=0),
                preferred_element_type=jnp.float32,
            )
            last = cumulative[block - 1 : block, :]
            centre = cumulative[block // 2 - 1 : block // 2, :]
            log_ref[h, here, :] = cumulative
            kmid[h, here, :] = (keys * jnp.exp(centre - cumulative)).astype(jnp.bfloat16)
            k_last = (keys * jnp.exp(last - cumulative)).astype(jnp.bfloat16)
            gain_state[h, c] = dot_t(proj[h, 1, here, :], k_last, 0, 0)
            fade[h, c] = jnp.exp(last)
            return carry

        lax.fori_loop(0, steps, one, 0, unroll=4)
        state = gain_state[h, 0]
        whole = fade[h, 0]
        for c in range(1, steps):
            state = fade[h, c] * state + gain_state[h, c]
            whole = whole * fade[h, c]
        last_state[h] = state
        last_fade[h] = whole
        post(h, state, whole)

    def post(h, state, whole):
        ssend[h, :HG_VDIM, :] = state.astype(jnp.bfloat16)
        ssend[h, HG_VDIM:, :] = jnp.concatenate(
            list(three(whole)) + [jnp.zeros((ssend.shape[1] - HG_VDIM - 3, kd), jnp.bfloat16)],
            axis=0,
        )

    def state_up(h, k):
        return remote(
            ssend.at[h], sbuf.at[z, h], stsend_sem.at[h, k - 1], stsem.at[h, z], up(k)
        )

    def send_state(h):
        @pl.when((z == 0) | (z == 2 - 2 * h))
        def _():
            state_up(h, 1).start()

    def joined(h):
        post(h, last_fade[h] * sin_state[h] + last_state[h], last_fade[h])

    def take_state(h):
        sin_state[h] = jnp.zeros(sin_state.shape[1:], jnp.float32)

        @pl.when(z == 1)
        def _():
            wait_in(sbuf.at[0, h], stsem.at[h, 0])
            sin_state[h] = sbuf[0, h, :HG_VDIM, :].astype(jnp.float32)
            joined(h)
            state_up(h, 1).start()
            if h == 0:
                state_up(h, 2).start()

        if h == 0:

            @pl.when(z > 1)
            def _():
                wait_in(sbuf.at[1, h], stsem.at[h, 1])
                sin_state[h] = sbuf[1, h, :HG_VDIM, :].astype(jnp.float32)

            @pl.when(z > 2)
            def _():
                wait_in(sbuf.at[2, h], stsem.at[h, 2])
                came = sbuf[2, h].astype(jnp.float32)
                whole = sum(came[HG_VDIM + n : HG_VDIM + n + 1] for n in range(3))
                sin_state[h] = whole * sin_state[h] + came[:HG_VDIM]
        else:

            @pl.when(z == 2)
            def _():
                wait_in(sbuf.at[1, h], stsem.at[h, 1])
                sin_state[h] = sbuf[1, h, :HG_VDIM, :].astype(jnp.float32)
                joined(h)
                state_up(h, 1).start()

            @pl.when(z > 2)
            def _():
                wait_in(sbuf.at[2, h], stsem.at[h, 2])
                sin_state[h] = sbuf[2, h, :HG_VDIM, :].astype(jnp.float32)

    gain = gain_ref[...]

    def carry_states(h):
        state = sin_state[h]
        for c in range(steps):
            state_ref[h, c] = state.astype(jnp.bfloat16)
            state = fade[h, c] * state + gain_state[h, c]

    def query_pass(h):
        for j in range(group - 1, -1, -1):
            i = pj(j)
            for n in range(per_row):
                c = i * per_row + n
                here = chunk(c)
                queries = proj[h, 0, here, :].astype(jnp.float32)
                cumulative = log_ref[h, here, :]
                centre = cumulative[block // 2 - 1 : block // 2, :]
                q_mid = (queries * jnp.exp(cumulative - centre)).astype(jnp.bfloat16)
                q_in = (queries * jnp.exp(cumulative)).astype(jnp.bfloat16)
                scores = jnp.where(
                    lower_mask, dot_t(q_mid, kmid[h, here, :], 1, 1), 0.0
                ).astype(jnp.bfloat16)
                raw = dot_t(scores, proj[h, 1, here, :], 1, 0) + dot_t(
                    q_in, state_ref[h, c], 1, 1
                )
                size = lax.rsqrt(jnp.mean(raw * raw, axis=-1, keepdims=True) + NORM_EPS)
                normed = (raw * size * gain).astype(jnp.bfloat16)
                if j:
                    ro[h, i, n * block : (n + 1) * block, :] = normed
                else:
                    ra[h, p, n * block : (n + 1) * block, :] = normed
            if j:
                launch(
                    remote(
                        ro.at[h, i], ra.at[h, p], rsend_sem.at[h], rsem.at[h], z * group + i
                    )
                )

    tiles = osend.shape[0]
    wide = osend.shape[2]

    def spot(side):
        return pl.ds(pl.multiple_of(side * half, half), half)

    def tile(n):
        return slice(n * wide, (n + 1) * wide)

    def gathered(h, at):
        return jnp.concatenate([ra[h, i, at, :] for i in range(group)], axis=1)

    project_part(0)
    project_last(0)
    keys_pass(0)
    send_state(0)
    loads[8].wait()
    for n in range(tiles):
        oacc[n] = dot_t(att_ref[...], woa[:, tile(n)], 0, 0)
    for j in range(group):
        forward(1, j, 1, 2)

    project_part(1)
    for k in range(2):
        for j in range(group):
            forward(2, j, k, 2)
    take_state(0)
    carry_states(0)
    query_pass(0)
    project_last(1)
    keys_pass(1)
    send_state(1)
    project_part(2)
    take_state(1)
    carry_states(1)
    project_last(2)
    query_pass(1)
    for h in range(heads):
        wait_in(wor.at[h], wor_sem.at[h])
    wait_in(ra.at[0, pl.ds(0, group - 1)], rsem.at[0])
    for n in range(tiles):
        oacc[n] += jnp.dot(
            gathered(0, slice(None)), wor[0, :, tile(n)], preferred_element_type=jnp.float32
        )
    wait_in(ra.at[1, pl.ds(0, group - 1)], rsem.at[1])

    def out_copy(n):
        return pltpu.make_async_copy(odone.at[n], out_ref.at[:, tile(n)], out_sem.at[0])

    def mix(side, n):
        return oacc[n, spot(side), :] + jnp.dot(
            gathered(1, spot(side)), wor[1, :, tile(n)], preferred_element_type=jnp.float32
        )

    for n in range(tiles):
        osend[n] = mix(other, n).astype(jnp.bfloat16)
        launch(remote(osend.at[n], orecv.at[n], osend_sem.at[0], orecv_sem.at[n], sp, other))
    for n in range(tiles):
        oacc[n, spot(tp), :] = mix(tp, n)
    for n in range(tiles):
        wait_in(orecv.at[n], orecv_sem.at[n])
        odone[n] = (oacc[n, spot(tp), :] + orecv[n].astype(jnp.float32)).astype(jnp.bfloat16)
        out_copy(n).start()

    wait_in(odone, out_sem.at[0])
    wait_in(osend, osend_sem.at[0])
    wait_in(hb.at[:, 0], hdsend_sem.at[0])
    wait_in(hb.at[pl.ds(0, 2), 0], hsend_sem.at[0])
    wait_in(hb.at[0, 0], hsend_sem.at[1])
    wait_in(dsrc.at[pl.ds(0, group - 1)], dsend_sem.at[0])
    wait_in(lbuf.at[0], lsend_sem.at[0])
    for s in range(len(streams)):
        wait_in(wb[s].at[pl.ds(0, group - 1)], wsend_sem.at[s])
        wait_in(wb[s].at[pl.ds(0, 2 * group)], zsend_sem.at[s])

    @pl.when(inner == 1)
    def _():
        for s in range(len(streams)):
            wait_in(wb[s].at[pl.ds(0, 2 * group)], fsend_sem.at[s])

    for h in range(heads):
        wait_in(ro.at[h, pl.ds(0, group - 1)], rsend_sem.at[h])

        @pl.when(z < depth - 1)
        def _(h=h):
            state_up(h, 1).wait_send()

        if h == 0:

            @pl.when(z == 1)
            def _(h=h):
                state_up(h, 2).wait_send()

    for k in range(1, depth):

        @pl.when(z + k < depth)
        def _(k=k):
            key_up(k).wait_send()

    for g in range(depth):

        @pl.when(z >= g)
        def _(g=g):
            wait_in(kbuf.at[pl.ds(0, group - 1), 0], ksend_sem.at[g])
            wait_in(kbuf.at[pl.ds(0, group if g else group - 1), 0], kdsend_sem.at[g])


def fast_shards(
    sp_size,
    group,
    hidden_in,
    w_query_rec,
    w_forget,
    w_input,
    forget_gap,
    decay_extra,
    rec_gain,
    w_q_down,
    w_kv_down,
    w_key_rope,
    q_gain,
    kv_gain,
    w_q_nope,
    w_q_rope,
    w_k_up,
    w_v_up,
    w_out_rec,
    w_out_att,
):
    rows, span = hidden_in.shape
    krows, cols = w_query_rec.shape
    all_heads = cols // HG_KDIM
    heads = all_heads // group
    att_heads = w_q_nope.shape[1] // NOPE
    kv_rank = w_k_up.shape[0]
    wide = w_out_rec.shape[1]
    half = rows // 2
    depth = sp_size // group
    block = 2 * HG_BLOCK
    pad = 128 * math.ceil((NOPE + ROPE) / 128)
    tiles = 4
    blocks = (group, heads, rows // block, 1, block)
    operands = (
        hidden_in,
        w_query_rec,
        w_forget,
        w_input,
        forget_gap.reshape(1, -1),
        decay_extra.T,
        rec_gain.reshape(1, -1),
        w_q_down,
        w_kv_down,
        w_key_rope.T,
        q_gain.reshape(1, -1),
        kv_gain.reshape(1, -1),
        w_q_nope,
        w_q_rope,
        w_k_up,
        w_v_up,
        w_out_rec,
        w_out_att,
    )
    far = pl.BlockSpec(memory_space=pl.ANY)
    near = pl.BlockSpec(memory_space=pltpu.VMEM)
    small = (4, 5, 6, 10, 11)
    bf16, f32 = jnp.bfloat16, jnp.float32
    dma = pltpu.SemaphoreType.DMA
    scratch = [
        pltpu.VMEM((group, 2, rows, span), bf16),
        pltpu.VMEM((sp_size, krows, 3 * HG_KDIM), bf16),
        pltpu.VMEM((sp_size, krows, 2 * HG_KDIM), bf16),
        pltpu.VMEM((sp_size, krows, HG_KDIM), bf16),
        pltpu.VMEM(blocks, f32),
        pltpu.VMEM((sp_size, 2, half + ROPE // 2, kv_rank), bf16),
        pltpu.VMEM((2, rows, w_q_down.shape[1] + w_kv_down.shape[1]), bf16),
        pltpu.VMEM(w_q_down.shape, bf16),
        pltpu.VMEM(w_kv_down.shape, bf16),
        pltpu.VMEM(w_key_rope.shape[::-1], bf16),
        pltpu.VMEM(w_q_nope.shape, bf16),
        pltpu.VMEM(w_q_rope.shape, bf16),
        pltpu.VMEM(w_k_up.shape, bf16),
        pltpu.VMEM(w_v_up.shape, bf16),
        pltpu.VMEM((heads, group * HG_VDIM, wide), bf16),
        pltpu.VMEM(w_out_att.shape, bf16),
        pltpu.VMEM((kv_rank, att_heads * pad), bf16),
        pltpu.VMEM(w_v_up.shape[::-1], bf16),
        pltpu.VMEM((rows, w_q_nope.shape[0]), bf16),
        pltpu.VMEM((att_heads, pad, rows), bf16),
        pltpu.VMEM((att_heads, 1, rows), f32),
        pltpu.VMEM((att_heads, 1, rows), f32),
        pltpu.VMEM((att_heads, MLA_V, rows), f32),
        pltpu.VMEM((att_heads * MLA_V, rows), bf16),
        pltpu.VMEM((group * rows, 3 * HG_KDIM), f32),
        pltpu.VMEM((heads, 2, group * rows, HG_KDIM), bf16),
        pltpu.VMEM((heads, group * rows, HG_KDIM), f32),
        pltpu.VMEM((heads, group * rows, HG_KDIM), f32),
        pltpu.VMEM((heads, group * rows, HG_KDIM), bf16),
        pltpu.VMEM((heads, group * rows // block, HG_VDIM, HG_KDIM), f32),
        pltpu.VMEM((heads, group * rows // block, 1, HG_KDIM), f32),
        pltpu.VMEM((heads, group * rows // block, HG_VDIM, HG_KDIM), bf16),
        pltpu.VMEM(blocks, f32),
        pltpu.VMEM((heads, HG_VDIM + 16, HG_KDIM), bf16),
        pltpu.VMEM((depth, heads, HG_VDIM + 16, HG_KDIM), bf16),
        pltpu.VMEM((heads, HG_VDIM, HG_KDIM), f32),
        pltpu.VMEM((heads, HG_VDIM, HG_KDIM), f32),
        pltpu.VMEM((heads, 1, HG_KDIM), f32),
        pltpu.VMEM((heads, group, rows, HG_VDIM), bf16),
        pltpu.VMEM((heads, group, rows, HG_VDIM), bf16),
        pltpu.VMEM((tiles, half, wide // tiles), bf16),
        pltpu.VMEM((tiles, half, wide // tiles), bf16),
        pltpu.VMEM((tiles, rows, wide // tiles), f32),
        pltpu.VMEM((tiles, half, wide // tiles), bf16),
        dma((9,)),
        dma((heads,)),
        dma((3,)),
        dma((3,)),
        dma((3, sp_size)),
        dma((3,)),
        dma((3,)),
        dma((2,)),
        dma((group, 2)),
        dma((1,)),
        dma((group,)),
        dma((1,)),
        dma((1,)),
        dma((1,)),
        dma((1,)),
        dma((2 * depth - 1,)),
        dma((sp_size,)),
        dma((depth,)),
        dma((sp_size,)),
        dma((heads, depth - 1)),
        dma((heads, depth - 1)),
        dma((heads,)),
        dma((heads,)),
        dma((1,)),
        dma((tiles,)),
        dma((1,)),
    ]

    def body(*refs):
        fast_kernel(sp_size, group, *refs)

    return pl.pallas_call(
        body,
        in_specs=[near if i in small else far for i in range(len(operands))],
        out_specs=far,
        out_shape=jax.ShapeDtypeStruct((half, wide), bf16),
        scratch_shapes=scratch,
        compiler_params=pltpu.CompilerParams(
            collective_id=0, has_side_effects=True, vmem_limit_bytes=56 * 1024 * 1024
        ),
        name="layer",
    )(*operands)


def solution(mesh):
    placed = (
        P(("zz", "pl"), "tp"),
        P(("zz", "pl"), "tp"),
        P(("zz", "pl"), "tp"),
        P(("zz", "pl"), "tp"),
        P("tp"),
        P(("zz", "pl"), "tp"),
        P(),
        P(None, "tp"),
        P(None, "tp"),
        P(),
        P(),
        P(),
        P(None, "tp"),
        P(None, "tp"),
        P(None, "tp"),
        P(None, "tp"),
        P("tp", None),
        P("tp", None),
    )
    sp_size, tp_size = mesh.shape["sp"], mesh.shape["tp"]

    def run(hidden_in, w_query_rec, *rest):
        heads_dev = w_query_rec.shape[1] // HG_KDIM // tp_size
        if tp_size == 2 and sp_size == 16 and heads_dev == 8:

            def body(*arrays):
                return fast_shards(sp_size, 4, *arrays)

            flat = [
                P(*("sp" if axis == ("zz", "pl") else axis for axis in spec)) for spec in placed
            ]
            return jax.shard_map(
                body,
                mesh=mesh,
                in_specs=tuple(flat),
                out_specs=P(("sp", "tp"), None),
                check_vma=False,
            )(hidden_in, w_query_rec, *rest)
        group = math.gcd(math.gcd(heads_dev, 4), sp_size)
        split_mesh = Mesh(
            mesh.devices.reshape(sp_size // group, group, tp_size), ("zz", "pl", "tp")
        )
        return jax.shard_map(
            shards,
            mesh=split_mesh,
            in_specs=placed,
            out_specs=P(("zz", "pl", "tp"), None),
            check_vma=False,
        )(hidden_in, w_query_rec, *rest)

    return run
```

```python
import math

import jax
import jax.numpy as jnp
from jax import lax
from jax.experimental import pallas as pl
from jax.experimental.pallas import tpu as pltpu
from jax.sharding import Mesh
from jax.sharding import PartitionSpec as P

HG_KDIM = 128
HG_VDIM = 128
HG_BLOCK = 64
NOPE = 64
ROPE = 32
MLA_V = 64


NORM_EPS = 1e-06
ROPE_BASE = 10000.0
NEG_BIG = -1e30
MESH = pl.DeviceIdType.MESH


def rotate_half(values, cosine, sine_table):
    half_width = values.shape[-1] // 2
    lower_half = values[..., :half_width]
    upper_half = values[..., half_width:]
    return jnp.concatenate(
        [
            lower_half * cosine - upper_half * sine_table,
            lower_half * sine_table + upper_half * cosine,
        ],
        axis=-1,
    )


def rotary_tables(row_count, offset, rot_width):
    positions = jnp.arange(row_count, dtype=jnp.float32) + offset
    frequency = 1.0 / ROPE_BASE ** (jnp.arange(0, rot_width, 2, dtype=jnp.float32) / rot_width)
    angles = positions[:, None] * frequency[None, :]
    return (jnp.cos(angles), jnp.sin(angles))


def dot_t(left, right, left_dim, right_dim):
    return lax.dot_general(
        left, right, (((left_dim,), (right_dim,)), ((), ())), preferred_element_type=jnp.float32
    )


def recurrence_body(rows, q_ref, k_ref, v_ref, lf_ref, s_ref, gain_ref, out_ref, state_ref):
    row_id = lax.broadcasted_iota(jnp.int32, (rows, rows), 0)
    col_id = lax.broadcasted_iota(jnp.int32, (rows, rows), 1)
    lower = row_id >= col_id
    ones = jnp.where(lower, 1.0, 0.0).astype(jnp.float32)
    state = s_ref[0]
    for step in range(k_ref.shape[0] // rows):
        here = pl.ds(step * rows, rows)
        cumulative = jnp.dot(
            ones,
            lf_ref[here, :],
            precision=lax.Precision.HIGHEST,
            preferred_element_type=jnp.float32,
        )
        last = cumulative[rows - 1 : rows, :]
        keys = k_ref[here, :]
        values = v_ref[here, :]
        if out_ref is not None:
            centre = cumulative[rows // 2 - 1 : rows // 2, :]
            queries = q_ref[here, :].astype(jnp.float32)
            q_mid = (queries * jnp.exp(cumulative - centre)).astype(jnp.bfloat16)
            k_mid = (keys * jnp.exp(centre - cumulative)).astype(jnp.bfloat16)
            scores = jnp.where(lower, dot_t(q_mid, k_mid, 1, 1), 0.0).astype(jnp.bfloat16)
            raw = dot_t(scores, values, 1, 0) + dot_t(
                (queries * jnp.exp(cumulative)).astype(jnp.bfloat16),
                state.astype(jnp.bfloat16),
                1,
                1,
            )
            scale = lax.rsqrt(jnp.mean(raw * raw, axis=-1, keepdims=True) + NORM_EPS)
            out_ref[here, :] = (raw * scale * gain_ref[...]).astype(jnp.bfloat16)
        k_last = (keys * jnp.exp(last - cumulative)).astype(jnp.bfloat16)
        state = jnp.exp(last) * state + dot_t(values, k_last, 0, 0)
    if state_ref is not None:
        state_ref[0] = state


def recurrence(queries, keys, values, log_forget, state, gain, emit):
    tokens, width = keys.shape
    heads = width // HG_KDIM
    rows = 2 * HG_BLOCK

    def body(q_ref, k_ref, v_ref, lf_ref, s_ref, gain_ref, out_ref):
        recurrence_body(
            rows,
            q_ref,
            k_ref,
            v_ref,
            lf_ref,
            s_ref,
            gain_ref,
            out_ref if emit else None,
            None if emit else out_ref,
        )

    column = pl.BlockSpec((tokens, HG_KDIM), lambda h: (0, h))
    one_state = pl.BlockSpec((1, HG_VDIM, HG_KDIM), lambda h: (h, 0, 0))
    return pl.pallas_call(
        body,
        grid=(heads,),
        in_specs=[
            column,
            column,
            column,
            column,
            one_state,
            pl.BlockSpec((1, HG_VDIM), lambda h: (0, 0)),
        ],
        out_specs=column if emit else one_state,
        out_shape=jax.ShapeDtypeStruct((tokens, width), jnp.bfloat16)
        if emit
        else jax.ShapeDtypeStruct(state.shape, jnp.float32),
        compiler_params=pltpu.CompilerParams(vmem_limit_bytes=32 * 1024 * 1024),
        cost_estimate=pl.CostEstimate(
            flops=tokens * width * 4000, bytes_accessed=tokens * width * 14, transcendentals=0
        ),
        name="rec_out" if emit else "rec_state",
    )(queries, keys, values, log_forget, state, gain)


def attention_body(
    heads, at_ref, q_ref, lat_ref, rope_ref, wk_ref, wv_ref, out_ref, top_ref, tot_ref, acc_ref
):
    step = pl.program_id(0)
    mine = at_ref[0]

    @pl.when(step == 0)
    def _():
        top_ref[...] = jnp.full(top_ref.shape, NEG_BIG, jnp.float32)
        tot_ref[...] = jnp.zeros(tot_ref.shape, jnp.float32)
        acc_ref[...] = jnp.zeros(acc_ref.shape, jnp.float32)

    def visit(masked):
        latent = lat_ref[...]
        rope = rope_ref[...]
        k_all = dot_t(wk_ref[...], latent, 1, 1).astype(jnp.bfloat16)
        v_all = dot_t(wv_ref[...], latent, 1, 1).astype(jnp.bfloat16)
        for head in range(heads):
            k_head = jnp.concatenate([k_all[head * NOPE : (head + 1) * NOPE], rope], axis=0)
            scores = dot_t(k_head, q_ref[head], 0, 0) * (1.0 / math.sqrt(NOPE + ROPE))
            if masked:
                key_id = lax.broadcasted_iota(jnp.int32, scores.shape, 0)
                query_id = lax.broadcasted_iota(jnp.int32, scores.shape, 1)
                scores = jnp.where(key_id <= query_id, scores, NEG_BIG)
            peak = jnp.max(scores, axis=0, keepdims=True)
            weights = jnp.exp(scores - peak)
            total = jnp.sum(weights, axis=0, keepdims=True)
            part = dot_t(
                v_all[head * MLA_V : (head + 1) * MLA_V], weights.astype(jnp.bfloat16), 1, 0
            )
            before = top_ref[head]
            top = jnp.maximum(before, peak)
            old = jnp.exp(before - top)
            new = jnp.exp(peak - top)
            top_ref[head] = top
            tot_ref[head] = tot_ref[head] * old + total * new
            acc_ref[head] = acc_ref[head] * old + part * new

    @pl.when(step < mine)
    def _():
        visit(False)

    @pl.when(step == mine)
    def _():
        visit(True)
        for head in range(heads):
            out_ref[head * MLA_V : (head + 1) * MLA_V, :] = (
                acc_ref[head] / tot_ref[head]
            ).astype(jnp.bfloat16)


def attention(place, queries, latent, rope, w_key, w_value):
    heads, width, rows = queries.shape
    blocks = latent.shape[0] // rows
    grid_spec = pltpu.PrefetchScalarGridSpec(
        num_scalar_prefetch=1,
        grid=(blocks,),
        in_specs=[
            pl.BlockSpec((heads, width, rows), lambda i, at: (0, 0, 0)),
            pl.BlockSpec((rows, latent.shape[1]), lambda i, at: (jnp.minimum(i, at[0]), 0)),
            pl.BlockSpec((rope.shape[0], rows), lambda i, at: (0, jnp.minimum(i, at[0]))),
            pl.BlockSpec(w_key.shape, lambda i, at: (0, 0)),
            pl.BlockSpec(w_value.shape, lambda i, at: (0, 0)),
        ],
        out_specs=pl.BlockSpec((heads * MLA_V, rows), lambda i, at: (0, 0)),
        scratch_shapes=[
            pltpu.VMEM((heads, 1, rows), jnp.float32),
            pltpu.VMEM((heads, 1, rows), jnp.float32),
            pltpu.VMEM((heads, MLA_V, rows), jnp.float32),
        ],
    )

    def body(*refs):
        attention_body(heads, *refs)

    return pl.pallas_call(
        body,
        grid_spec=grid_spec,
        out_shape=jax.ShapeDtypeStruct((heads * MLA_V, rows), jnp.bfloat16),
        compiler_params=pltpu.CompilerParams(
            dimension_semantics=("arbitrary",), vmem_limit_bytes=32 * 1024 * 1024
        ),
        cost_estimate=pl.CostEstimate(
            flops=blocks * heads * rows * rows * 2000,
            bytes_accessed=latent.size * 2,
            transcendentals=0,
        ),
        name="attend",
    )(place, queries, latent, rope, w_key, w_value)


def both_halves(part, axis):
    if lax.axis_size("tp") != 2:
        return lax.all_gather(part, "tp", axis=axis, tiled=True)
    other = lax.ppermute(part, "tp", [(0, 1), (1, 0)])
    first = lax.axis_index("tp") == 0
    return jnp.concatenate(
        [jnp.where(first, part, other), jnp.where(first, other, part)], axis=axis
    )


def shards(
    hidden_in,
    w_query_rec,
    w_forget,
    w_input,
    forget_gap,
    decay_extra,
    rec_gain,
    w_q_down,
    w_kv_down,
    w_key_rope,
    q_gain,
    kv_gain,
    w_q_nope,
    w_q_rope,
    w_k_up,
    w_v_up,
    w_out_rec,
    w_out_att,
):
    tok_dev = hidden_in.shape[0]
    group = lax.axis_size("pl")
    pl_index = lax.axis_index("pl")
    zz_index = lax.axis_index("zz")
    tp_index = lax.axis_index("tp")
    tp_size = lax.axis_size("tp")
    sp_index = zz_index * group + pl_index

    cols = w_query_rec.shape[1] // group
    heads = cols // HG_KDIM
    depth = w_query_rec.shape[0]
    packed = jnp.concatenate(
        [w.reshape(depth, group, cols) for w in (w_query_rec, w_forget, w_input)], axis=2
    )
    swapped = lax.all_to_all(packed, "pl", split_axis=1, concat_axis=0, tiled=True)
    left_weight = lax.all_gather(
        swapped.reshape(group * depth, 3 * cols), "zz", axis=0, tiled=True
    )
    feature_piece = both_halves(hidden_in, 1)
    member_rows = [feature_piece]
    for gap_to in range(1, group):
        piece = lax.ppermute(hidden_in, "pl", [(i, i ^ gap_to) for i in range(group)])
        member_rows.append(both_halves(piece, 1))
    group_decay = lax.all_gather(decay_extra, "pl", axis=0, tiled=True)
    group_decay = lax.dynamic_slice_in_dim(group_decay, pl_index * heads, heads, 1)

    right_weight = jnp.concatenate([w_q_down, w_kv_down, w_key_rope], axis=1)
    right_sum = jnp.dot(feature_piece, right_weight, preferred_element_type=jnp.float32)
    q_cols = w_q_down.shape[1]
    kv_cols = w_kv_down.shape[1]
    right_round = right_sum[:, : q_cols + kv_cols].astype(jnp.bfloat16)
    both = both_halves(right_round[None], 0).astype(jnp.float32)
    q_latent = jnp.concatenate([both[i, :, :q_cols] for i in range(tp_size)], axis=1)
    kv_latent = jnp.concatenate([both[i, :, q_cols:] for i in range(tp_size)], axis=1)
    q_normed = (
        q_latent
        * lax.rsqrt(jnp.mean(q_latent * q_latent, axis=-1, keepdims=True) + NORM_EPS)
        * q_gain
    ).astype(jnp.bfloat16)
    latent = (
        kv_latent
        * lax.rsqrt(jnp.mean(kv_latent * kv_latent, axis=-1, keepdims=True) + NORM_EPS)
        * kv_gain
    ).astype(jnp.bfloat16)
    q_start = sp_index * tok_dev
    cosine, sine_table = rotary_tables(tok_dev, q_start.astype(jnp.float32), ROPE)
    key_rope = rotate_half(right_sum[:, q_cols + kv_cols :], cosine, sine_table).astype(
        jnp.bfloat16
    )
    group_keys = lax.all_gather(
        jnp.concatenate([latent, key_rope], axis=1), "pl", axis=0, tiled=True
    )
    keys_all = lax.all_gather(group_keys, "zz", axis=0, tiled=True)
    att_heads = w_q_nope.shape[1] // NOPE
    q_nope = jnp.dot(q_normed, w_q_nope, preferred_element_type=jnp.float32).astype(jnp.bfloat16)
    q_rope = jnp.dot(q_normed, w_q_rope, preferred_element_type=jnp.float32).reshape(
        tok_dev, att_heads, ROPE
    )
    q_rope = rotate_half(q_rope, cosine[:, None, :], sine_table[:, None, :]).astype(jnp.bfloat16)
    queries = jnp.concatenate([q_nope.reshape(tok_dev, att_heads, NOPE), q_rope], axis=2)
    att_out = attention(
        sp_index.astype(jnp.int32).reshape(1),
        queries.transpose(1, 2, 0),
        keys_all[:, : latent.shape[1]],
        keys_all[:, latent.shape[1] :].T,
        w_k_up.T,
        w_v_up.T,
    )

    left_weight, att_out = lax.optimization_barrier((left_weight, att_out))
    left_round = jnp.zeros((group * tok_dev, 3 * cols), jnp.bfloat16)
    for gap_to, rows in enumerate(member_rows):
        projected = jnp.dot(rows, left_weight, preferred_element_type=jnp.float32)
        left_round = lax.dynamic_update_slice_in_dim(
            left_round, projected.astype(jnp.bfloat16), (pl_index ^ gap_to) * tok_dev, 0
        )
    rec_query = left_round[:, :cols]
    rec_value = left_round[:, 2 * cols :]
    gap = lax.dynamic_slice_in_dim(forget_gap, pl_index * cols, cols, 0)
    key_in = gap * jax.nn.sigmoid(-left_round[:, cols : 2 * cols].astype(jnp.float32))
    log_forget = jnp.log1p(-key_in) + jnp.repeat(group_decay, HG_KDIM, axis=1)
    gain = rec_gain.reshape(1, HG_VDIM)
    zero_state = jnp.zeros((heads, HG_VDIM, HG_KDIM), jnp.float32)
    local_state = recurrence(rec_query, key_in, rec_value, log_forget, zero_state, gain, False)
    decay = jnp.exp(jnp.sum(log_forget, axis=0)).reshape(heads, 1, HG_KDIM)
    reached = jnp.concatenate([local_state, decay], axis=1)
    zz_size = lax.axis_size("zz")
    into_state = zero_state
    if zz_size <= 4:
        for back in range(zz_size - 1, 0, -1):
            came = lax.ppermute(reached, "zz", [(i, i + back) for i in range(zz_size - back)])
            into_state = came[:, HG_VDIM:] * into_state + came[:, :HG_VDIM]
    else:
        reached = lax.all_gather(reached, "zz", axis=0)
        for place in range(zz_size - 1):
            later = reached[place, :, HG_VDIM:] * into_state + reached[place, :, :HG_VDIM]
            into_state = jnp.where(place < zz_index, later, into_state)
    group_out = recurrence(rec_query, key_in, rec_value, log_forget, into_state, gain, True)
    rec_out = lax.all_to_all(group_out, "pl", split_axis=0, concat_axis=1, tiled=True)

    mixed = jnp.dot(rec_out, w_out_rec, preferred_element_type=jnp.float32) + dot_t(
        att_out, w_out_att, 0, 0
    )
    if tp_size != 2:
        return lax.psum_scatter(
            mixed.astype(jnp.bfloat16), "tp", scatter_dimension=0, tiled=True
        )
    half = tok_dev // 2
    sent = lax.dynamic_slice_in_dim(mixed, (1 - tp_index) * half, half, 0).astype(jnp.bfloat16)
    kept = lax.dynamic_slice_in_dim(mixed, tp_index * half, half, 0)
    came = lax.ppermute(sent, "tp", [(0, 1), (1, 0)])
    return (kept + came.astype(jnp.float32)).astype(jnp.bfloat16)


def fast_kernel(
    sp_size,
    group,
    hid,
    wq,
    wf,
    wi,
    gap_ref,
    dec,
    gain_ref,
    wqd_h,
    wkv_h,
    wkr_h,
    qg_ref,
    kg_ref,
    wqn_h,
    wqr_h,
    wk_h,
    wv_h,
    wor_h,
    woa_h,
    out_ref,
    hb,
    wb_all,
    wb_gate,
    wb_query,
    db,
    kbuf,
    lbuf,
    wqd,
    wkv,
    wkr,
    wqn,
    wqr,
    wk,
    wv,
    wor,
    woa,
    wkx,
    wvt,
    qn_ref,
    qbuf,
    top_ref,
    tot_ref,
    acc_ref,
    att_ref,
    pacc,
    proj,
    key_ref,
    log_ref,
    kmid,
    gain_state,
    fade,
    state_ref,
    dsrc,
    ssend,
    sbuf,
    sin_state,
    last_state,
    last_fade,
    ro,
    ra,
    osend,
    orecv,
    oacc,
    odone,
    loc_sem,
    wor_sem,
    own_sem,
    wsend_sem,
    wsem,
    zsend_sem,
    fsend_sem,
    hsend_sem,
    hsem,
    hdsend_sem,
    hdsem,
    dsend_sem,
    dsem,
    lsend_sem,
    lsem,
    ksend_sem,
    ksem,
    kdsend_sem,
    kdsem,
    stsend_sem,
    stsem,
    rsend_sem,
    rsem,
    osend_sem,
    orecv_sem,
    out_sem,
):
    sp = lax.axis_index("sp")
    tp = lax.axis_index("tp")
    depth = sp_size // group
    z = sp // group
    p = sp % group
    y = p // 2
    x = p % 2
    other = 1 - tp
    rows = hb.shape[2]
    half = rows // 2
    span = hb.shape[3]
    krows = wb_all.shape[1]
    heads = sin_state.shape[0]
    wb = (wb_all, wb_gate, wb_query)
    sources = (wq, wf, wi)
    streams = ((0, (0, 1, 2)), (1, (1, 2)), (1, (0,)))
    att_heads = qbuf.shape[0]
    kd = HG_KDIM
    pad = qbuf.shape[1]


    def pj(j):
        return 2 * ((y + j // 2) % 2) + (x + j) % 2

    toward = 1 - 2 * (z // 2)
    inner = ((z + 1) // 2) % 2
    near = z + toward
    far = z + 2 * toward
    last_from = inner * (z - toward) + (1 - inner) * (z + 3 * toward)

    def column(place):
        return place * group + p

    def up(k):
        return ((z + k) % depth) * group + p

    def remote(src, dst, send, recv, place, side=tp):
        return pltpu.make_async_remote_copy(
            src_ref=src,
            dst_ref=dst,
            send_sem=send,
            recv_sem=recv,
            device_id=(place, side),
            device_id_type=MESH,
        )

    def wait_in(ref, sem):
        pltpu.make_async_copy(ref, ref, sem).wait()

    loads = [
        pltpu.make_async_copy(hid, hb.at[p, tp], loc_sem.at[0]),
        pltpu.make_async_copy(wqd_h, wqd, loc_sem.at[1]),
        pltpu.make_async_copy(wkv_h, wkv, loc_sem.at[2]),
        pltpu.make_async_copy(wkr_h, wkr, loc_sem.at[3]),
        pltpu.make_async_copy(wqn_h, wqn, loc_sem.at[4]),
        pltpu.make_async_copy(wqr_h, wqr, loc_sem.at[5]),
        pltpu.make_async_copy(wk_h, wk, loc_sem.at[6]),
        pltpu.make_async_copy(wv_h, wv, loc_sem.at[7]),
        pltpu.make_async_copy(woa_h, woa, loc_sem.at[8]),
    ]
    loads[0].start()
    for s, (h, kinds) in enumerate(streams):
        for n, kind in enumerate(kinds):
            pltpu.make_async_copy(
                sources[kind].at[:, pl.ds(pl.multiple_of((p * heads + h) * kd, kd), kd)],
                wb[s].at[sp, :, pl.ds(n * kd, kd)],
                own_sem.at[s],
            ).start()
    for load in [loads[i] for i in (1, 2, 3, 6, 7, 4, 5, 8)]:
        load.start()
    for h in range(heads):
        for i in range(group):
            pltpu.make_async_copy(
                wor_h.at[pl.ds((i * heads + h) * kd, kd), :],
                wor.at[h, pl.ds(i * kd, kd), :],
                wor_sem.at[h],
            ).start()

    barrier = pltpu.get_barrier_semaphore()
    partners = [(z * group + pj(j), tp) for j in range(1, group)]
    partners += [(up(k), tp) for k in range(1, depth)]
    partners += [(sp, other)]
    for place in partners:
        pl.semaphore_signal(barrier, inc=1, device_id=place, device_id_type=MESH)
    pl.semaphore_wait(barrier, len(partners))

    def launch(copy):
        copy.start()

    launch(remote(hid, hb.at[p, tp], hdsend_sem.at[0], hdsem.at[p], sp, other))

    def plane_copies(s):
        h, kinds = streams[s]
        return [
            remote(
                sources[kind].at[:, pl.ds(pl.multiple_of((pj(j) * heads + h) * kd, kd), kd)],
                wb[s].at[sp, :, pl.ds(n * kd, kd)],
                wsend_sem.at[s],
                wsem.at[s, sp],
                z * group + pj(j),
            )
            for j in range(1, group)
            for n, kind in enumerate(kinds)
        ]

    def plane_weights(s):
        for copy in plane_copies(s):
            launch(copy)

    def weights_in(s, slot):
        wait_in(wb[s].at[slot], wsem.at[s, slot])

    def around(s, j):
        slot = z * group + pj(j)
        if j == 0:
            wait_in(wb[s].at[slot], own_sem.at[s])
        else:
            weights_in(s, slot)
        for copy in around_copies(s, j):
            copy.start()

    def around_copies(s, j):
        slot = z * group + pj(j)
        return [
            remote(
                wb[s].at[slot],
                wb[s].at[slot],
                zsend_sem.at[s],
                wsem.at[s, slot],
                column(place),
            )
            for place in (inner * (z - toward) + (1 - inner) * far, near)
        ]

    def forward(s, j, k, place):
        slot = (near if k == 0 else far) * group + pj(j)

        @pl.when(z == place)
        def _():
            weights_in(s, slot)
            remote(
                wb[s].at[slot],
                wb[s].at[slot],
                fsend_sem.at[s],
                wsem.at[s, slot],
                column(z - toward),
            ).start()

    plane_weights(0)
    around(0, 0)
    def three(values):
        high = values.astype(jnp.bfloat16)
        rest = values - high.astype(jnp.float32)
        mid = rest.astype(jnp.bfloat16)
        low = (rest - mid.astype(jnp.float32)).astype(jnp.bfloat16)
        return high, mid, low

    turned = dec[...]
    block = 2 * HG_BLOCK
    per_row = rows // block
    for i in range(group):
        for h in range(heads):
            for n in range(per_row):
                row = i * heads + h
                dsrc[i, h, n] = turned[row : row + 1, n * block : (n + 1) * block]
    db[p] = dsrc[p]
    for j in range(1, group):
        launch(
            remote(dsrc.at[pj(j)], db.at[p], dsend_sem.at[0], dsem.at[0], z * group + pj(j))
        )
    kr = ROPE // 2
    where = (sp * rows + lax.broadcasted_iota(jnp.int32, (kr, rows), 1)).astype(jnp.float32)
    order = lax.broadcasted_iota(jnp.int32, (kr, rows), 0).astype(jnp.float32)
    angles = where * jnp.exp(order * (-math.log(ROPE_BASE) / kr))
    cosine = jnp.cos(angles)
    sine = jnp.sin(angles)
    loads[6].wait()
    loads[7].wait()
    for head in range(att_heads):
        wkx[:, head * pad : head * pad + NOPE] = wk[
            :, head * NOPE : (head + 1) * NOPE
        ]
        wkx[:, head * pad + NOPE : (head + 1) * pad] = jnp.zeros(
            (wk.shape[0], pad - NOPE), jnp.bfloat16
        )
        qbuf[head, NOPE + ROPE :, :] = jnp.zeros((pad - NOPE - ROPE, rows), jnp.bfloat16)
    wvt[...] = jnp.transpose(wv[...].astype(jnp.float32)).astype(jnp.bfloat16)
    loads[0].wait()
    loads[1].wait()
    loads[2].wait()
    loads[3].wait()
    wait_in(hb.at[p, other], hdsem.at[p])

    def over_features(weight):
        return jnp.dot(
            hb[p, 0], weight[:span, :], preferred_element_type=jnp.float32
        ) + jnp.dot(hb[p, 1], weight[span:, :], preferred_element_type=jnp.float32)

    q_cols = wqd.shape[1]
    kv_cols = wkv.shape[1]
    lbuf[tp, :, :q_cols] = over_features(wqd).astype(jnp.bfloat16)
    lbuf[tp, :, q_cols:] = over_features(wkv).astype(jnp.bfloat16)
    launch(remote(lbuf.at[tp], lbuf.at[tp], lsend_sem.at[0], lsem.at[0], sp, other))
    key_rope = dot_t(wkr[:, :span], hb[p, 0], 1, 1) + dot_t(wkr[:, span:], hb[p, 1], 1, 1)
    first = key_rope[:kr] * cosine - key_rope[kr:] * sine
    second = key_rope[:kr] * sine + key_rope[kr:] * cosine
    kbuf[sp, 0, half:, :] = first.astype(jnp.bfloat16)
    kbuf[sp, 1, half:, :] = second.astype(jnp.bfloat16)
    wait_in(lbuf.at[other], lsem.at[0])
    kv_latent = jnp.concatenate(
        [lbuf[0, :, q_cols:], lbuf[1, :, q_cols:]], axis=1
    ).astype(jnp.float32)
    latent = (
        kv_latent
        * lax.rsqrt(jnp.mean(kv_latent * kv_latent, axis=-1, keepdims=True) + NORM_EPS)
        * kg_ref[...]
    ).astype(jnp.bfloat16)
    kbuf[sp, 0, :half, :] = latent[:half]
    kbuf[sp, 1, :half, :] = latent[half:]

    def key_up(k):
        return remote(
            kbuf.at[sp, tp], kbuf.at[sp, tp], ksend_sem.at[depth + k - 1], ksem.at[sp], up(k)
        )

    def key_plane(g):
        block = ((z + depth - g) % depth) * group + p
        return [
            remote(
                kbuf.at[block, tp],
                kbuf.at[block, tp],
                ksend_sem.at[g],
                ksem.at[block],
                z * group + pj(j),
            )
            for j in range(1, group)
        ]

    def key_core(block, g):
        return remote(
            kbuf.at[block, tp],
            kbuf.at[block, tp],
            kdsend_sem.at[g],
            kdsem.at[block],
            sp,
            other,
        )

    for k in range(1, depth):

        @pl.when(z + k < depth)
        def _(k=k):
            key_up(k).start()

    for copy in key_plane(0):
        copy.start()

    plane_weights(1)
    around(0, 1)
    around(0, 2)

    q_latent = jnp.concatenate(
        [lbuf[0, :, :q_cols], lbuf[1, :, :q_cols]], axis=1
    ).astype(jnp.float32)
    qn_ref[...] = (
        q_latent
        * lax.rsqrt(jnp.mean(q_latent * q_latent, axis=-1, keepdims=True) + NORM_EPS)
        * qg_ref[...]
    ).astype(jnp.bfloat16)
    loads[4].wait()
    loads[5].wait()
    q_nope = dot_t(wqn[...], qn_ref[...], 0, 1)
    q_rope = dot_t(wqr[...], qn_ref[...], 0, 1)
    for head in range(att_heads):
        qbuf[head, :NOPE, :] = q_nope[head * NOPE : (head + 1) * NOPE].astype(jnp.bfloat16)
        lower = q_rope[head * ROPE : head * ROPE + kr]
        upper = q_rope[head * ROPE + kr : (head + 1) * ROPE]
        qbuf[head, NOPE : NOPE + kr, :] = (lower * cosine - upper * sine).astype(jnp.bfloat16)
        qbuf[head, NOPE + kr : NOPE + ROPE, :] = (lower * sine + upper * cosine).astype(jnp.bfloat16)
    top_ref[...] = jnp.full(top_ref.shape, NEG_BIG, jnp.float32)
    tot_ref[...] = jnp.zeros(tot_ref.shape, jnp.float32)
    acc_ref[...] = jnp.zeros(acc_ref.shape, jnp.float32)
    around(0, 3)

    def rows_to(j, part, slot):
        at = hb.at[slot, tp, pl.ds(part * half, half), :]
        return remote(
            at, at, hsend_sem.at[0 if slot is p else 1], hsem.at[slot, part],
            z * group + pj(j),
        )

    def onward(j, part, to):
        wait_in(hb.at[pj(j), tp, pl.ds(part * half, half), :], hsem.at[pj(j), part])
        return rows_to(to, part, pj(j))

    def across(j, part=None):
        if part is not None:
            rows_in(j, part)
        return remote(
            hb.at[pj(j), tp], hb.at[pj(j), tp], hdsend_sem.at[0], hdsem.at[pj(j)], sp, other
        )

    def rows_in(j, part):
        wait_in(hb.at[pj(j), tp, pl.ds(part * half, half), :], hsem.at[pj(j), part])

    scale = math.log2(math.e) / math.sqrt(NOPE + ROPE)
    lane = lax.broadcasted_iota(jnp.int32, (rows, pad), 1)

    def visit(block, masked):
        latent_all = jnp.concatenate([kbuf[block, 0, :half], kbuf[block, 1, :half]], axis=0)
        rope = jnp.concatenate([kbuf[block, 0, half:], kbuf[block, 1, half:]], axis=0)
        v_all = dot_t(wvt[...], latent_all, 1, 1).astype(jnp.bfloat16)
        rope_wide = jnp.transpose(
            jnp.concatenate(
                [
                    jnp.zeros((NOPE, rows), jnp.float32),
                    rope.astype(jnp.float32),
                    jnp.zeros((pad - NOPE - ROPE, rows), jnp.float32),
                ],
                axis=0,
            )
        ).astype(jnp.bfloat16)
        pairs = {}

        def scored(head):
            pair = head // 2
            if pair not in pairs:
                pairs[pair] = jnp.dot(
                    latent_all,
                    wkx[:, pair * 2 * pad : (pair + 1) * 2 * pad],
                    preferred_element_type=jnp.float32,
                ).astype(jnp.bfloat16)
            nope = pairs[pair][:, (head % 2) * pad : (head % 2 + 1) * pad]
            keys = jnp.where(lane < NOPE, nope, rope_wide)
            scores = jnp.dot(keys, qbuf[head], preferred_element_type=jnp.float32)
            if masked:
                key_id = lax.broadcasted_iota(jnp.int32, scores.shape, 0)
                query_id = lax.broadcasted_iota(jnp.int32, scores.shape, 1)
                scores = jnp.where(key_id <= query_id, scores, NEG_BIG)
            return scores

        ahead = [scored(0), scored(1)]
        for head in range(att_heads):
            if head + 2 < att_heads:
                ahead.append(scored(head + 2))
            scores = ahead[head]
            before = top_ref[head]
            top = jnp.maximum(before, jnp.max(scores, axis=0, keepdims=True))
            weights = jnp.exp2(scores * scale - top * scale)
            old = jnp.exp2((before - top) * scale)
            top_ref[head] = top
            tot_ref[head] = tot_ref[head] * old + jnp.sum(weights, axis=0, keepdims=True)
            acc_ref[head] = acc_ref[head] * old + dot_t(
                v_all[head * MLA_V : (head + 1) * MLA_V], weights.astype(jnp.bfloat16), 1, 0
            )

    def block_at(i):
        return ((z + depth - i // group) % depth) * group + pj(i % group)

    def fetch(i):
        wait_in(kbuf.at[block_at(i), tp], ksem.at[block_at(i)])
        key_core(block_at(i), i // group).start()

    count = (z + 1) * group
    fetch(1)
    visit(sp, True)
    around(1, 0)
    around(1, 1)
    around(1, 2)

    def act(copy):
        copy.start()

    def column_keys(g):
        @pl.when(z >= g)
        def _():
            at = ((z + depth - g) % depth) * group + p
            wait_in(kbuf.at[at, tp], ksem.at[at])
            for copy in key_plane(g):
                copy.start()
            key_core(at, g).start()

    def start_bulk():
        for copy in plane_copies(2) + [
            rows_to(j, part, p) for j, part in ((1, 0), (2, 1), (1, 1), (2, 0))
        ]:
            copy.start()

    def spread(side, j):
        @pl.when(inner == side)
        def _():
            around(2, j)

    def diagonal_rows():
        for part in range(2):
            rows_in(group - 1, part)
        across(group - 1).start()

    def pass_on(h, k, *places):
        return [
            lambda j=j, place=place: forward(h, j, k, place)
            for j in range(group)
            for place in places
        ]

    late = {n: [] for n in range(1, sp_size)}
    for n, actions in (
        (2, [lambda g=g: column_keys(g) for g in range(1, depth)]),
        (3, [start_bulk, lambda: around(1, 3), lambda: around(2, 0)]),
        (5, pass_on(0, 0, 1)),
        (7, pass_on(0, 0, 2)),
        (8, pass_on(0, 1, 1)),
        (9, pass_on(0, 1, 2)),
        (6, [lambda j=j: spread(1, j) for j in range(1, group)]),
        (10, [lambda j=j: spread(0, j) for j in range(1, group)]),
        (11, [lambda: act(onward(1, 0, 2)), lambda: act(onward(2, 1, 1))]),
        (12, pass_on(1, 0, 1, 2)),
        (13, [lambda: act(across(1, 1)), lambda: act(across(2, 0))]),
        (14, pass_on(1, 1, 1)),
        (15, [diagonal_rows] + pass_on(2, 0, 1) + pass_on(2, 1, 1)),
    ):
        late[n] += actions

    def step(i, carry):
        for n, actions in late.items():
            for action in actions:
                pl.when(i == n)(action)

        @pl.when(((i + 1) % group != 0) & (i + 1 < count))
        def _():
            fetch(i + 1)

        @pl.when(i < count)
        def _():
            wait_in(kbuf.at[block_at(i), other], kdsem.at[block_at(i)])

            @pl.when(block_at(i) < sp)
            def _():
                visit(block_at(i), False)

        return carry

    lax.fori_loop(1, sp_size, step, 0)
    for head in range(att_heads):
        att_ref[head * MLA_V : (head + 1) * MLA_V, :] = (acc_ref[head] / tot_ref[head]).astype(
            jnp.bfloat16
        )
    slab = group * krows
    place_count = span // slab

    def weights_of(s, place):
        return wb[s][pl.ds(place * group, group)].reshape(slab, wb[s].shape[2])

    def features(i, place):
        columns = pl.ds(pl.multiple_of((place % place_count) * slab, slab), slab)
        return hb[i, place // place_count, :, columns]

    def rows_of(i):
        return pl.ds(pl.multiple_of(i * rows, rows), rows)

    def early_weights(s):
        @pl.when(inner == 0)
        def _():
            for j in range(group):
                for place in (near, far):
                    weights_in(s, place * group + pj(j))

    def project_part(s):
        early_weights(s)
        if s == 0:
            wait_in(db.at[pl.ds(0, group - 1)], dsem.at[0])

        def one(j, carry):
            i = pj(j)
            if s == 0:

                @pl.when(j > 0)
                def _():
                    wait_in(hb.at[i, other], hdsem.at[i])

            pacc[rows_of(i), : wb[s].shape[2]] = sum(
                jnp.dot(
                    features(i, place), weights_of(s, place), preferred_element_type=jnp.float32
                )
                for place in (z, near, far)
            )
            return carry

        lax.fori_loop(0, group, one, 0)

    def project_last(s):
        h, kinds = streams[s]
        for j in range(group):
            weights_in(s, last_from * group + pj(j))

        def one(i, carry):
            here = rows_of(i)
            both = (
                pacc[here, : wb[s].shape[2]]
                + jnp.dot(
                    features(i, last_from),
                    weights_of(s, last_from),
                    preferred_element_type=jnp.float32,
                )
            ).astype(jnp.bfloat16)
            for n, kind in enumerate(kinds):
                piece = both[:, n * kd : (n + 1) * kd]
                if kind == 1:
                    gap = gap_ref[:, pl.ds(pl.multiple_of((p * heads + h) * kd, kd), kd)]
                    keys = gap * jax.nn.sigmoid(-piece.astype(jnp.float32))
                    key_ref[h, here, :] = keys
                    log_ref[h, here, :] = jnp.log1p(-keys)
                else:
                    proj[h, kind // 2, here, :] = piece
            return carry

        lax.fori_loop(0, group, one, 0)

    row_id = lax.broadcasted_iota(jnp.int32, (block, block), 0)
    col_id = lax.broadcasted_iota(jnp.int32, (block, block), 1)
    lower_mask = row_id >= col_id
    tri = jnp.where(lower_mask, 1.0, 0.0).astype(jnp.bfloat16)
    ones = jnp.ones((block, block), jnp.bfloat16)
    steps = group * per_row

    def chunk(c):
        return pl.ds(pl.multiple_of(c * block, block), block)

    def keys_pass(h):
        def one(c, carry):
            here = chunk(c)
            keys = key_ref[h, here, :]
            extras = [
                jnp.where(lower_mask, e.astype(jnp.float32), 0.0).astype(jnp.bfloat16)
                for e in three(db[c // per_row, h, c % per_row])
            ]
            cumulative = jnp.dot(
                jnp.concatenate([tri, tri, tri] + extras, axis=1),
                jnp.concatenate(list(three(log_ref[h, here, :])) + [ones, ones, ones], axis=0),
                preferred_element_type=jnp.float32,
            )
            last = cumulative[block - 1 : block, :]
            centre = cumulative[block // 2 - 1 : block // 2, :]
            log_ref[h, here, :] = cumulative
            kmid[h, here, :] = (keys * jnp.exp(centre - cumulative)).astype(jnp.bfloat16)
            k_last = (keys * jnp.exp(last - cumulative)).astype(jnp.bfloat16)
            gain_state[h, c] = dot_t(proj[h, 1, here, :], k_last, 0, 0)
            fade[h, c] = jnp.exp(last)
            return carry

        lax.fori_loop(0, steps, one, 0, unroll=4)
        state = gain_state[h, 0]
        whole = fade[h, 0]
        for c in range(1, steps):
            state = fade[h, c] * state + gain_state[h, c]
            whole = whole * fade[h, c]
        last_state[h] = state
        last_fade[h] = whole
        post(h, state, whole)

    def post(h, state, whole):
        ssend[h, :HG_VDIM, :] = state.astype(jnp.bfloat16)
        ssend[h, HG_VDIM:, :] = jnp.concatenate(
            list(three(whole)) + [jnp.zeros((ssend.shape[1] - HG_VDIM - 3, kd), jnp.bfloat16)],
            axis=0,
        )

    def state_up(h, k):
        return remote(
            ssend.at[h], sbuf.at[z, h], stsend_sem.at[h, k - 1], stsem.at[h, z], up(k)
        )

    def send_state(h):
        @pl.when((z == 0) | (z == 2 - 2 * h))
        def _():
            state_up(h, 1).start()

    def joined(h):
        post(h, last_fade[h] * sin_state[h] + last_state[h], last_fade[h])

    def take_state(h):
        sin_state[h] = jnp.zeros(sin_state.shape[1:], jnp.float32)

        @pl.when(z == 1)
        def _():
            wait_in(sbuf.at[0, h], stsem.at[h, 0])
            sin_state[h] = sbuf[0, h, :HG_VDIM, :].astype(jnp.float32)
            joined(h)
            state_up(h, 1).start()
            if h == 0:
                state_up(h, 2).start()

        if h == 0:

            @pl.when(z > 1)
            def _():
                wait_in(sbuf.at[1, h], stsem.at[h, 1])
                sin_state[h] = sbuf[1, h, :HG_VDIM, :].astype(jnp.float32)

            @pl.when(z > 2)
            def _():
                wait_in(sbuf.at[2, h], stsem.at[h, 2])
                came = sbuf[2, h].astype(jnp.float32)
                whole = sum(came[HG_VDIM + n : HG_VDIM + n + 1] for n in range(3))
                sin_state[h] = whole * sin_state[h] + came[:HG_VDIM]
        else:

            @pl.when(z == 2)
            def _():
                wait_in(sbuf.at[1, h], stsem.at[h, 1])
                sin_state[h] = sbuf[1, h, :HG_VDIM, :].astype(jnp.float32)
                joined(h)
                state_up(h, 1).start()

            @pl.when(z > 2)
            def _():
                wait_in(sbuf.at[2, h], stsem.at[h, 2])
                sin_state[h] = sbuf[2, h, :HG_VDIM, :].astype(jnp.float32)

    gain = gain_ref[...]

    def carry_states(h):
        state = sin_state[h]
        for c in range(steps):
            state_ref[h, c] = state.astype(jnp.bfloat16)
            state = fade[h, c] * state + gain_state[h, c]

    def query_pass(h):
        for j in range(group - 1, -1, -1):
            i = pj(j)
            for n in range(per_row):
                c = i * per_row + n
                here = chunk(c)
                queries = proj[h, 0, here, :].astype(jnp.float32)
                cumulative = log_ref[h, here, :]
                centre = cumulative[block // 2 - 1 : block // 2, :]
                q_mid = (queries * jnp.exp(cumulative - centre)).astype(jnp.bfloat16)
                q_in = (queries * jnp.exp(cumulative)).astype(jnp.bfloat16)
                scores = jnp.where(
                    lower_mask, dot_t(q_mid, kmid[h, here, :], 1, 1), 0.0
                ).astype(jnp.bfloat16)
                raw = dot_t(scores, proj[h, 1, here, :], 1, 0) + dot_t(
                    q_in, state_ref[h, c], 1, 1
                )
                size = lax.rsqrt(jnp.mean(raw * raw, axis=-1, keepdims=True) + NORM_EPS)
                normed = (raw * size * gain).astype(jnp.bfloat16)
                if j:
                    ro[h, i, n * block : (n + 1) * block, :] = normed
                else:
                    ra[h, p, n * block : (n + 1) * block, :] = normed
            if j:
                launch(
                    remote(
                        ro.at[h, i], ra.at[h, p], rsend_sem.at[h], rsem.at[h], z * group + i
                    )
                )

    tiles = osend.shape[0]
    wide = osend.shape[2]

    def spot(side):
        return pl.ds(pl.multiple_of(side * half, half), half)

    def tile(n):
        return slice(n * wide, (n + 1) * wide)

    def gathered(h, at):
        return jnp.concatenate([ra[h, i, at, :] for i in range(group)], axis=1)

    project_part(0)
    project_last(0)
    keys_pass(0)
    send_state(0)
    loads[8].wait()
    for n in range(tiles):
        oacc[n] = dot_t(att_ref[...], woa[:, tile(n)], 0, 0)
    for j in range(group):
        forward(1, j, 1, 2)

    project_part(1)
    for k in range(2):
        for j in range(group):
            forward(2, j, k, 2)
    take_state(0)
    carry_states(0)
    query_pass(0)
    project_last(1)
    keys_pass(1)
    send_state(1)
    project_part(2)
    take_state(1)
    carry_states(1)
    project_last(2)
    query_pass(1)
    for h in range(heads):
        wait_in(wor.at[h], wor_sem.at[h])
    wait_in(ra.at[0, pl.ds(0, group - 1)], rsem.at[0])
    for n in range(tiles):
        oacc[n] += jnp.dot(
            gathered(0, slice(None)), wor[0, :, tile(n)], preferred_element_type=jnp.float32
        )
    wait_in(ra.at[1, pl.ds(0, group - 1)], rsem.at[1])

    def out_copy(n):
        return pltpu.make_async_copy(odone.at[n], out_ref.at[:, tile(n)], out_sem.at[0])

    def mix(side, n):
        return oacc[n, spot(side), :] + jnp.dot(
            gathered(1, spot(side)), wor[1, :, tile(n)], preferred_element_type=jnp.float32
        )

    for n in range(tiles):
        osend[n] = mix(other, n).astype(jnp.bfloat16)
        launch(remote(osend.at[n], orecv.at[n], osend_sem.at[0], orecv_sem.at[n], sp, other))
    for n in range(tiles):
        kept = mix(tp, n)
        wait_in(orecv.at[n], orecv_sem.at[n])
        odone[n] = (kept + orecv[n].astype(jnp.float32)).astype(jnp.bfloat16)
        out_copy(n).start()

    wait_in(odone, out_sem.at[0])
    wait_in(osend, osend_sem.at[0])
    wait_in(hb.at[:, 0], hdsend_sem.at[0])
    wait_in(hb.at[pl.ds(0, 2), 0], hsend_sem.at[0])
    wait_in(hb.at[0, 0], hsend_sem.at[1])
    wait_in(dsrc.at[pl.ds(0, group - 1)], dsend_sem.at[0])
    wait_in(lbuf.at[0], lsend_sem.at[0])
    for s in range(len(streams)):
        wait_in(wb[s].at[pl.ds(0, group - 1)], wsend_sem.at[s])
        wait_in(wb[s].at[pl.ds(0, 2 * group)], zsend_sem.at[s])

    @pl.when(inner == 1)
    def _():
        for s in range(len(streams)):
            wait_in(wb[s].at[pl.ds(0, 2 * group)], fsend_sem.at[s])

    for h in range(heads):
        wait_in(ro.at[h, pl.ds(0, group - 1)], rsend_sem.at[h])

        @pl.when(z < depth - 1)
        def _(h=h):
            state_up(h, 1).wait_send()

        if h == 0:

            @pl.when(z == 1)
            def _(h=h):
                state_up(h, 2).wait_send()

    for k in range(1, depth):

        @pl.when(z + k < depth)
        def _(k=k):
            key_up(k).wait_send()

    for g in range(depth):

        @pl.when(z >= g)
        def _(g=g):
            wait_in(kbuf.at[pl.ds(0, group - 1), 0], ksend_sem.at[g])
            wait_in(kbuf.at[pl.ds(0, group if g else group - 1), 0], kdsend_sem.at[g])


def fast_shards(
    sp_size,
    group,
    hidden_in,
    w_query_rec,
    w_forget,
    w_input,
    forget_gap,
    decay_extra,
    rec_gain,
    w_q_down,
    w_kv_down,
    w_key_rope,
    q_gain,
    kv_gain,
    w_q_nope,
    w_q_rope,
    w_k_up,
    w_v_up,
    w_out_rec,
    w_out_att,
):
    rows, span = hidden_in.shape
    krows, cols = w_query_rec.shape
    all_heads = cols // HG_KDIM
    heads = all_heads // group
    att_heads = w_q_nope.shape[1] // NOPE
    kv_rank = w_k_up.shape[0]
    wide = w_out_rec.shape[1]
    half = rows // 2
    depth = sp_size // group
    block = 2 * HG_BLOCK
    pad = 128 * math.ceil((NOPE + ROPE) / 128)
    tiles = 4
    blocks = (group, heads, rows // block, 1, block)
    operands = (
        hidden_in,
        w_query_rec,
        w_forget,
        w_input,
        forget_gap.reshape(1, -1),
        decay_extra.T,
        rec_gain.reshape(1, -1),
        w_q_down,
        w_kv_down,
        w_key_rope.T,
        q_gain.reshape(1, -1),
        kv_gain.reshape(1, -1),
        w_q_nope,
        w_q_rope,
        w_k_up,
        w_v_up,
        w_out_rec,
        w_out_att,
    )
    far = pl.BlockSpec(memory_space=pl.ANY)
    near = pl.BlockSpec(memory_space=pltpu.VMEM)
    small = (4, 5, 6, 10, 11)
    bf16, f32 = jnp.bfloat16, jnp.float32
    dma = pltpu.SemaphoreType.DMA
    scratch = [
        pltpu.VMEM((group, 2, rows, span), bf16),
        pltpu.VMEM((sp_size, krows, 3 * HG_KDIM), bf16),
        pltpu.VMEM((sp_size, krows, 2 * HG_KDIM), bf16),
        pltpu.VMEM((sp_size, krows, HG_KDIM), bf16),
        pltpu.VMEM(blocks, f32),
        pltpu.VMEM((sp_size, 2, half + ROPE // 2, kv_rank), bf16),
        pltpu.VMEM((2, rows, w_q_down.shape[1] + w_kv_down.shape[1]), bf16),
        pltpu.VMEM(w_q_down.shape, bf16),
        pltpu.VMEM(w_kv_down.shape, bf16),
        pltpu.VMEM(w_key_rope.shape[::-1], bf16),
        pltpu.VMEM(w_q_nope.shape, bf16),
        pltpu.VMEM(w_q_rope.shape, bf16),
        pltpu.VMEM(w_k_up.shape, bf16),
        pltpu.VMEM(w_v_up.shape, bf16),
        pltpu.VMEM((heads, group * HG_VDIM, wide), bf16),
        pltpu.VMEM(w_out_att.shape, bf16),
        pltpu.VMEM((kv_rank, att_heads * pad), bf16),
        pltpu.VMEM(w_v_up.shape[::-1], bf16),
        pltpu.VMEM((rows, w_q_nope.shape[0]), bf16),
        pltpu.VMEM((att_heads, pad, rows), bf16),
        pltpu.VMEM((att_heads, 1, rows), f32),
        pltpu.VMEM((att_heads, 1, rows), f32),
        pltpu.VMEM((att_heads, MLA_V, rows), f32),
        pltpu.VMEM((att_heads * MLA_V, rows), bf16),
        pltpu.VMEM((group * rows, 3 * HG_KDIM), f32),
        pltpu.VMEM((heads, 2, group * rows, HG_KDIM), bf16),
        pltpu.VMEM((heads, group * rows, HG_KDIM), f32),
        pltpu.VMEM((heads, group * rows, HG_KDIM), f32),
        pltpu.VMEM((heads, group * rows, HG_KDIM), bf16),
        pltpu.VMEM((heads, group * rows // block, HG_VDIM, HG_KDIM), f32),
        pltpu.VMEM((heads, group * rows // block, 1, HG_KDIM), f32),
        pltpu.VMEM((heads, group * rows // block, HG_VDIM, HG_KDIM), bf16),
        pltpu.VMEM(blocks, f32),
        pltpu.VMEM((heads, HG_VDIM + 16, HG_KDIM), bf16),
        pltpu.VMEM((depth, heads, HG_VDIM + 16, HG_KDIM), bf16),
        pltpu.VMEM((heads, HG_VDIM, HG_KDIM), f32),
        pltpu.VMEM((heads, HG_VDIM, HG_KDIM), f32),
        pltpu.VMEM((heads, 1, HG_KDIM), f32),
        pltpu.VMEM((heads, group, rows, HG_VDIM), bf16),
        pltpu.VMEM((heads, group, rows, HG_VDIM), bf16),
        pltpu.VMEM((tiles, half, wide // tiles), bf16),
        pltpu.VMEM((tiles, half, wide // tiles), bf16),
        pltpu.VMEM((tiles, rows, wide // tiles), f32),
        pltpu.VMEM((tiles, half, wide // tiles), bf16),
        dma((9,)),
        dma((heads,)),
        dma((3,)),
        dma((3,)),
        dma((3, sp_size)),
        dma((3,)),
        dma((3,)),
        dma((2,)),
        dma((group, 2)),
        dma((1,)),
        dma((group,)),
        dma((1,)),
        dma((1,)),
        dma((1,)),
        dma((1,)),
        dma((2 * depth - 1,)),
        dma((sp_size,)),
        dma((depth,)),
        dma((sp_size,)),
        dma((heads, depth - 1)),
        dma((heads, depth - 1)),
        dma((heads,)),
        dma((heads,)),
        dma((1,)),
        dma((tiles,)),
        dma((1,)),
    ]

    def body(*refs):
        fast_kernel(sp_size, group, *refs)

    return pl.pallas_call(
        body,
        in_specs=[near if i in small else far for i in range(len(operands))],
        out_specs=far,
        out_shape=jax.ShapeDtypeStruct((half, wide), bf16),
        scratch_shapes=scratch,
        compiler_params=pltpu.CompilerParams(
            collective_id=0, has_side_effects=True, vmem_limit_bytes=56 * 1024 * 1024
        ),
        name="layer",
    )(*operands)


def solution(mesh):
    placed = (
        P(("zz", "pl"), "tp"),
        P(("zz", "pl"), "tp"),
        P(("zz", "pl"), "tp"),
        P(("zz", "pl"), "tp"),
        P("tp"),
        P(("zz", "pl"), "tp"),
        P(),
        P(None, "tp"),
        P(None, "tp"),
        P(),
        P(),
        P(),
        P(None, "tp"),
        P(None, "tp"),
        P(None, "tp"),
        P(None, "tp"),
        P("tp", None),
        P("tp", None),
    )
    sp_size, tp_size = mesh.shape["sp"], mesh.shape["tp"]

    def run(hidden_in, w_query_rec, *rest):
        heads_dev = w_query_rec.shape[1] // HG_KDIM // tp_size
        if tp_size == 2 and sp_size == 16 and heads_dev == 8:

            def body(*arrays):
                return fast_shards(sp_size, 4, *arrays)

            flat = [
                P(*("sp" if axis == ("zz", "pl") else axis for axis in spec)) for spec in placed
            ]
            return jax.shard_map(
                body,
                mesh=mesh,
                in_specs=tuple(flat),
                out_specs=P(("sp", "tp"), None),
                check_vma=False,
            )(hidden_in, w_query_rec, *rest)
        group = math.gcd(math.gcd(heads_dev, 4), sp_size)
        split_mesh = Mesh(
            mesh.devices.reshape(sp_size // group, group, tp_size), ("zz", "pl", "tp")
        )
        return jax.shard_map(
            shards,
            mesh=split_mesh,
            in_specs=placed,
            out_specs=P(("zz", "pl", "tp"), None),
            check_vma=False,
        )(hidden_in, w_query_rec, *rest)

    return run
```
